32 devices in a mesh: ep: 8 (over z, core), tp: 4 (over y, x).
Axes of the slice: x: 2, y: 2, z: 4, core: 2. Of those that a mesh axis runs over, the one named last changes fastest.
Arguments:
- mixer_value_input: bfloat16 [2048, 4096], P('ep', 'tp'), may hold values from -6 to 6
- input_state_matrix: bfloat16 [2048, 2048], P('ep', 'tp'), may hold values from -6 to 6
- output_state_matrix: bfloat16 [2048, 2048], P('ep', 'tp'), may hold values from -6 to 6
- output_gate_input: bfloat16 [2048, 4096], P('ep', 'tp'), may hold values from -6 to 6
- step_input: float32 [2048, 64], P('ep', 'tp'), may hold values from -6 to -2
- extra_log_decay: float32 [2048, 64], P('ep', 'tp'), may hold values from -1 to 0
- head_log_decay: float32 [64], P('tp'), may hold values from -10 to 1
- head_skip_scale: float32 [64], P('tp'), may hold values from 0.5 to 2
- value_kernel: float32 [4, 4096], P(None, 'tp'), may hold values from -3 to 3
- input_matrix_kernel: float32 [4, 2048], P(None, 'tp'), may hold values from -3 to 3
- output_matrix_kernel: float32 [4, 2048], P(None, 'tp'), may hold values from -3 to 3
- mixer_norm_scale: float32 [4096], P('tp'), may hold values from 0.1 to 1.9
- mixer_output_weight: bfloat16 [4096, 2048], P(None, 'tp'), may hold values from -0.09375 to 0.09375
- second_token_rows: bfloat16 [2048, 2048], P('ep'), may hold values from -6 to 6
- expert_norm_scale: float32 [2048], replicated, may hold values from 0.1 to 1.9
- routed_expert_index: int32 [2048, 4], P('ep'), may hold values from 0 to 15, all different within a row; in each aligned block of 256 rows (0 to 255, 256 to 511, ...) at most 96 rows name the same one
- routed_expert_weight: float32 [2048, 4], P('ep'), may hold values from 0.1 to 1
- routed_gate_weight: bfloat16 [16, 2048, 1024], P('ep', None, 'tp'), may hold values from -0.125 to 0.125
- routed_up_weight: bfloat16 [16, 2048, 1024], P('ep', None, 'tp'), may hold values from -0.125 to 0.125
- routed_down_weight: bfloat16 [16, 1024, 2048], P('ep', None, 'tp'), may hold values from -0.1875 to 0.1875
- shared_gate_weight: bfloat16 [2048, 1024], P(None, 'tp'), may hold values from -0.125 to 0.125
- shared_up_weight: bfloat16 [2048, 1024], P(None, 'tp'), may hold values from -0.125 to 0.125
- shared_down_weight: bfloat16 [1024, 2048], P(None, 'tp'), may hold values from -0.1875 to 0.1875
Outputs:
- mixer_output: bfloat16 [2048, 2048], P('ep', 'tp')
- routed_out: bfloat16 [2048, 2048], P('ep', 'tp')
The draws below stay inside these ranges and needn't reach their ends.
Inputs may be any that keep to these rules, and one draw needn't show every extreme that they name: `routed_expert_index`: in each aligned block of 256 rows (the rows of one index of ep) no expert is named more than 96 times, a bound that some block reaches.
All inputs are finite; a program needn't handle non-finite values.
Results may differ from the reference program's by a relative error of at most 0.012.
Values may be sent and summed in bfloat16 or wider, within the bound.
A program may use at most 64 MiB of HBM per device.

```python
import math
from functools import partial
import jax
import jax.numpy as jnp
import numpy as np
from jax import lax

D = 2048
HEADS = 64
HEAD_DIM = 64
INNER = 4096
GROUPS = 16
STATE = 128
CONV_TAPS = 4
BLOCK = 128
EXPERT_FF = 1024
SHARED_FF = 1024
EXPERTS = 16
TOP_K = 4
TOK_B = 256
TOKENS_A = 2048
TOKENS_B = 2048
CAP = 96
N_EP = 8


def draw_step_input(key, part):
    first_key, second_key = jax.random.split(jax.random.fold_in(key, 11))
    nblocks = TOKENS_A // BLOCK
    offset = jax.random.uniform(first_key, (nblocks, 1, HEADS), jnp.float32, -0.7, 0.7)
    noise = 0.3 * jax.random.truncated_normal(second_key, -2.0, 2.0, (nblocks, BLOCK, HEADS), jnp.float32)
    return (-4.0 + offset + noise).reshape(TOKENS_A, HEADS)


def draw_extra_log_decay(key, part):
    first_key, second_key = jax.random.split(jax.random.fold_in(key, 23))
    spots = jax.random.randint(first_key, (2,), 0, TOKENS_A)
    positions = jnp.arange(TOKENS_A)
    struck = jnp.any(positions[:, None] == spots[None, :], axis=1)
    losses = jnp.log(jax.random.uniform(second_key, (TOKENS_A, HEADS), jnp.float32, 0.5, 0.8))
    return jnp.where(struck[:, None], losses, 0.0).astype(jnp.float32)


def draw_head_log_decay(key, part):
    first_key, second_key, third_key = jax.random.split(jax.random.fold_in(key, 37), 3)
    slow_share = 0.5
    slow_heads = jax.random.uniform(first_key, (HEADS,), jnp.float32) < slow_share
    slow_rate = jax.random.uniform(second_key, (HEADS,), jnp.float32, 0.2, 1.0) * 30.0 / TOKENS_A
    fast_rate = jnp.exp(jax.random.uniform(third_key, (HEADS,), jnp.float32, jnp.log(0.5), jnp.log(1.5)))
    return jnp.log(jnp.where(slow_heads, slow_rate, fast_rate)).astype(jnp.float32)


def shard_levels(key, dims, shards, smallest, top_value):
    def one(axis_at, blocks):
        heights = jax.random.uniform(jax.random.fold_in(jax.random.fold_in(key, 6), axis_at), (blocks,), jnp.float32, smallest / len(shards), top_value / len(shards))
        return jnp.repeat(jnp.exp(heights), dims[axis_at] // blocks).reshape((-1,) + (1,) * (len(dims) - axis_at - 1))

    level = one(*shards[0])
    for cut in shards[1:]:
        level = level * one(*cut)
    return level


def deal_out(rng, own, number, rows, count, top, limit, lean):
    sequence = jax.random.permutation(rng, count)
    packed, common = portions_of(count, rows * top, limit, lean, True), portions_of(count, rows * top, limit, lean, False)
    places = jnp.arange(count)

    def named(tallies, turn):
        used = int((tallies > 0).sum())
        fixed = max(1, used // 4)
        moved = fixed + (places - fixed + turn * (used - fixed)) % max(1, count - fixed)
        return jnp.zeros((count,), jnp.int32).at[sequence[jnp.where(places < fixed, places, moved)]].set(jnp.asarray(tallies, jnp.int32))

    tallies = jnp.where(number % 4 == 0, named(packed, number // 4), named(common, number - number // 4 - 1))
    mixed = jax.random.permutation(jax.random.fold_in(own, 3), count)
    donor, sink = mixed[0:count // 2 * 2:2], mixed[1:count // 2 * 2:2]
    slack = jnp.minimum(tallies[donor] - 1, limit - tallies[sink]) // 2
    slack = jnp.where((donor == sequence[0]) | (sink == sequence[0]) | (tallies[sink] == 0), 0, jnp.maximum(slack, 0))
    moved = jax.random.randint(jax.random.fold_in(own, 4), (count // 2,), 0, 1 << 20) % (slack + 1)
    tallies = tallies.at[donor].add(-moved).at[sink].add(moved)
    labels = jnp.searchsorted(jnp.cumsum(tallies), jnp.arange(rows * top), side="right").astype(jnp.int32)
    table = labels.reshape(top, rows).T
    table = table[jax.random.permutation(jax.random.fold_in(own, 1), rows)]
    turn = jax.random.randint(jax.random.fold_in(own, 2), (rows, 1), 0, top)
    return jnp.take_along_axis(table, (jnp.arange(top)[None, :] + turn) % top, axis=1)


def portions_of(amount, total, bound, skew, full):
    weights = [(1 << 20) // math.isqrt(grade ** skew) + 1 for grade in range(1, amount + 1)]
    largest = bound if full else min(bound, max(-(-total // amount), total * weights[0] // sum(weights)))
    least = 1 if total - largest >= amount - 1 else 0
    counts, spare = [largest] + [least] * (amount - 1), total - largest - least * (amount - 1)
    while spare > 0:
        candidates = [i for i in range(1, amount) if counts[i] < largest] or [i for i in range(1, amount) if counts[i] < bound]
        whole, remaining = sum([weights[i] for i in candidates]), spare
        for i in candidates:
            extra = min(bound - counts[i], max(1, remaining * weights[i] // whole), spare)
            counts[i] = counts[i] + extra
            spare = spare - extra
    return np.array(counts)


def gaussian(key, shape, width, most, cuts=(), kind=jnp.bfloat16):
    array = jax.random.normal(key, shape, jnp.float32) * width
    if len(cuts) > 0:
        array = shard_levels(key, shape, cuts, -0.22, 0.18) * array
    return jnp.clip(array, min=-most, max=most).astype(kind)


def setup_inputs(seed: int = 0) -> dict:
    arg_keys = jax.random.split(jax.random.key(seed), 24)
    mixer_value_input = gaussian(arg_keys[0], (TOKENS_A, INNER), 1.0, 6.0, ((0, 8), (1, 4)))
    input_state_matrix = gaussian(arg_keys[1], (TOKENS_A, GROUPS * STATE), 1.0, 6.0, ((0, 8), (1, 4)))
    output_state_matrix = gaussian(arg_keys[2], (TOKENS_A, GROUPS * STATE), 1.0, 6.0, ((0, 8), (1, 4)))
    output_gate_input = gaussian(arg_keys[3], (TOKENS_A, INNER), 1.0, 6.0, ((0, 8), (1, 4)))
    step_input = draw_step_input(jax.random.fold_in(arg_keys[23], 71), 0)
    extra_log_decay = draw_extra_log_decay(jax.random.fold_in(arg_keys[23], 71), 0)
    head_log_decay = draw_head_log_decay(jax.random.fold_in(arg_keys[23], 71), 0)
    head_skip_scale = jnp.clip(0.5 + 1.5 * jax.random.uniform(arg_keys[7], (HEADS,), jnp.float32) ** shard_levels(arg_keys[7], (HEADS,), ((0, 4),), -0.2, 0.2), 0.5, 2.0)
    value_kernel = gaussian(arg_keys[8], (CONV_TAPS, INNER), 0.5, 3.0, ((1, 4),), jnp.float32)
    input_matrix_kernel = gaussian(arg_keys[9], (CONV_TAPS, GROUPS * STATE), 0.5, 3.0, ((1, 4),), jnp.float32)
    output_matrix_kernel = gaussian(arg_keys[10], (CONV_TAPS, GROUPS * STATE), 0.5, 3.0, ((1, 4),), jnp.float32)
    mixer_norm_scale = jnp.clip(1.0 + 0.18 * jax.random.normal(arg_keys[11], (INNER,), jnp.float32), 0.1, 1.9)
    mixer_output_weight = gaussian(arg_keys[12], (INNER, D), INNER ** -0.5, 0.09375, ((1, 4),))
    second_token_rows = gaussian(arg_keys[13], (TOKENS_B, D), 1.0, 6.0, ((0, 8),))
    expert_norm_scale = jnp.clip(1.0 + 0.18 * jax.random.normal(arg_keys[14], (D,), jnp.float32), 0.1, 1.9)
    routed_expert_index_keys = jax.random.split(jax.random.fold_in(arg_keys[15], 1), TOKENS_B // TOK_B)
    routed_expert_index_turns = jax.random.permutation(jax.random.fold_in(arg_keys[15], 3), TOKENS_B // TOK_B)
    routed_expert_index = jax.vmap(lambda own, number: deal_out(jax.random.fold_in(arg_keys[15], 2), own, number, TOK_B, EXPERTS, TOP_K, CAP, 2))(routed_expert_index_keys, routed_expert_index_turns).reshape((TOKENS_B, TOP_K))
    routed_expert_weight = jnp.clip(0.1 + 0.9 * jax.random.uniform(arg_keys[16], (TOKENS_B, TOP_K), jnp.float32) ** shard_levels(arg_keys[16], (TOKENS_B, TOP_K), ((0, 8),), -0.2, 0.2), 0.1, 1.0)
    routed_gate_weight = gaussian(arg_keys[17], (EXPERTS, D, EXPERT_FF), D ** -0.5, 0.125, ((0, 8), (2, 4)))
    routed_up_weight = gaussian(arg_keys[18], (EXPERTS, D, EXPERT_FF), D ** -0.5, 0.125, ((0, 8), (2, 4)))
    routed_down_weight = gaussian(arg_keys[19], (EXPERTS, EXPERT_FF, D), EXPERT_FF ** -0.5, 0.1875, ((0, 8), (2, 4)))
    shared_gate_weight = gaussian(arg_keys[20], (D, SHARED_FF), D ** -0.5, 0.125, ((1, 4),))
    shared_up_weight = gaussian(arg_keys[21], (D, SHARED_FF), D ** -0.5, 0.125, ((1, 4),))
    shared_down_weight = gaussian(arg_keys[22], (SHARED_FF, D), SHARED_FF ** -0.5, 0.1875, ((1, 4),))
    return {"mixer_value_input": mixer_value_input, "input_state_matrix": input_state_matrix, "output_state_matrix": output_state_matrix, "output_gate_input": output_gate_input, "step_input": step_input, "extra_log_decay": extra_log_decay, "head_log_decay": head_log_decay, "head_skip_scale": head_skip_scale, "value_kernel": value_kernel, "input_matrix_kernel": input_matrix_kernel, "output_matrix_kernel": output_matrix_kernel, "mixer_norm_scale": mixer_norm_scale, "mixer_output_weight": mixer_output_weight, "second_token_rows": second_token_rows, "expert_norm_scale": expert_norm_scale, "routed_expert_index": routed_expert_index, "routed_expert_weight": routed_expert_weight, "routed_gate_weight": routed_gate_weight, "routed_up_weight": routed_up_weight, "routed_down_weight": routed_down_weight, "shared_gate_weight": shared_gate_weight, "shared_up_weight": shared_up_weight, "shared_down_weight": shared_down_weight}


epsilon = 1e-05
precise = lax.Precision.HIGHEST

def conv_silu(source, weights):
    length = source.shape[0]
    padded = jnp.concatenate([jnp.zeros((CONV_TAPS - 1, source.shape[1]), source.dtype), source], axis=0)
    total_sum = jnp.zeros(source.shape, jnp.float32)
    for tap_index in range(CONV_TAPS):
        total_sum = total_sum + padded[tap_index:tap_index + length].astype(jnp.float32) * weights[tap_index]
    return jax.nn.silu(total_sum).astype(jnp.bfloat16)

def route_slots(route_block, experts, capacity):
    flat_ids = route_block.reshape(-1)
    onehot = (flat_ids[:, None] == jnp.arange(experts, dtype=jnp.int32)[None, :]).astype(jnp.int32)
    earlier = jnp.cumsum(onehot, axis=0) - onehot
    position_in = lax.optimization_barrier(jnp.sum(earlier * onehot, axis=1)).astype(jnp.int32)
    slot_index = (flat_ids * capacity + position_in).astype(jnp.int32)
    owner_row = (jnp.arange(flat_ids.shape[0], dtype=jnp.int32) // route_block.shape[1]).astype(jnp.int32)
    slot_owner = jnp.full((experts * capacity,), route_block.shape[0], jnp.int32).at[slot_index].set(owner_row)
    return (slot_owner, slot_index)

def spread_weights(slot_index, weights, count):
    return jnp.zeros((count,), jnp.float32).at[slot_index].set(weights)

def mixer_portion(mixer_value_input, input_state_matrix, output_state_matrix, output_gate_input, step_input, extra_log_decay, head_log_decay, head_skip_scale, value_kernel, input_matrix_kernel, output_matrix_kernel, mixer_norm_scale, mixer_output_weight):
    length = mixer_value_input.shape[0]
    values = conv_silu(mixer_value_input, value_kernel)
    in_mat = conv_silu(input_state_matrix, input_matrix_kernel)
    out_mat = conv_silu(output_state_matrix, output_matrix_kernel)
    step_length = jax.nn.softplus(step_input)
    decay_logarithm = -jnp.exp(head_log_decay)[None, :] * step_length + extra_log_decay
    head_ratio = HEADS // GROUPS
    nblocks = length // BLOCK
    value_wide = values.astype(jnp.float32).reshape(nblocks, BLOCK, HEADS, HEAD_DIM)
    in_wide = in_mat.astype(jnp.float32).reshape(nblocks, BLOCK, GROUPS, STATE)
    out_wide = out_mat.astype(jnp.float32).reshape(nblocks, BLOCK, GROUPS, STATE)
    step_blocks = step_length.reshape(nblocks, BLOCK, HEADS)
    log_blocks = decay_logarithm.reshape(nblocks, BLOCK, HEADS)
    lower_mask = jnp.tril(jnp.ones((BLOCK, BLOCK), bool))

    def advance(carried, inputs):
        value_blk, in_blk, out_blk, step_blk, log_blk = inputs
        running = jnp.cumsum(log_blk, axis=0)
        scaled = value_blk * step_blk[:, :, None]
        scores = jnp.einsum('ign,jgn->gij', out_blk, in_blk, precision=precise)
        scores = jnp.repeat(scores, head_ratio, axis=0)
        spread = jnp.transpose(running[:, None, :] - running[None, :, :], (2, 0, 1))
        decay_mat = jnp.where(lower_mask[None], jnp.exp(jnp.where(lower_mask[None], spread, 0.0)), 0.0)
        inside = jnp.einsum('hij,jhp->ihp', scores * decay_mat, scaled, precision=precise)
        out_head = jnp.repeat(out_blk, head_ratio, axis=1)
        in_head = jnp.repeat(in_blk, head_ratio, axis=1)
        carried_term = jnp.einsum('ihn,hpn->ihp', out_head, carried, precision=precise) * jnp.exp(running)[:, :, None]
        to_end = jnp.exp(running[-1][None, :] - running)
        updated = carried * jnp.exp(running[-1])[:, None, None] + jnp.einsum('jhn,jh,jhp->hpn', in_head, to_end, scaled, precision=precise)
        return (updated, inside + carried_term)
    start_state = jnp.zeros((HEADS, HEAD_DIM, STATE), jnp.float32)
    _, mixed_heads = lax.scan(advance, start_state, (value_wide, in_wide, out_wide, step_blocks, log_blocks))
    mixed_heads = mixed_heads.reshape(length, HEADS, HEAD_DIM) + head_skip_scale[None, :, None] * value_wide.reshape(length, HEADS, HEAD_DIM)
    gated_heads = mixed_heads * jax.nn.silu(output_gate_input.astype(jnp.float32)).reshape(length, HEADS, HEAD_DIM)
    grouped = gated_heads.reshape(length, GROUPS, head_ratio * HEAD_DIM)
    grouped = grouped * lax.rsqrt(lax.optimization_barrier(jnp.mean(grouped * grouped, axis=-1, keepdims=True)) + epsilon)
    normed = (grouped.reshape(length, HEADS * HEAD_DIM) * mixer_norm_scale).astype(jnp.bfloat16)
    return jnp.dot(normed, mixer_output_weight, preferred_element_type=jnp.float32).astype(jnp.bfloat16)

def expert_part(second_token_rows, expert_norm_scale, routed_expert_index, routed_expert_weight, routed_gate_weight, routed_up_weight, routed_down_weight, shared_gate_weight, shared_up_weight, shared_down_weight):
    total_rows = second_token_rows.shape[0]
    rows_wide = second_token_rows.astype(jnp.float32)
    normed = (rows_wide * lax.rsqrt(lax.optimization_barrier(jnp.mean(rows_wide * rows_wide, axis=-1, keepdims=True)) + epsilon) * expert_norm_scale).astype(jnp.bfloat16)
    block_ids = routed_expert_index.reshape(N_EP, TOK_B, TOP_K)
    tables, slot_sets = jax.vmap(partial(route_slots, experts=EXPERTS, capacity=CAP))(block_ids)
    offsets = (jnp.arange(N_EP, dtype=jnp.int32) * TOK_B)[:, None]
    global_rows = jnp.where(tables == TOK_B, total_rows, tables + offsets).astype(jnp.int32)
    slot_weights = jax.vmap(partial(spread_weights, count=EXPERTS * CAP))(slot_sets, routed_expert_weight.reshape(N_EP, TOK_B * TOP_K))
    expert_rows = global_rows.reshape(N_EP, EXPERTS, CAP).transpose(1, 0, 2).reshape(EXPERTS, N_EP * CAP)
    expert_weights = slot_weights.reshape(N_EP, EXPERTS, CAP).transpose(1, 0, 2).reshape(EXPERTS, N_EP * CAP)
    padded = jnp.concatenate([normed, jnp.zeros((1, normed.shape[1]), jnp.bfloat16)], axis=0)

    def one_expert(accumulated, inputs):
        row_index, weights, gate_w, up_w, down_w = inputs
        picked = jnp.take(padded, row_index, axis=0)
        hidden = (jax.nn.silu(jnp.dot(picked, gate_w, preferred_element_type=jnp.float32)) * jnp.dot(picked, up_w, preferred_element_type=jnp.float32)).astype(jnp.bfloat16)
        output = jnp.dot(hidden, down_w, preferred_element_type=jnp.float32).astype(jnp.bfloat16)
        return (accumulated.at[row_index].add(output.astype(jnp.float32) * weights[:, None]), None)
    accumulated = jnp.zeros((total_rows + 1, normed.shape[1]), jnp.float32)
    accumulated, _ = lax.scan(one_expert, accumulated, (expert_rows, expert_weights, routed_gate_weight, routed_up_weight, routed_down_weight))
    shared_hidden = (jax.nn.silu(jnp.dot(normed, shared_gate_weight, preferred_element_type=jnp.float32)) * jnp.dot(normed, shared_up_weight, preferred_element_type=jnp.float32)).astype(jnp.bfloat16)
    shared_result = jnp.dot(shared_hidden, shared_down_weight, preferred_element_type=jnp.float32)
    return (accumulated[:total_rows] + shared_result).astype(jnp.bfloat16)

def reference(mixer_value_input, input_state_matrix, output_state_matrix, output_gate_input, step_input, extra_log_decay, head_log_decay, head_skip_scale, value_kernel, input_matrix_kernel, output_matrix_kernel, mixer_norm_scale, mixer_output_weight, second_token_rows, expert_norm_scale, routed_expert_index, routed_expert_weight, routed_gate_weight, routed_up_weight, routed_down_weight, shared_gate_weight, shared_up_weight, shared_down_weight):
    mixer_output = mixer_portion(mixer_value_input, input_state_matrix, output_state_matrix, output_gate_input, step_input, extra_log_decay, head_log_decay, head_skip_scale, value_kernel, input_matrix_kernel, output_matrix_kernel, mixer_norm_scale, mixer_output_weight)
    routed_out = expert_part(second_token_rows, expert_norm_scale, routed_expert_index, routed_expert_weight, routed_gate_weight, routed_up_weight, routed_down_weight, shared_gate_weight, shared_up_weight, shared_down_weight)
    return (mixer_output, routed_out)
```

```python
import functools
import types

import jax
import jax.numpy as jnp
from jax import lax
from jax.experimental import pallas as pl
from jax.experimental.pallas import tpu as pltpu
from jax.sharding import PartitionSpec as P

HEAD_DIM = 64
STATE = 128
CONV_TAPS = 4
BLOCK = 128
TOP_K = 4


epsilon = 1e-05
precise = lax.Precision.HIGHEST


def passed_along(x, axis, by):
    size = lax.axis_size(axis)
    pairs = [(i, i + by) for i in range(size) if 0 <= i + by < size]
    return lax.ppermute(x, axis, pairs)


def carried_in(total_log, state, axis):
    size = lax.axis_size(axis)
    place = lax.axis_index(axis)
    log = passed_along(total_log, axis, 1)
    hold = passed_along(state.astype(jnp.bfloat16), axis, 1).astype(jnp.float32)
    by = 1
    while by < size - 1:
        before = passed_along(hold.astype(jnp.bfloat16), axis, by).astype(jnp.float32)
        hold = hold + jnp.exp(log)[:, None, None] * before
        log = log + passed_along(log, axis, by)
        by *= 2
    return hold


def conv_silu(tail_rows, source, weights):
    length = source.shape[0]
    padded = jnp.concatenate([tail_rows, source], axis=0)
    total_sum = jnp.zeros(source.shape, jnp.float32)
    for tap_index in range(CONV_TAPS):
        total_sum = (
            total_sum
            + padded[tap_index : tap_index + length].astype(jnp.float32) * weights[tap_index]
        )
    return jax.nn.silu(total_sum).astype(jnp.bfloat16)


def carry_blocks(carried, inputs):
    block_decay, block_state = inputs
    return (carried * block_decay[:, None, None] + block_state, carried)


def earlier_counts(mask, rows):
    at = jnp.arange(rows)
    tri = (at[:, None] < at[None, :]).astype(jnp.bfloat16)
    return lax.dot_general(
        mask.astype(jnp.bfloat16),
        tri,
        (((mask.ndim - 1,), (0,)), ((), ())),
        preferred_element_type=jnp.float32,
    )


def on_device(
    mixer_value_input,
    input_state_matrix,
    output_state_matrix,
    output_gate_input,
    step_input,
    extra_log_decay,
    head_log_decay,
    head_skip_scale,
    value_kernel,
    input_matrix_kernel,
    output_matrix_kernel,
    mixer_norm_scale,
    mixer_output_weight,
    second_token_rows,
    expert_norm_scale,
    routed_expert_index,
    routed_expert_weight,
    routed_gate_weight,
    routed_up_weight,
    routed_down_weight,
    shared_gate_weight,
    shared_up_weight,
    shared_down_weight,
):
    length = mixer_value_input.shape[0]
    heads_local = step_input.shape[1]
    width_x = mixer_value_input.shape[1]
    width_b = input_state_matrix.shape[1]
    groups_local = width_b // STATE
    head_ratio = heads_local // groups_local
    nblocks = length // BLOCK
    lead_row = length - CONV_TAPS + 1
    edge_rows = jnp.concatenate(
        [
            mixer_value_input[lead_row:],
            input_state_matrix[lead_row:],
            output_state_matrix[lead_row:],
        ],
        axis=1,
    )
    tail_rows = passed_along(edge_rows, "ep", 1)
    rows_local = second_token_rows.shape[0]
    model_width = second_token_rows.shape[1]
    local_experts = routed_gate_weight.shape[0]
    ep_count = lax.axis_size("ep")
    experts = local_experts * ep_count
    capacity = max(2, 3 * rows_local * TOP_K // (2 * experts))
    col_width = model_width // lax.axis_size("tp")
    rows_wide = second_token_rows.astype(jnp.float32)
    normed = (
        rows_wide
        * lax.rsqrt(jnp.mean(rows_wide * rows_wide, axis=-1, keepdims=True) + epsilon)
        * expert_norm_scale
    ).astype(jnp.bfloat16)
    ids = routed_expert_index.T.astype(jnp.float32)
    id_rows = -(-ids.size // col_width)
    id_block = jnp.pad(
        ids.astype(jnp.bfloat16).reshape(-1), (0, id_rows * col_width - ids.size)
    ).reshape(id_rows, col_width)
    id_block = jnp.pad(id_block, ((0, -id_rows % 8), (0, 0)))
    my_columns = lax.dynamic_slice_in_dim(normed, lax.axis_index("tp") * col_width, col_width, 1)
    outgoing, value_rows, in_rows, out_rows = lax.optimization_barrier(
        (
            jnp.concatenate([my_columns, id_block], axis=0),
            mixer_value_input,
            input_state_matrix,
            output_state_matrix,
        )
    )
    everyone = lax.all_gather(outgoing, "ep", axis=0)
    values = conv_silu(tail_rows[:, :width_x], value_rows, value_kernel)
    in_mat = conv_silu(
        tail_rows[:, width_x : width_x + width_b], in_rows, input_matrix_kernel
    )
    out_mat = conv_silu(
        tail_rows[:, width_x + width_b :], out_rows, output_matrix_kernel
    )
    step_length = jax.nn.softplus(step_input)
    decay_logarithm = -jnp.exp(head_log_decay)[None, :] * step_length + extra_log_decay
    running = jnp.cumsum(decay_logarithm.reshape(nblocks, BLOCK, heads_local), axis=1)
    value_wide = values.astype(jnp.float32).reshape(nblocks, BLOCK, heads_local, HEAD_DIM)
    scaled = value_wide * step_length.reshape(nblocks, BLOCK, heads_local)[..., None]
    in_blocks = in_mat.reshape(nblocks, BLOCK, groups_local, STATE)
    out_blocks = out_mat.reshape(nblocks, BLOCK, groups_local, STATE)
    scores = jnp.einsum(
        "bign,bjgn->bgij", out_blocks, in_blocks, preferred_element_type=jnp.float32
    )
    scores = jnp.repeat(scores, head_ratio, axis=1)
    spread = jnp.transpose(running[:, :, None, :] - running[:, None, :, :], (0, 3, 1, 2))
    lower_mask = jnp.tril(jnp.ones((BLOCK, BLOCK), bool))[None, None]
    decay_mat = jnp.where(lower_mask, jnp.exp(jnp.where(lower_mask, spread, 0.0)), 0.0)
    inside = jnp.einsum("bhij,bjhp->bihp", scores * decay_mat, scaled, precision=precise)
    out_head = jnp.repeat(out_blocks.astype(jnp.float32), head_ratio, axis=2)
    in_head = jnp.repeat(in_blocks.astype(jnp.float32), head_ratio, axis=2)
    block_logs = running[:, -1]
    to_end = jnp.exp(block_logs[:, None, :] - running)
    block_state = jnp.einsum("bjhn,bjh,bjhp->bhpn", in_head, to_end, scaled, precision=precise)
    start_state = jnp.zeros((heads_local, HEAD_DIM, STATE), jnp.float32)
    local_total, local_prev = lax.scan(
        carry_blocks, start_state, (jnp.exp(block_logs), block_state)
    )
    before_logs = jnp.cumsum(block_logs, axis=0) - block_logs
    everyone, local_total = lax.optimization_barrier((everyone, local_total))
    incoming = carried_in(jnp.sum(block_logs, axis=0), local_total, "ep")
    their_rows = everyone[:, :rows_local]
    their_ids = everyone[:, rows_local : rows_local + id_rows].reshape(ep_count, -1)
    their_ids = their_ids[:, : ids.size].reshape(ep_count, TOP_K, rows_local).astype(jnp.float32)
    mine = (lax.axis_index("ep") * local_experts + jnp.arange(local_experts)).astype(jnp.float32)
    named = jnp.any(their_ids[:, None] == mine[None, :, None, None], axis=2)
    seat = jnp.where(named, earlier_counts(named, rows_local), -1.0)
    seats = jnp.arange(capacity, dtype=jnp.float32)
    pick = (seat[:, :, None, :] == seats[None, None, :, None]).astype(jnp.bfloat16)
    arrived = jnp.stack(
        [
            jnp.einsum(
                "bsr,brd->bsd", pick[:, j], their_rows, preferred_element_type=jnp.float32
            )
            .astype(jnp.bfloat16)
            .reshape(ep_count * capacity, col_width)
            for j in range(local_experts)
        ]
    )
    column_piece = lax.all_gather(arrived, "tp", axis=2, tiled=True)
    column_piece, incoming = lax.optimization_barrier((column_piece, incoming))
    entering = local_prev + jnp.exp(before_logs)[:, :, None, None] * incoming[None]
    carried_term = (
        jnp.einsum("bihn,bhpn->bihp", out_head, entering, precision=precise)
        * jnp.exp(running)[..., None]
    )
    mixed_heads = (inside + carried_term).reshape(length, heads_local, HEAD_DIM)
    mixed_heads = mixed_heads + head_skip_scale[None, :, None] * value_wide.reshape(
        length, heads_local, HEAD_DIM
    )
    gated_heads = mixed_heads * jax.nn.silu(output_gate_input.astype(jnp.float32)).reshape(
        length, heads_local, HEAD_DIM
    )
    grouped = gated_heads.reshape(length, groups_local, head_ratio * HEAD_DIM)
    grouped = grouped * lax.rsqrt(jnp.mean(grouped * grouped, axis=-1, keepdims=True) + epsilon)
    mixer_normed = (grouped.reshape(length, width_x) * mixer_norm_scale).astype(jnp.bfloat16)
    gate_pre = jnp.einsum(
        "esd,edf->esf", column_piece, routed_gate_weight, preferred_element_type=jnp.float32
    )
    up_pre = jnp.einsum(
        "esd,edf->esf", column_piece, routed_up_weight, preferred_element_type=jnp.float32
    )
    hidden = (jax.nn.silu(gate_pre) * up_pre).astype(jnp.bfloat16)
    shared_hidden = (
        jax.nn.silu(jnp.dot(normed, shared_gate_weight, preferred_element_type=jnp.float32))
        * jnp.dot(normed, shared_up_weight, preferred_element_type=jnp.float32)
    ).astype(jnp.bfloat16)
    whole_hidden = lax.all_gather(hidden, "tp", axis=2, tiled=True)
    both = lax.all_gather(
        jnp.concatenate([mixer_normed, shared_hidden], axis=1), "tp", axis=1, tiled=True
    ).reshape(length, lax.axis_size("tp"), -1)
    whole_mix = both[:, :, :width_x].reshape(length, -1)
    whole_shared = both[:, :, width_x:].reshape(length, -1)
    mixer_output = jnp.dot(
        whole_mix, mixer_output_weight, preferred_element_type=jnp.float32
    ).astype(jnp.bfloat16)
    expert_result = jnp.einsum(
        "esf,efd->esd", whole_hidden, routed_down_weight, preferred_element_type=jnp.float32
    ).astype(jnp.bfloat16)
    going = jnp.concatenate(
        [expert_result[j].reshape(ep_count, capacity, col_width) for j in range(local_experts)],
        axis=1,
    )
    returned = lax.all_to_all(going, "ep", split_axis=0, concat_axis=0, tiled=True)
    returned = returned.reshape(experts * capacity, col_width)
    kinds = jnp.arange(experts, dtype=jnp.float32)
    chosen = ids[:, None, :] == kinds[None, :, None]
    count = earlier_counts(jnp.any(chosen, axis=0), rows_local)
    position = jnp.sum(jnp.where(chosen, count[None], 0.0), axis=1)
    slot = (ids * capacity + position).T.astype(jnp.int32)
    columns = jnp.arange(experts * capacity, dtype=jnp.int32)[None, :]
    spread = jnp.zeros((rows_local, experts * capacity), jnp.float32)
    for k in range(TOP_K):
        spread = spread + jnp.where(
            slot[:, k : k + 1] == columns, routed_expert_weight[:, k : k + 1], 0.0
        )
    high = lax.reduce_precision(spread, 8, 7)
    low = (spread - high).astype(jnp.bfloat16)
    routed_sum = jnp.dot(
        high.astype(jnp.bfloat16), returned, preferred_element_type=jnp.float32
    ) + jnp.dot(low, returned, preferred_element_type=jnp.float32)
    shared_result = jnp.dot(whole_shared, shared_down_weight, preferred_element_type=jnp.float32)
    routed_out = (routed_sum + shared_result).astype(jnp.bfloat16)
    return (mixer_output, routed_out)


MESH = pl.DeviceIdType.MESH
HALO = 16
LANES = 128


def silu(v):
    return v / (1.0 + jnp.exp(-v))


def dot(a, b, contract=((1,), (0,)), exact=False):
    return lax.dot_general(
        a,
        b,
        (contract, ((), ())),
        precision=precise if exact else None,
        preferred_element_type=jnp.float32,
    )


def iota(shape, axis):
    return lax.broadcasted_iota(jnp.int32, shape, axis)


def at(start, size):
    return pl.ds(pl.multiple_of(start, size), size)


def body(dims, names, *refs):
    r = types.SimpleNamespace(**dict(zip(names, refs)))
    n_ep, rows, cap, ratio = dims.n_ep, dims.rows, dims.cap, dims.ratio
    nz = n_ep // 2
    half = rows // 2
    tp = dims.tp
    quarter = dims.quarter
    heads, groups, width = dims.heads, dims.groups, dims.width
    band = ratio * HEAD_DIM
    ff, sff = dims.ff, dims.sff
    f32, bf16 = jnp.float32, jnp.bfloat16

    e, t = lax.axis_index("ep"), lax.axis_index("tp")
    z, c = lax.div(e, 2), lax.rem(e, 2)
    other = 1 - c
    partner = e + 1 - 2 * c
    tx = t + 1 - 2 * lax.rem(t, 2)
    ty = lax.rem(t + 2, tp)
    td = tp - 1 - t

    def remote(src, dst, send, recv, to):
        return pltpu.make_async_remote_copy(
            src_ref=src, dst_ref=dst, send_sem=send, recv_sem=recv, device_id=to, device_id_type=MESH
        )

    fetched = dims.fetched

    def fetch(name):
        return pltpu.make_async_copy(
            getattr(r, name), getattr(r, "v_" + name), r.local_sem.at[fetched.index(name)]
        )

    for name in fetched:
        fetch(name).start()

    def got(*wanted):
        for name in wanted:
            fetch(name).wait()

    barrier = pltpu.get_barrier_semaphore()
    for by in range(1, n_ep):
        pl.semaphore_signal(barrier, inc=1, device_id=(lax.rem(e + by, n_ep), t), device_id_type=MESH)
    for to in (tx, ty):
        pl.semaphore_signal(barrier, inc=1, device_id=(e, to), device_id_type=MESH)

    def zsource(k):
        return lax.rem(z + k, nz)

    def plane(buf, send, recv):
        def leg(q, piece, slot, to):
            return remote(buf(q, piece), buf(q, piece), send(slot), recv(slot), (e, to))

        def start():
            leg(t, 0, 0, tx).start()
            leg(t, 1, 3, ty).start()
            leg(t, 1, 1, tx).start()
            leg(t, 0, 2, ty).start()

        def relay():
            leg(tx, 0, 0, tx).wait_recv()
            leg(tx, 0, 4, ty).start()
            leg(ty, 1, 3, ty).wait_recv()
            leg(ty, 1, 5, tx).start()

        def finish():
            leg(tx, 1, 1, tx).wait_recv()
            leg(ty, 0, 2, ty).wait_recv()
            leg(td, 0, 4, ty).wait_recv()
            leg(td, 1, 5, tx).wait_recv()

        def drain():
            leg(t, 0, 0, tx).wait_send()
            leg(t, 1, 1, tx).wait_send()
            leg(t, 0, 2, ty).wait_send()
            leg(t, 1, 3, ty).wait_send()
            leg(tx, 0, 4, ty).wait_send()
            leg(ty, 1, 5, tx).wait_send()

        return types.SimpleNamespace(start=start, relay=relay, finish=finish, drain=drain)

    def tokens(k):
        block = 2 * zsource(k) + c
        return plane(
            lambda q, piece: r.tok.at[block, q, pl.ds(piece * half, half)],
            lambda slot: r.tok_send.at[k, slot],
            lambda slot: r.tok_recv.at[k, slot],
        )

    def hiddens(k):
        return plane(
            lambda q, piece: r.hid.at[k, q, pl.ds(piece * 2 * cap, 2 * cap)],
            lambda slot: r.hid_send.at[k, slot],
            lambda slot: r.hid_recv.at[k, slot],
        )

    mixes = plane(
        lambda q, piece: r.mix.at[q, pl.ds(piece * half, half)],
        lambda slot: r.mix_send.at[slot],
        lambda slot: r.mix_recv.at[slot],
    )

    def across(k, q, whose):
        ref = r.tok.at[2 * zsource(k) + whose, q]
        return remote(ref, ref, r.pair_send.at[k, q], r.pair_recv.at[k, q], (partner, t))

    def along(k):
        to = 2 * lax.rem(z + nz - k, nz) + c
        ref = r.tok.at[e, t]
        return remote(ref, ref, r.z_send.at[k], r.z_recv.at[k], (to, t))

    def along_in(k):
        ref = r.tok.at[2 * zsource(k) + c, t]
        return remote(ref, ref, r.z_send.at[k], r.z_recv.at[k], (e, t))

    def route_to(by):
        ref = r.route.at[e]
        return remote(ref, ref, r.route_send.at[by], r.route_recv.at[e], (lax.rem(e + by, n_ep), t))

    def route_from(source):
        ref = r.route.at[source]
        return remote(ref, ref, r.route_send.at[0], r.route_recv.at[source], (e, t))

    edges = ((r.v_x, r.halo_x), (r.v_b, r.halo_b), (r.v_c, r.halo_c))

    def halo(i):
        src, dst = edges[i]
        return remote(
            src.at[pl.ds(rows - HALO, HALO)], dst, r.halo_send.at[i], r.halo_recv.at[i], (lax.rem(e + 1, n_ep), t)
        )

    got("rows", "scale")
    step_rows = 16

    def norm_rows(i, _):
        part = r.v_rows[at(i * step_rows, step_rows), :].astype(f32)
        by = lax.rsqrt(jnp.mean(part * part, axis=-1, keepdims=True) + epsilon)
        part = (part * by * r.v_scale[...]).astype(bf16)
        for q in range(tp):
            r.tok[e, q, at(i * step_rows, step_rows), :] = part[:, q * quarter : (q + 1) * quarter]
        return 0

    lax.fori_loop(0, rows // step_rows, norm_rows, 0)
    got("ids", "wts")
    below = iota((rows, rows), 0)
    right = iota((rows, rows), 1)
    eye = (below == right).astype(f32)
    r.earlier[...] = (below < right).astype(bf16)
    r.route[e, 0:TOP_K, :] = dot(r.v_ids[...].astype(f32), eye, ((0,), (0,)), exact=True)
    r.route[e, TOP_K : 2 * TOP_K, :] = dot(r.v_wts[...], eye, ((0,), (0,)), exact=True)
    got("x", "b", "c")
    pl.semaphore_wait(barrier, n_ep - 1 + 2)

    @pl.when(e + 1 < n_ep)
    def _():
        for i in range(3):
            halo(i).start()

    for by in range(1, n_ep):
        route_to(by).start()
    for k in range(1, nz):
        along(k).start()
    for q in range(tp):
        across(0, q, c).start()

    @pl.when(e > 0)
    def _():
        for i in range(3):
            halo(i).wait_recv()

    @pl.when(e == 0)
    def _():
        for _, dst in edges:
            dst[...] = jnp.zeros_like(dst)

    got("vk", "bk", "ck", "step", "extra", "hld")

    def conv(src, edge, taps, out):
        def chunk(i, _):
            lanes = at(i * LANES, LANES)
            r.padded[0:8, :] = edge[:, lanes].astype(f32)[HALO - 8 :]
            r.padded[8 : 8 + rows, :] = src[:, lanes].astype(f32)
            total = jnp.zeros((rows, LANES), f32)
            for k in range(CONV_TAPS):
                lead = 8 - CONV_TAPS + 1 + k
                total = total + r.padded[lead : lead + rows, :] * taps[k : k + 1, lanes]
            out[:, lanes] = silu(total).astype(bf16)
            return 0

        lax.fori_loop(0, src.shape[1] // LANES, chunk, 0)

    conv(r.v_x, r.halo_x, r.v_vk, r.vals)
    conv(r.v_b, r.halo_b, r.v_bk, r.inm)
    conv(r.v_c, r.halo_c, r.v_ck, r.outm)
    pre = r.v_step[...]
    steps = jnp.maximum(pre, 0.0) + jnp.log(1.0 + jnp.exp(-jnp.abs(pre)))
    decay = -jnp.exp(r.v_hld[...]) * steps + r.v_extra[...]
    upto = (below <= right).astype(f32)
    cum = dot(upto, decay, ((0,), (0,)), exact=True)
    r.cum[...] = cum
    r.cum_t[...] = dot(decay, upto, ((0,), (0,)), exact=True)
    r.step_t[...] = dot(steps, eye, ((0,), (0,)), exact=True)
    spread_heads = (lax.div(iota((heads, width), 1), HEAD_DIM) == iota((heads, width), 0)).astype(f32)
    r.growth[...] = dot(jnp.exp(cum), spread_heads, exact=True)
    to_end = jnp.exp(cum[rows - 1 : rows, :] - cum) * steps
    r.to_end[...] = dot(to_end, spread_heads, exact=True)
    for g in range(groups):
        lanes = pl.ds(g * band, band)
        weighted = (r.vals[:, lanes].astype(f32) * r.to_end[:, lanes]).astype(bf16)
        r.state[:, lanes] = dot(r.inm[:, g * STATE : (g + 1) * STATE], weighted, ((0,), (0,)))
    r.state_out[...] = r.state[...].astype(bf16)
    r.decay_out[...] = jnp.broadcast_to(r.growth[rows - 1 : rows, :], (8, width))

    def swap(i):
        src, dst = ((r.state_out, r.state_in), (r.decay_out, r.decay_in))[i]
        return remote(src, dst, r.swap_send.at[i], r.swap_recv.at[i], (partner, t))

    for i in range(2):
        swap(i).start()
    side = width // 2
    mine_lanes = at(c * side, side)

    def chain(i, by):
        src, dst = ((r.chip_state, r.chain_state), (r.chip_decay, r.chain_decay))[i]
        to = 2 * lax.rem(z + by, nz) + c
        return remote(src, dst.at[z], r.chain_send.at[i, by], r.chain_recv.at[i, z], (to, t))

    def chain_in(i, source):
        src, dst = ((r.chip_state, r.chain_state), (r.chip_decay, r.chain_decay))[i]
        return remote(src, dst.at[source], r.chain_send.at[i, 0], r.chain_recv.at[i, source], (e, t))

    def send_chain():
        for i in range(2):
            swap(i).wait_recv()
        ours, theirs = r.state[:, mine_lanes], r.state_in[:, mine_lanes].astype(f32)
        our_decay, their_decay = r.decay_out[:, mine_lanes], r.decay_in[:, mine_lanes]
        first = jnp.where(c == 0, ours, theirs)
        second = jnp.where(c == 0, theirs, ours)
        late = jnp.where(c == 0, their_decay, our_decay)
        r.chip_state[...] = (late[0:1, :] * first + second).astype(bf16)
        r.chip_decay[...] = our_decay * their_decay
        for by in range(1, nz):

            @pl.when(z + by < nz)
            def _():
                for i in range(2):
                    chain(i, by).start()

    def inside():
        mid = rows // 2
        lane = iota((mid, 2 * HEAD_DIM), 1) < HEAD_DIM
        for g in range(groups):
            cols = slice(g * STATE, (g + 1) * STATE)
            for part in range(2):
                span = slice(part * mid, (part + 1) * mid)
                reach = (part + 1) * mid
                scores = dot(r.outm[span, cols], r.inm[0:reach, cols], ((1,), (1,)))
                mask = iota((mid, reach), 0) + part * mid >= iota((mid, reach), 1)
                for p in range(ratio // 2):
                    pair = []
                    head = g * ratio + 2 * p
                    lanes = slice(head * HEAD_DIM, (head + 2) * HEAD_DIM)
                    for h in (head, head + 1):
                        diff = r.cum[span, h : h + 1] - r.cum_t[h : h + 1, 0:reach]
                        grid = scores * jnp.exp(jnp.where(mask, diff, -1e30)) * r.step_t[h : h + 1, 0:reach]
                        pair.append(dot(grid.astype(bf16), r.vals[0:reach, lanes]))
                    r.near[span, lanes] = jnp.where(lane, pair[0], pair[1])

    def shared():
        got("sg", "su")
        gate, up = 0.0, 0.0
        for q in range(tp):
            part = r.tok[e, q]
            gate = gate + dot(part, r.v_sg[q * quarter : (q + 1) * quarter, :])
            up = up + dot(part, r.v_su[q * quarter : (q + 1) * quarter, :])
        r.mix[t, :, width : width + sff] = (silu(gate) * up).astype(bf16)

    def enter(k):
        source = zsource(k)
        seats = iota((cap, rows), 0).astype(f32)
        for c2 in range(2):
            block = 2 * source + c2
            ids = r.route[block, 0:TOP_K, :]
            weights = r.route[block, TOP_K : 2 * TOP_K, :]
            for j in range(2):
                hit = ids == (2 * e + j).astype(f32)
                named = jnp.sum(jnp.where(hit, 1.0, 0.0), axis=0, keepdims=True)
                given = jnp.sum(jnp.where(hit, weights, 0.0), axis=0, keepdims=True)
                count = dot(jnp.broadcast_to(named, (16, rows)).astype(bf16), r.earlier[...])
                seat = jnp.where(named > 0.0, count[0:1, :], -1.0)
                taken = seats == seat
                r.pick[k, c2, j * cap : (j + 1) * cap, :] = jnp.where(taken, 1.0, 0.0).astype(bf16)
                amount = jnp.sum(jnp.where(taken, given, 0.0), axis=1, keepdims=True)
                r.amount[k, j, c2 * cap : (c2 + 1) * cap, :] = jnp.broadcast_to(amount, (cap, LANES))
            for q in range(tp):
                chosen = dot(r.pick[k, c2], r.tok[block, q]).astype(bf16)
                for j in range(2):
                    r.arrived[j, c2 * cap : (c2 + 1) * cap, q * quarter : (q + 1) * quarter] = chosen[
                        j * cap : (j + 1) * cap, :
                    ]
        for j in range(2):
            gate = dot(r.arrived[j], r.v_wg[j])
            up = dot(r.arrived[j], r.v_wu[j])
            r.hid[k, t, j * 2 * cap : (j + 1) * 2 * cap, :] = (silu(gate) * up).astype(bf16)

    def stage(k, _):
        @pl.when(k > 0)
        def _():
            tokens(k).relay()

        @pl.when(k + 1 < nz)
        def _():
            along_in(k + 1).wait_recv()
            tokens(k + 1).start()
            across(k + 1, t, c).start()

        @pl.when(k == 0)
        def _():
            send_chain()
            route_from(partner).wait_recv()
            got("wg", "wu")

        @pl.when(k == 1)
        def _():
            inside()

        @pl.when(k == 2)
        def _():
            shared()

        @pl.when(k > 0)
        def _():
            tokens(k).finish()
            for q in (tx, ty, td):
                across(k, q, c).start()
            for c2 in range(2):
                route_from(2 * zsource(k) + c2).wait_recv()

        @pl.when(k > 1)
        def _():
            hiddens(k - 2).relay()

        for q in range(tp):
            across(k, q, other).wait_recv()
        enter(k)
        hiddens(k).start()
        return 0

    lax.fori_loop(0, nz, stage, 0)
    hiddens(nz - 2).relay()

    r.before[...] = jnp.zeros_like(r.before)

    def add_chain(source, _):
        @pl.when(source < z)
        def _():
            for i in range(2):
                chain_in(i, source).wait_recv()
            r.before[...] = r.chain_decay[source, 0:1, :] * r.before[...] + r.chain_state[source].astype(f32)

        return 0

    lax.fori_loop(0, nz, add_chain, 0)
    r.incoming[c] = r.before[...].astype(bf16)

    def halves(whose):
        ref = r.incoming.at[whose]
        return remote(ref, ref, r.half_sem.at[0], r.half_sem.at[1], (partner, t))

    halves(c).start()
    hiddens(nz - 1).relay()
    got("wd", "gate", "skip", "mscale")

    def back_pair(k):
        return remote(r.yours.at[k], r.theirs.at[k], r.pair_y_send.at[k], r.pair_y_recv.at[k], (partner, t))

    def back(k):
        return remote(
            r.going.at[k], r.coming.at[k], r.y_send.at[k], r.y_recv.at[k], (2 * zsource(k) + c, t)
        )

    def leave(k):
        hiddens(k).finish()
        for j in range(2):
            total = 0.0
            for q in range(tp):
                total = total + dot(
                    r.hid[k, q, j * 2 * cap : (j + 1) * 2 * cap, :], r.v_wd[j, q * ff : (q + 1) * ff, :]
                )
            total = (total * r.amount[k, j, :, 0:1]).astype(bf16)
            for c2 in range(2):
                r.result[c2, j * cap : (j + 1) * cap, :] = total[c2 * cap : (c2 + 1) * cap, :]
        r.yours[k] = dot(r.pick[k, other], r.result[other], ((0,), (0,))).astype(bf16)
        back_pair(k).start()
        r.ours[k] = dot(r.pick[k, c], r.result[c], ((0,), (0,)))

    def send_back(k):
        back_pair(k).wait_recv()
        r.going[k] = (r.ours[k] + r.theirs[k].astype(f32)).astype(bf16)
        back(k).start()

    def mixer_end():
        halves(other).wait_recv()
        spread_heads = (lax.div(iota((heads, width), 1), HEAD_DIM) == iota((heads, width), 0)).astype(f32)
        skip = dot(jnp.broadcast_to(r.v_skip[...], (8, heads)), spread_heads, exact=True)[0:1, :]
        for s in range(2):
            lanes = slice(s * side, (s + 1) * side)
            hold = r.incoming[s].astype(f32)
            later = r.decay_in[0:1, lanes] * hold + r.state_in[:, lanes].astype(f32)
            r.entering[:, lanes] = jnp.where(c == 0, hold, later).astype(bf16)
        for g in range(groups):
            lanes = slice(g * band, (g + 1) * band)
            far = dot(r.outm[:, g * STATE : (g + 1) * STATE], r.entering[:, lanes]) * r.growth[:, lanes]
            mixed = r.near[:, lanes] + far + skip[:, lanes] * r.vals[:, lanes].astype(f32)
            gated = mixed * silu(r.v_gate[:, lanes].astype(f32))
            by = lax.rsqrt(jnp.mean(gated * gated, axis=-1, keepdims=True) + epsilon)
            r.mix[t, :, lanes] = (gated * by * r.v_mscale[:, lanes]).astype(bf16)

    def leaving(i, _):
        k = lax.rem(i + 1, nz)
        leave(k)

        @pl.when(i == 0)
        def _():
            mixer_end()
            mixes.start()

        @pl.when(i > 0)
        def _():
            send_back(i)

        return 0

    lax.fori_loop(0, nz, leaving, 0)
    mixes.relay()
    got("sd", "wm")

    back_pair(0).wait_recv()
    routed = r.ours[0] + r.theirs[0].astype(f32)
    r.routed_sum[...] = routed + dot(r.mix[t, :, width : width + sff], r.v_sd[at(t * sff, sff), :])
    r.mixer_sum[...] = dot(r.mix[t, :, 0:width], r.v_wm[at(t * width, width), :])
    mixes.finish()
    for q in (tx, ty, td):
        r.routed_sum[...] += dot(r.mix[q, :, width : width + sff], r.v_sd[at(q * sff, sff), :])
        r.mixer_sum[...] += dot(r.mix[q, :, 0:width], r.v_wm[at(q * width, width), :])
    r.mixer_out[...] = r.mixer_sum[...].astype(bf16)
    total = r.routed_sum[...]
    for k in range(1, nz):
        back(k).wait_recv()
        total = total + r.coming[k].astype(f32)
    r.routed_out[...] = total.astype(bf16)

    @pl.when(e + 1 < n_ep)
    def _():
        for i in range(3):
            halo(i).wait_send()

    for by in range(1, n_ep):
        route_to(by).wait_send()
    for i in range(2):
        swap(i).wait_send()
    for by in range(1, nz):

        @pl.when(z + by < nz)
        def _():
            for i in range(2):
                chain(i, by).wait_send()

    halves(c).wait_send()
    mixes.drain()

    def drain(k, _):
        @pl.when(k > 0)
        def _():
            along(k).wait_send()
            tokens(k).drain()
            back(k).wait_send()

        for q in range(tp):
            across(k, q, c).wait_send()
        hiddens(k).drain()
        back_pair(k).wait_send()
        return 0

    lax.fori_loop(0, nz, drain, 0)


def fused_on_device(*given):
    argument = dict(zip(ARGUMENTS, given))
    rows, model_width = argument["rows"].shape
    n_ep, tp = lax.axis_size("ep"), lax.axis_size("tp")
    nz = n_ep // 2
    heads = argument["step"].shape[1]
    width = argument["x"].shape[1]
    state_width = argument["b"].shape[1]
    groups = state_width // STATE
    local_experts, _, ff = argument["wg"].shape
    sff = argument["sg"].shape[1]
    quarter = argument["wd"].shape[2]
    cap = max(2, 3 * rows * TOP_K // (2 * local_experts * n_ep))
    for name in ("hld", "skip", "mscale", "scale"):
        argument[name] = argument[name].reshape(1, -1)
    dims = types.SimpleNamespace(
        n_ep=n_ep, tp=tp, rows=rows, cap=cap, ratio=heads // groups, quarter=quarter, heads=heads,
        groups=groups, width=width, ff=ff, sff=sff,
        fetched=FETCHED,
    )
    f32, bf16 = jnp.float32, jnp.bfloat16
    scratch = dict(("v_" + n, pltpu.VMEM(argument[n].shape, argument[n].dtype)) for n in FETCHED)
    vmem = dict(
        tok=((n_ep, tp, rows, quarter), bf16),
        hid=((nz, tp, 4 * cap, ff), bf16),
        mix=((tp, rows, width + sff), bf16),
        route=((n_ep, 2 * TOP_K, rows), f32),
        halo_x=((HALO, width), bf16),
        halo_b=((HALO, state_width), bf16),
        halo_c=((HALO, state_width), bf16),
        padded=((8 + rows, LANES), f32),
        vals=((rows, width), bf16),
        inm=((rows, state_width), bf16),
        outm=((rows, state_width), bf16),
        cum=((rows, heads), f32),
        cum_t=((heads, rows), f32),
        step_t=((heads, rows), f32),
        growth=((rows, width), f32),
        to_end=((rows, width), f32),
        state=((STATE, width), f32),
        state_out=((STATE, width), bf16),
        state_in=((STATE, width), bf16),
        decay_out=((8, width), f32),
        decay_in=((8, width), f32),
        chip_state=((STATE, width // 2), bf16),
        chip_decay=((8, width // 2), f32),
        chain_state=((nz, STATE, width // 2), bf16),
        chain_decay=((nz, 8, width // 2), f32),
        before=((STATE, width // 2), f32),
        incoming=((2, STATE, width // 2), bf16),
        entering=((STATE, width), bf16),
        near=((rows, width), f32),
        earlier=((rows, rows), bf16),
        pick=((nz, 2, 2 * cap, rows), bf16),
        amount=((nz, 2, 2 * cap, LANES), f32),
        arrived=((2, 2 * cap, model_width), bf16),
        result=((2, 2 * cap, quarter), bf16),
        yours=((nz, rows, quarter), bf16),
        theirs=((nz, rows, quarter), bf16),
        ours=((nz, rows, quarter), f32),
        going=((nz, rows, quarter), bf16),
        coming=((nz, rows, quarter), bf16),
        routed_sum=((rows, quarter), f32),
        mixer_sum=((rows, quarter), f32),
    )
    for name, (shape, dtype) in vmem.items():
        scratch[name] = pltpu.VMEM(shape, dtype)
    sems = dict(
        local_sem=(len(FETCHED),),
        tok_send=(nz, 6), tok_recv=(nz, 6), hid_send=(nz, 6), hid_recv=(nz, 6),
        mix_send=(6,), mix_recv=(6,), pair_send=(nz, tp), pair_recv=(nz, tp),
        z_send=(nz,), z_recv=(nz,), route_send=(n_ep,), route_recv=(n_ep,),
        halo_send=(3,), halo_recv=(3,), swap_send=(2,), swap_recv=(2,),
        chain_send=(2, nz), chain_recv=(2, nz), half_sem=(2,),
        pair_y_send=(nz,), pair_y_recv=(nz,), y_send=(nz,), y_recv=(nz,),
    )
    for name, shape in sems.items():
        scratch[name] = pltpu.SemaphoreType.DMA(shape)
    order = tuple(FETCHED)
    names = order + ("mixer_out", "routed_out") + tuple(scratch)
    out = jax.ShapeDtypeStruct((rows, quarter), bf16)
    return tuple(
        pl.pallas_call(
            functools.partial(body, dims, names),
            out_shape=(out, out),
            in_specs=[pl.BlockSpec(memory_space=pl.ANY)] * len(order),
            out_specs=(pl.BlockSpec(memory_space=pltpu.VMEM),) * 2,
            scratch_shapes=list(scratch.values()),
            compiler_params=pltpu.CompilerParams(
                collective_id=0, has_side_effects=True, vmem_limit_bytes=VMEM_LIMIT
            ),
            name="mixer_and_experts",
        )(*[argument[n] for n in order])
    )


VMEM_LIMIT = 60 * 1024 * 1024
ARGUMENTS = (
    "x", "b", "c", "gate", "step", "extra", "hld", "skip", "vk", "bk", "ck", "mscale", "wm",
    "rows", "scale", "ids", "wts", "wg", "wu", "wd", "sg", "su", "sd",
)
FETCHED = (
    "rows", "scale", "ids", "wts", "x", "b", "c", "vk", "bk", "ck", "step", "extra", "hld",
    "wg", "wu", "sg", "su", "gate", "skip", "mscale", "wd", "sd", "wm",
)


def choose(*given):
    argument = dict(zip(ARGUMENTS, given))
    n_ep, tp = lax.axis_size("ep"), lax.axis_size("tp")
    rows = argument["rows"].shape[0]
    experts = argument["wg"].shape[0]
    cap = max(2, 3 * rows * TOP_K // (2 * experts * n_ep))
    wide = all(argument[n].shape[-1] % LANES == 0 for n in ("x", "b", "wg", "wd", "sg"))
    fits = tp == 4 and n_ep % 2 == 0 and n_ep >= 6 and experts == 2
    fits = fits and wide and cap % 16 == 0 and rows % 32 == 0
    return fused_on_device(*given) if fits else on_device(*given)


def solution(mesh):
    return jax.shard_map(
        choose,
        mesh=mesh,
        in_specs=(
            P("ep", "tp"),
            P("ep", "tp"),
            P("ep", "tp"),
            P("ep", "tp"),
            P("ep", "tp"),
            P("ep", "tp"),
            P("tp"),
            P("tp"),
            P(None, "tp"),
            P(None, "tp"),
            P(None, "tp"),
            P("tp"),
            P(None, "tp"),
            P("ep", None),
            P(),
            P("ep", None),
            P("ep", None),
            P("ep", None, "tp"),
            P("ep", None, "tp"),
            P("ep", None, "tp"),
            P(None, "tp"),
            P(None, "tp"),
            P(None, "tp"),
        ),
        out_specs=(P("ep", "tp"), P("ep", "tp")),
        check_vma=False,
    )
```

```python
import functools
import types

import jax
import jax.numpy as jnp
from jax import lax
from jax.experimental import pallas as pl
from jax.experimental.pallas import tpu as pltpu
from jax.sharding import PartitionSpec as P

HEAD_DIM = 64
STATE = 128
CONV_TAPS = 4
BLOCK = 128
TOP_K = 4


epsilon = 1e-05
precise = lax.Precision.HIGHEST


def passed_along(x, axis, by):
    size = lax.axis_size(axis)
    pairs = [(i, i + by) for i in range(size) if 0 <= i + by < size]
    return lax.ppermute(x, axis, pairs)


def carried_in(total_log, state, axis):
    size = lax.axis_size(axis)
    place = lax.axis_index(axis)
    log = passed_along(total_log, axis, 1)
    hold = passed_along(state.astype(jnp.bfloat16), axis, 1).astype(jnp.float32)
    by = 1
    while by < size - 1:
        before = passed_along(hold.astype(jnp.bfloat16), axis, by).astype(jnp.float32)
        hold = hold + jnp.exp(log)[:, None, None] * before
        log = log + passed_along(log, axis, by)
        by *= 2
    return hold


def conv_silu(tail_rows, source, weights):
    length = source.shape[0]
    padded = jnp.concatenate([tail_rows, source], axis=0)
    total_sum = jnp.zeros(source.shape, jnp.float32)
    for tap_index in range(CONV_TAPS):
        total_sum = (
            total_sum
            + padded[tap_index : tap_index + length].astype(jnp.float32) * weights[tap_index]
        )
    return jax.nn.silu(total_sum).astype(jnp.bfloat16)


def carry_blocks(carried, inputs):
    block_decay, block_state = inputs
    return (carried * block_decay[:, None, None] + block_state, carried)


def earlier_counts(mask, rows):
    at = jnp.arange(rows)
    tri = (at[:, None] < at[None, :]).astype(jnp.bfloat16)
    return lax.dot_general(
        mask.astype(jnp.bfloat16),
        tri,
        (((mask.ndim - 1,), (0,)), ((), ())),
        preferred_element_type=jnp.float32,
    )


def on_device(
    mixer_value_input,
    input_state_matrix,
    output_state_matrix,
    output_gate_input,
    step_input,
    extra_log_decay,
    head_log_decay,
    head_skip_scale,
    value_kernel,
    input_matrix_kernel,
    output_matrix_kernel,
    mixer_norm_scale,
    mixer_output_weight,
    second_token_rows,
    expert_norm_scale,
    routed_expert_index,
    routed_expert_weight,
    routed_gate_weight,
    routed_up_weight,
    routed_down_weight,
    shared_gate_weight,
    shared_up_weight,
    shared_down_weight,
):
    length = mixer_value_input.shape[0]
    heads_local = step_input.shape[1]
    width_x = mixer_value_input.shape[1]
    width_b = input_state_matrix.shape[1]
    groups_local = width_b // STATE
    head_ratio = heads_local // groups_local
    nblocks = length // BLOCK
    lead_row = length - CONV_TAPS + 1
    edge_rows = jnp.concatenate(
        [
            mixer_value_input[lead_row:],
            input_state_matrix[lead_row:],
            output_state_matrix[lead_row:],
        ],
        axis=1,
    )
    tail_rows = passed_along(edge_rows, "ep", 1)
    rows_local = second_token_rows.shape[0]
    model_width = second_token_rows.shape[1]
    local_experts = routed_gate_weight.shape[0]
    ep_count = lax.axis_size("ep")
    experts = local_experts * ep_count
    capacity = max(2, 3 * rows_local * TOP_K // (2 * experts))
    col_width = model_width // lax.axis_size("tp")
    rows_wide = second_token_rows.astype(jnp.float32)
    normed = (
        rows_wide
        * lax.rsqrt(jnp.mean(rows_wide * rows_wide, axis=-1, keepdims=True) + epsilon)
        * expert_norm_scale
    ).astype(jnp.bfloat16)
    ids = routed_expert_index.T.astype(jnp.float32)
    id_rows = -(-ids.size // col_width)
    id_block = jnp.pad(
        ids.astype(jnp.bfloat16).reshape(-1), (0, id_rows * col_width - ids.size)
    ).reshape(id_rows, col_width)
    id_block = jnp.pad(id_block, ((0, -id_rows % 8), (0, 0)))
    my_columns = lax.dynamic_slice_in_dim(normed, lax.axis_index("tp") * col_width, col_width, 1)
    outgoing, value_rows, in_rows, out_rows = lax.optimization_barrier(
        (
            jnp.concatenate([my_columns, id_block], axis=0),
            mixer_value_input,
            input_state_matrix,
            output_state_matrix,
        )
    )
    everyone = lax.all_gather(outgoing, "ep", axis=0)
    values = conv_silu(tail_rows[:, :width_x], value_rows, value_kernel)
    in_mat = conv_silu(
        tail_rows[:, width_x : width_x + width_b], in_rows, input_matrix_kernel
    )
    out_mat = conv_silu(
        tail_rows[:, width_x + width_b :], out_rows, output_matrix_kernel
    )
    step_length = jax.nn.softplus(step_input)
    decay_logarithm = -jnp.exp(head_log_decay)[None, :] * step_length + extra_log_decay
    running = jnp.cumsum(decay_logarithm.reshape(nblocks, BLOCK, heads_local), axis=1)
    value_wide = values.astype(jnp.float32).reshape(nblocks, BLOCK, heads_local, HEAD_DIM)
    scaled = value_wide * step_length.reshape(nblocks, BLOCK, heads_local)[..., None]
    in_blocks = in_mat.reshape(nblocks, BLOCK, groups_local, STATE)
    out_blocks = out_mat.reshape(nblocks, BLOCK, groups_local, STATE)
    scores = jnp.einsum(
        "bign,bjgn->bgij", out_blocks, in_blocks, preferred_element_type=jnp.float32
    )
    scores = jnp.repeat(scores, head_ratio, axis=1)
    spread = jnp.transpose(running[:, :, None, :] - running[:, None, :, :], (0, 3, 1, 2))
    lower_mask = jnp.tril(jnp.ones((BLOCK, BLOCK), bool))[None, None]
    decay_mat = jnp.where(lower_mask, jnp.exp(jnp.where(lower_mask, spread, 0.0)), 0.0)
    inside = jnp.einsum("bhij,bjhp->bihp", scores * decay_mat, scaled, precision=precise)
    out_head = jnp.repeat(out_blocks.astype(jnp.float32), head_ratio, axis=2)
    in_head = jnp.repeat(in_blocks.astype(jnp.float32), head_ratio, axis=2)
    block_logs = running[:, -1]
    to_end = jnp.exp(block_logs[:, None, :] - running)
    block_state = jnp.einsum("bjhn,bjh,bjhp->bhpn", in_head, to_end, scaled, precision=precise)
    start_state = jnp.zeros((heads_local, HEAD_DIM, STATE), jnp.float32)
    local_total, local_prev = lax.scan(
        carry_blocks, start_state, (jnp.exp(block_logs), block_state)
    )
    before_logs = jnp.cumsum(block_logs, axis=0) - block_logs
    everyone, local_total = lax.optimization_barrier((everyone, local_total))
    incoming = carried_in(jnp.sum(block_logs, axis=0), local_total, "ep")
    their_rows = everyone[:, :rows_local]
    their_ids = everyone[:, rows_local : rows_local + id_rows].reshape(ep_count, -1)
    their_ids = their_ids[:, : ids.size].reshape(ep_count, TOP_K, rows_local).astype(jnp.float32)
    mine = (lax.axis_index("ep") * local_experts + jnp.arange(local_experts)).astype(jnp.float32)
    named = jnp.any(their_ids[:, None] == mine[None, :, None, None], axis=2)
    seat = jnp.where(named, earlier_counts(named, rows_local), -1.0)
    seats = jnp.arange(capacity, dtype=jnp.float32)
    pick = (seat[:, :, None, :] == seats[None, None, :, None]).astype(jnp.bfloat16)
    arrived = jnp.stack(
        [
            jnp.einsum(
                "bsr,brd->bsd", pick[:, j], their_rows, preferred_element_type=jnp.float32
            )
            .astype(jnp.bfloat16)
            .reshape(ep_count * capacity, col_width)
            for j in range(local_experts)
        ]
    )
    column_piece = lax.all_gather(arrived, "tp", axis=2, tiled=True)
    column_piece, incoming = lax.optimization_barrier((column_piece, incoming))
    entering = local_prev + jnp.exp(before_logs)[:, :, None, None] * incoming[None]
    carried_term = (
        jnp.einsum("bihn,bhpn->bihp", out_head, entering, precision=precise)
        * jnp.exp(running)[..., None]
    )
    mixed_heads = (inside + carried_term).reshape(length, heads_local, HEAD_DIM)
    mixed_heads = mixed_heads + head_skip_scale[None, :, None] * value_wide.reshape(
        length, heads_local, HEAD_DIM
    )
    gated_heads = mixed_heads * jax.nn.silu(output_gate_input.astype(jnp.float32)).reshape(
        length, heads_local, HEAD_DIM
    )
    grouped = gated_heads.reshape(length, groups_local, head_ratio * HEAD_DIM)
    grouped = grouped * lax.rsqrt(jnp.mean(grouped * grouped, axis=-1, keepdims=True) + epsilon)
    mixer_normed = (grouped.reshape(length, width_x) * mixer_norm_scale).astype(jnp.bfloat16)
    gate_pre = jnp.einsum(
        "esd,edf->esf", column_piece, routed_gate_weight, preferred_element_type=jnp.float32
    )
    up_pre = jnp.einsum(
        "esd,edf->esf", column_piece, routed_up_weight, preferred_element_type=jnp.float32
    )
    hidden = (jax.nn.silu(gate_pre) * up_pre).astype(jnp.bfloat16)
    shared_hidden = (
        jax.nn.silu(jnp.dot(normed, shared_gate_weight, preferred_element_type=jnp.float32))
        * jnp.dot(normed, shared_up_weight, preferred_element_type=jnp.float32)
    ).astype(jnp.bfloat16)
    whole_hidden = lax.all_gather(hidden, "tp", axis=2, tiled=True)
    both = lax.all_gather(
        jnp.concatenate([mixer_normed, shared_hidden], axis=1), "tp", axis=1, tiled=True
    ).reshape(length, lax.axis_size("tp"), -1)
    whole_mix = both[:, :, :width_x].reshape(length, -1)
    whole_shared = both[:, :, width_x:].reshape(length, -1)
    mixer_output = jnp.dot(
        whole_mix, mixer_output_weight, preferred_element_type=jnp.float32
    ).astype(jnp.bfloat16)
    expert_result = jnp.einsum(
        "esf,efd->esd", whole_hidden, routed_down_weight, preferred_element_type=jnp.float32
    ).astype(jnp.bfloat16)
    going = jnp.concatenate(
        [expert_result[j].reshape(ep_count, capacity, col_width) for j in range(local_experts)],
        axis=1,
    )
    returned = lax.all_to_all(going, "ep", split_axis=0, concat_axis=0, tiled=True)
    returned = returned.reshape(experts * capacity, col_width)
    kinds = jnp.arange(experts, dtype=jnp.float32)
    chosen = ids[:, None, :] == kinds[None, :, None]
    count = earlier_counts(jnp.any(chosen, axis=0), rows_local)
    position = jnp.sum(jnp.where(chosen, count[None], 0.0), axis=1)
    slot = (ids * capacity + position).T.astype(jnp.int32)
    columns = jnp.arange(experts * capacity, dtype=jnp.int32)[None, :]
    spread = jnp.zeros((rows_local, experts * capacity), jnp.float32)
    for k in range(TOP_K):
        spread = spread + jnp.where(
            slot[:, k : k + 1] == columns, routed_expert_weight[:, k : k + 1], 0.0
        )
    high = lax.reduce_precision(spread, 8, 7)
    low = (spread - high).astype(jnp.bfloat16)
    routed_sum = jnp.dot(
        high.astype(jnp.bfloat16), returned, preferred_element_type=jnp.float32
    ) + jnp.dot(low, returned, preferred_element_type=jnp.float32)
    shared_result = jnp.dot(whole_shared, shared_down_weight, preferred_element_type=jnp.float32)
    routed_out = (routed_sum + shared_result).astype(jnp.bfloat16)
    return (mixer_output, routed_out)


MESH = pl.DeviceIdType.MESH
HALO = 16
LANES = 128


def silu(v):
    return v / (1.0 + jnp.exp(-v))


def dot(a, b, contract=((1,), (0,)), exact=False):
    return lax.dot_general(
        a,
        b,
        (contract, ((), ())),
        precision=precise if exact else None,
        preferred_element_type=jnp.float32,
    )


def iota(shape, axis):
    return lax.broadcasted_iota(jnp.int32, shape, axis)


def at(start, size):
    return pl.ds(pl.multiple_of(start, size), size)


def body(dims, names, *refs):
    r = types.SimpleNamespace(**dict(zip(names, refs)))
    n_ep, rows, cap, ratio = dims.n_ep, dims.rows, dims.cap, dims.ratio
    nz = n_ep // 2
    half = rows // 2
    tp = dims.tp
    quarter = dims.quarter
    heads, groups, width = dims.heads, dims.groups, dims.width
    band = ratio * HEAD_DIM
    ff, sff = dims.ff, dims.sff
    f32, bf16 = jnp.float32, jnp.bfloat16

    e, t = lax.axis_index("ep"), lax.axis_index("tp")
    z, c = lax.div(e, 2), lax.rem(e, 2)
    other = 1 - c
    partner = e + 1 - 2 * c
    tx = t + 1 - 2 * lax.rem(t, 2)
    ty = lax.rem(t + 2, tp)
    td = tp - 1 - t

    def remote(src, dst, send, recv, to):
        return pltpu.make_async_remote_copy(
            src_ref=src, dst_ref=dst, send_sem=send, recv_sem=recv, device_id=to, device_id_type=MESH
        )

    fetched = dims.fetched

    def fetch(name):
        return pltpu.make_async_copy(
            getattr(r, name), getattr(r, "v_" + name), r.local_sem.at[fetched.index(name)]
        )

    for name in fetched:
        fetch(name).start()

    def got(*wanted):
        for name in wanted:
            fetch(name).wait()

    barrier = pltpu.get_barrier_semaphore()
    for by in range(1, n_ep):
        pl.semaphore_signal(barrier, inc=1, device_id=(lax.rem(e + by, n_ep), t), device_id_type=MESH)
    for to in (tx, ty):
        pl.semaphore_signal(barrier, inc=1, device_id=(e, to), device_id_type=MESH)

    paired = jnp.minimum(z, nz - 1 - z)

    def zsource(k):
        inward = jnp.where(2 * z > nz - 1, -1, 1)
        alternate = z + inward * lax.div(k + 1, 2) * (2 * lax.rem(k, 2) - 1)
        rest = z + inward * (k - paired)
        return jnp.where(k <= 2 * paired, alternate, rest)

    def plane(buf, send, recv):
        def leg(q, piece, slot, to):
            return remote(buf(q, piece), buf(q, piece), send(slot), recv(slot), (e, to))

        def start():
            leg(t, 0, 0, tx).start()
            leg(t, 1, 3, ty).start()
            leg(t, 1, 1, tx).start()
            leg(t, 0, 2, ty).start()

        def relay():
            leg(tx, 0, 0, tx).wait_recv()
            leg(tx, 0, 4, ty).start()
            leg(ty, 1, 3, ty).wait_recv()
            leg(ty, 1, 5, tx).start()

        def rest():
            return leg(tx, 1, 1, tx), leg(ty, 0, 2, ty), leg(td, 0, 4, ty), leg(td, 1, 5, tx)

        def finish():
            for one in rest():
                one.wait_recv()

        def drain():
            leg(t, 0, 0, tx).wait_send()
            leg(t, 1, 1, tx).wait_send()
            leg(t, 0, 2, ty).wait_send()
            leg(t, 1, 3, ty).wait_send()
            leg(tx, 0, 4, ty).wait_send()
            leg(ty, 1, 5, tx).wait_send()

        return types.SimpleNamespace(start=start, relay=relay, rest=rest, finish=finish, drain=drain)

    def token_leg(source, q, piece, slot, to):
        ref = r.tok.at[2 * source + c, q, pl.ds(piece * half, half)]
        return remote(ref, ref, r.tok_send.at[source, slot], r.tok_recv.at[source, slot], (e, to))

    def token_legs(source, piece):
        return token_leg(source, t, piece, piece, tx), token_leg(source, t, piece, 2 + piece, ty)

    def hiddens(k):
        return plane(
            lambda q, piece: r.hid.at[k, q, pl.ds(piece * 2 * cap, 2 * cap)],
            lambda slot: r.hid_send.at[k, slot],
            lambda slot: r.hid_recv.at[k, slot],
        )

    shares = plane(
        lambda q, piece: r.share.at[q, pl.ds(piece * half, half)],
        lambda slot: r.share_send.at[slot],
        lambda slot: r.share_recv.at[slot],
    )
    mixes = plane(
        lambda q, piece: r.mix.at[q, pl.ds(piece * half, half)],
        lambda slot: r.mix_send.at[slot],
        lambda slot: r.mix_recv.at[slot],
    )

    def across(source, q, whose):
        ref = r.tok.at[2 * source + whose, q]
        return remote(ref, ref, r.pair_send.at[source, q], r.pair_recv.at[source, q], (partner, t))

    def along(source, slot, up):
        block = 2 * source + c
        ref = r.tok.at[block, td] if slot == 2 else r.tok.at[block, t, pl.ds(slot * half, half)]
        to = 2 * (z - 1 + 2 * up) + c
        return remote(ref, ref, r.z_send.at[source, slot, up], r.z_recv.at[source, slot], (to, t))

    def onward(up):
        return z + 1 < nz if up else z - 1 >= 0

    def sides(s, act):
        @pl.when(z - s >= 0)
        def _():
            act(z - s, 1)

        @pl.when(z + s < nz)
        def _():
            act(z + s, 0)

    def pass_on(source, slot, up):
        along(source, slot, 1 - up).wait_recv()

        @pl.when(onward(up))
        def _():
            along(source, slot, up).start()

    def near_piece(piece, source, up):
        pass_on(source, piece, up)
        for one in token_legs(source, piece):
            one.start()

    def near_part(source, up):
        near_piece(0, source, up)
        near_piece(1, source, up)
        across(source, t, c).start()

    def near_rest(source, up):
        near_piece(1, source, up)
        across(source, t, c).start()

    def far_part(source, up):
        pass_on(source, 2, up)
        across(source, td, c).start()

    def route_to(by):
        ref = r.route.at[e]
        return remote(ref, ref, r.route_send.at[by], r.route_recv.at[e], (lax.rem(e + by, n_ep), t))

    def route_from(source):
        ref = r.route.at[source]
        return remote(ref, ref, r.route_send.at[0], r.route_recv.at[source], (e, t))

    edges = ((r.v_x, r.halo_x), (r.v_b, r.halo_b), (r.v_c, r.halo_c))

    def halo(i):
        src, dst = edges[i]
        return remote(
            src.at[pl.ds(rows - HALO, HALO)], dst, r.halo_send.at[i], r.halo_recv.at[i], (lax.rem(e + 1, n_ep), t)
        )

    got("rows", "scale")
    step_rows = 16

    def norm_rows(i, _):
        part = r.v_rows[at(i * step_rows, step_rows), :].astype(f32)
        by = lax.rsqrt(jnp.mean(part * part, axis=-1, keepdims=True) + epsilon)
        part = (part * by * r.v_scale[...]).astype(bf16)
        for q in range(tp):
            r.tok[e, q, at(i * step_rows, step_rows), :] = part[:, q * quarter : (q + 1) * quarter]
        return 0

    lax.fori_loop(0, rows // step_rows, norm_rows, 0, unroll=4)
    got("ids", "wts")
    below = iota((rows, rows), 0)
    right = iota((rows, rows), 1)
    r.earlier[...] = (below < right).astype(bf16)
    r.route[e, 0:TOP_K, :] = r.v_ids[...].astype(f32)
    r.route[e, TOP_K : 2 * TOP_K, :] = r.v_wts[...]
    got("x", "b", "c")
    pl.semaphore_wait(barrier, n_ep - 1 + 2)

    @pl.when(e + 1 < n_ep)
    def _():
        for i in range(3):
            halo(i).start()

    for by in range(1, n_ep):
        route_to(by).start()
    for slot in range(3):
        for up in (1, 0):

            @pl.when(onward(up))
            def _():
                along(z, slot, up).start()

    for q in range(tp):
        across(z, q, c).start()
    got("sg", "su")
    gate, up = 0.0, 0.0
    for q in range(tp):
        part = r.tok[e, q]
        gate = gate + dot(part, r.v_sg[q * quarter : (q + 1) * quarter, :])
        up = up + dot(part, r.v_su[q * quarter : (q + 1) * quarter, :])
    r.share[t] = (silu(gate) * up).astype(bf16)
    shares.start()

    def enter(k):
        source = zsource(k)
        seats = iota((cap, rows), 0).astype(f32)
        for c2 in range(2):
            block = 2 * source + c2
            ids = r.route[block, 0:TOP_K, :]
            weights = r.route[block, TOP_K : 2 * TOP_K, :]
            for j in range(2):
                hit = ids == (2 * e + j).astype(f32)
                named = jnp.sum(jnp.where(hit, 1.0, 0.0), axis=0, keepdims=True)
                given = jnp.sum(jnp.where(hit, weights, 0.0), axis=0, keepdims=True)
                count = dot(jnp.broadcast_to(named, (16, rows)).astype(bf16), r.earlier[...])
                seat = jnp.where(named > 0.0, count[0:1, :], -1.0)
                taken = seats == seat
                r.pick[k, c2, j * cap : (j + 1) * cap, :] = jnp.where(taken, 1.0, 0.0).astype(bf16)
                amount = jnp.sum(jnp.where(taken, given, 0.0), axis=1, keepdims=True)
                r.amount[k, j, c2 * cap : (c2 + 1) * cap, :] = jnp.broadcast_to(amount, (cap, LANES))
            for q in range(tp):
                chosen = dot(r.pick[k, c2], r.tok[block, q]).astype(bf16)
                for j in range(2):
                    r.arrived[j, c2 * cap : (c2 + 1) * cap, q * quarter : (q + 1) * quarter] = chosen[
                        j * cap : (j + 1) * cap, :
                    ]
        for j in range(2):
            gate = dot(r.arrived[j], r.v_wg[j])
            up = dot(r.arrived[j], r.v_wu[j])
            r.hid[k, t, j * 2 * cap : (j + 1) * 2 * cap, :] = (silu(gate) * up).astype(bf16)

    @pl.when(e > 0)
    def _():
        for i in range(3):
            halo(i).wait_recv()

    @pl.when(e == 0)
    def _():
        for _, dst in edges:
            dst[...] = jnp.zeros_like(dst)

    got("vk", "bk", "ck", "step", "extra", "hld")

    def conv(src, edge, taps, out):
        def chunk(i, _):
            lanes = at(i * LANES, LANES)
            r.padded[0:8, :] = edge[:, lanes].astype(f32)[HALO - 8 :]
            r.padded[8 : 8 + rows, :] = src[:, lanes].astype(f32)
            total = jnp.zeros((rows, LANES), f32)
            for k in range(CONV_TAPS):
                lead = 8 - CONV_TAPS + 1 + k
                total = total + r.padded[lead : lead + rows, :] * taps[k : k + 1, lanes]
            out[:, lanes] = silu(total).astype(bf16)
            return 0

        lax.fori_loop(0, src.shape[1] // LANES, chunk, 0)

    conv(r.v_x, r.halo_x, r.v_vk, r.vals)
    conv(r.v_b, r.halo_b, r.v_bk, r.inm)
    conv(r.v_c, r.halo_c, r.v_ck, r.outm)
    route_from(partner).wait_recv()
    got("wg", "wu")
    for q in range(tp):
        across(z, q, other).wait_recv()
    enter(0)
    hiddens(0).start()
    shares.relay()
    sides(1, functools.partial(near_piece, 0))
    pre = r.v_step[...]
    steps = jnp.maximum(pre, 0.0) + jnp.log(1.0 + jnp.exp(-jnp.abs(pre)))
    diagonal = iota((heads, heads), 0) == iota((heads, heads), 1)
    rate = jnp.sum(jnp.where(diagonal, jnp.exp(r.v_hld[...]), 0.0), axis=1, keepdims=True)
    decay = -rate * steps + r.v_extra[...]
    upto = (below <= right).astype(f32)
    cum_t = dot(decay, upto, exact=True)
    cum = dot((right <= below).astype(f32), decay, ((1,), (1,)), exact=True)
    r.cum[...] = cum
    r.cum_t[...] = cum_t
    r.step_t[...] = steps
    spread_heads = (lax.div(iota((heads, width), 1), HEAD_DIM) == iota((heads, width), 0)).astype(f32)
    r.growth[...] = dot(jnp.exp(cum), spread_heads, exact=True)
    to_end = jnp.exp(cum_t[:, rows - 1 : rows] - cum_t) * steps
    r.to_end[...] = dot(to_end, spread_heads, ((0,), (0,)), exact=True)
    for g in range(groups):
        lanes = pl.ds(g * band, band)
        weighted = (r.vals[:, lanes].astype(f32) * r.to_end[:, lanes]).astype(bf16)
        r.state[:, lanes] = dot(r.inm[:, g * STATE : (g + 1) * STATE], weighted, ((0,), (0,)))
    r.state_out[...] = r.state[...].astype(bf16)
    r.decay_out[...] = jnp.broadcast_to(r.growth[rows - 1 : rows, :], (8, width))

    def swap(i):
        src, dst = ((r.state_out, r.state_in), (r.decay_out, r.decay_in))[i]
        return remote(src, dst, r.swap_send.at[i], r.swap_recv.at[i], (partner, t))

    for i in range(2):
        swap(i).start()
    side = width // 2
    mine_lanes = at(c * side, side)

    def chain(i, by):
        src, dst = ((r.chip_state, r.chain_state), (r.chip_decay, r.chain_decay))[i]
        to = 2 * lax.rem(z + by, nz) + c
        return remote(src, dst.at[z], r.chain_send.at[i, by], r.chain_recv.at[i, z], (to, t))

    def chain_in(i, source):
        src, dst = ((r.chip_state, r.chain_state), (r.chip_decay, r.chain_decay))[i]
        return remote(src, dst.at[source], r.chain_send.at[i, 0], r.chain_recv.at[i, source], (e, t))

    def send_chain():
        for i in range(2):
            swap(i).wait_recv()
        ours, theirs = r.state[:, mine_lanes], r.state_in[:, mine_lanes].astype(f32)
        our_decay, their_decay = r.decay_out[:, mine_lanes], r.decay_in[:, mine_lanes]
        first = jnp.where(c == 0, ours, theirs)
        second = jnp.where(c == 0, theirs, ours)
        late = jnp.where(c == 0, their_decay, our_decay)
        r.chip_state[...] = (late[0:1, :] * first + second).astype(bf16)
        r.chip_decay[...] = our_decay * their_decay
        for by in range(1, nz):

            @pl.when(z + by < nz)
            def _():
                for i in range(2):
                    chain(i, by).start()

    def inside():
        mid = rows // 2
        lane = iota((mid, 2 * HEAD_DIM), 1) < HEAD_DIM
        for g in range(groups):
            cols = slice(g * STATE, (g + 1) * STATE)
            for part in range(2):
                span = slice(part * mid, (part + 1) * mid)
                reach = (part + 1) * mid
                scores = dot(r.outm[span, cols], r.inm[0:reach, cols], ((1,), (1,)))
                mask = iota((mid, reach), 0) + part * mid >= iota((mid, reach), 1)
                for p in range(ratio // 2):
                    pair = []
                    head = g * ratio + 2 * p
                    lanes = slice(head * HEAD_DIM, (head + 2) * HEAD_DIM)
                    for h in (head, head + 1):
                        diff = r.cum[span, h : h + 1] - r.cum_t[h : h + 1, 0:reach]
                        grid = scores * jnp.exp(jnp.where(mask, diff, -1e30)) * r.step_t[h : h + 1, 0:reach]
                        pair.append(dot(grid.astype(bf16), r.vals[0:reach, lanes]))
                    r.near[span, lanes] = jnp.where(lane, pair[0], pair[1])

    def back_pair(k):
        return remote(r.yours.at[k], r.theirs.at[k], r.pair_y_send.at[k], r.pair_y_recv.at[k], (partner, t))

    def back(k):
        source = zsource(k)
        return remote(r.going.at[k], r.coming.at[z], r.y_send.at[k], r.y_recv.at[z], (2 * source + c, t))

    def back_in(source):
        return remote(r.going.at[0], r.coming.at[source], r.y_send.at[0], r.y_recv.at[source], (e, t))

    def leave(k, carry=0):
        hiddens(k).finish()
        for j in range(2):
            total = 0.0
            for q in range(tp):
                total = total + dot(
                    r.hid[k, q, j * 2 * cap : (j + 1) * 2 * cap, :], r.v_wd[j, q * ff : (q + 1) * ff, :]
                )
            total = (total * r.amount[k, j, :, 0:1]).astype(bf16)
            for c2 in range(2):
                r.result[c2, j * cap : (j + 1) * cap, :] = total[c2 * cap : (c2 + 1) * cap, :]
        r.yours[k] = dot(r.pick[k, other], r.result[other], ((0,), (0,))).astype(bf16)
        back_pair(k).start()
        r.ours[k] = dot(r.pick[k, c], r.result[c], ((0,), (0,)))
        return carry

    def send_back(k, carry=0):
        back_pair(k).wait_recv()
        r.going[k] = (r.ours[k] + r.theirs[k].astype(f32)).astype(bf16)
        back(k).start()
        return carry

    sides(1, near_rest)
    hiddens(0).relay()

    def stage(k, _):
        source = zsource(k)

        sides(k, far_part)

        @pl.when(k == 1)
        def _():
            inside()

        @pl.when(k == 2)
        def _():
            got("wd")

        @pl.when(k == nz - 1)
        def _():
            send_chain()

        for piece in range(2):
            token_leg(source, tx, piece, piece, tx).wait_recv()
        across(source, tx, c).start()
        for piece in range(2):
            token_leg(source, ty, piece, 2 + piece, ty).wait_recv()
        across(source, ty, c).start()
        for c2 in range(2):
            route_from(2 * source + c2).wait_recv()

        sides(k + 1, near_part)
        for q in range(tp):
            across(source, q, other).wait_recv()
        enter(k)

        @pl.when(jnp.logical_and(k > 1, k < nz - 1))
        def _():
            hiddens(k - 1).relay()

        hiddens(k).start()
        return 0

    lax.fori_loop(1, nz, stage, 0)
    lax.fori_loop(1, nz - 2, leave, 0)
    hiddens(nz - 2).relay()
    lax.fori_loop(1, nz - 2, send_back, 0)

    r.before[...] = jnp.zeros_like(r.before)

    def add_chain(source, _):
        @pl.when(source < z)
        def _():
            for i in range(2):
                chain_in(i, source).wait_recv()
            r.before[...] = r.chain_decay[source, 0:1, :] * r.before[...] + r.chain_state[source].astype(f32)

        return 0

    lax.fori_loop(0, nz, add_chain, 0)
    r.incoming[c] = r.before[...].astype(bf16)

    def halves(whose):
        ref = r.incoming.at[whose]
        return remote(ref, ref, r.half_sem.at[0], r.half_sem.at[1], (partner, t))

    halves(c).start()
    got("gate", "skip", "mscale")

    def mixer_end():
        halves(other).wait_recv()
        spread_heads = (lax.div(iota((heads, width), 1), HEAD_DIM) == iota((heads, width), 0)).astype(f32)
        skip = dot(jnp.broadcast_to(r.v_skip[...], (8, heads)), spread_heads, exact=True)[0:1, :]
        for s in range(2):
            lanes = slice(s * side, (s + 1) * side)
            hold = r.incoming[s].astype(f32)
            later = r.decay_in[0:1, lanes] * hold + r.state_in[:, lanes].astype(f32)
            r.entering[:, lanes] = jnp.where(c == 0, hold, later).astype(bf16)
        for g in range(groups):
            lanes = slice(g * band, (g + 1) * band)
            far = dot(r.outm[:, g * STATE : (g + 1) * STATE], r.entering[:, lanes]) * r.growth[:, lanes]
            mixed = r.near[:, lanes] + far + skip[:, lanes] * r.vals[:, lanes].astype(f32)
            gated = mixed * silu(r.v_gate[:, lanes].astype(f32))
            by = lax.rsqrt(jnp.mean(gated * gated, axis=-1, keepdims=True) + epsilon)
            r.mix[t, :, lanes] = (gated * by * r.v_mscale[:, lanes]).astype(bf16)

    hiddens(nz - 1).relay()
    mixer_end()
    mixes.start()
    leave(nz - 2)
    leave(nz - 1)
    send_back(nz - 2)
    leave(0)
    send_back(nz - 1)
    got("sd", "wm")

    shares.finish()
    routed = 0.0
    for q in range(tp):
        routed = routed + dot(r.share[q], r.v_sd[q * sff : (q + 1) * sff, :])
    r.mixer_sum[...] = dot(r.mix[t], r.v_wm[at(t * width, width), :])
    mixes.relay()
    back_pair(0).wait_recv()
    r.routed_sum[...] = routed + r.ours[0] + r.theirs[0].astype(f32)

    def add_back(k, _):
        back_in(zsource(k)).wait_recv()
        r.routed_sum[...] += r.coming[zsource(k)].astype(f32)
        return 0

    def add_mix(q):
        r.mixer_sum[...] += dot(r.mix[q], r.v_wm[at(q * width, width), :])

    def outcopy(i):
        src, dst = ((r.mixer_bf, r.mixer_out), (r.routed_bf, r.routed_out))[i]
        return pltpu.make_async_copy(src, dst, r.out_sem.at[i])

    legs = mixes.rest()
    legs[0].wait_recv()
    add_mix(tx)
    legs[1].wait_recv()
    add_mix(ty)
    lax.fori_loop(1, nz, add_back, 0)
    r.routed_bf[...] = r.routed_sum[...].astype(bf16)
    outcopy(1).start()
    legs[2].wait_recv()
    legs[3].wait_recv()
    add_mix(td)
    r.mixer_bf[...] = r.mixer_sum[...].astype(bf16)
    outcopy(0).start()

    @pl.when(e + 1 < n_ep)
    def _():
        for i in range(3):
            halo(i).wait_send()

    for by in range(1, n_ep):
        route_to(by).wait_send()
    for i in range(2):
        swap(i).wait_send()
    for by in range(1, nz):

        @pl.when(z + by < nz)
        def _():
            for i in range(2):
                chain(i, by).wait_send()

    halves(c).wait_send()
    mixes.drain()
    shares.drain()

    def drain(k, _):
        source = zsource(k)

        def sent(up):
            for slot in range(3):
                along(source, slot, up).wait_send()

        @pl.when(jnp.logical_and(source <= z, onward(1)))
        def _():
            sent(1)

        @pl.when(jnp.logical_and(source >= z, onward(0)))
        def _():
            sent(0)

        @pl.when(k > 0)
        def _():
            for piece in range(2):
                for one in token_legs(source, piece):
                    one.wait_send()
            back(k).wait_send()

        for q in range(tp):
            across(source, q, c).wait_send()
        hiddens(k).drain()
        back_pair(k).wait_send()
        return 0

    lax.fori_loop(0, nz, drain, 0)
    for i in range(2):
        outcopy(i).wait()


def fused_on_device(*given):
    argument = dict(zip(ARGUMENTS, given))
    rows, model_width = argument["rows"].shape
    n_ep, tp = lax.axis_size("ep"), lax.axis_size("tp")
    nz = n_ep // 2
    heads = argument["step"].shape[1]
    width = argument["x"].shape[1]
    state_width = argument["b"].shape[1]
    groups = state_width // STATE
    local_experts, _, ff = argument["wg"].shape
    sff = argument["sg"].shape[1]
    quarter = argument["wd"].shape[2]
    cap = max(2, 3 * rows * TOP_K // (2 * local_experts * n_ep))
    for name in ("hld", "skip", "mscale", "scale"):
        argument[name] = argument[name].reshape(1, -1)
    for name in ("ids", "wts", "step", "extra"):
        argument[name] = argument[name].T
    dims = types.SimpleNamespace(
        n_ep=n_ep, tp=tp, rows=rows, cap=cap, ratio=heads // groups, quarter=quarter, heads=heads,
        groups=groups, width=width, ff=ff, sff=sff,
        fetched=FETCHED,
    )
    f32, bf16 = jnp.float32, jnp.bfloat16
    scratch = dict(("v_" + n, pltpu.VMEM(argument[n].shape, argument[n].dtype)) for n in FETCHED)
    vmem = dict(
        tok=((n_ep, tp, rows, quarter), bf16),
        hid=((nz, tp, 4 * cap, ff), bf16),
        mix=((tp, rows, width), bf16),
        share=((tp, rows, sff), bf16),
        route=((n_ep, 2 * TOP_K, rows), f32),
        halo_x=((HALO, width), bf16),
        halo_b=((HALO, state_width), bf16),
        halo_c=((HALO, state_width), bf16),
        padded=((8 + rows, LANES), f32),
        vals=((rows, width), bf16),
        inm=((rows, state_width), bf16),
        outm=((rows, state_width), bf16),
        cum=((rows, heads), f32),
        cum_t=((heads, rows), f32),
        step_t=((heads, rows), f32),
        growth=((rows, width), f32),
        to_end=((rows, width), f32),
        state=((STATE, width), f32),
        state_out=((STATE, width), bf16),
        state_in=((STATE, width), bf16),
        decay_out=((8, width), f32),
        decay_in=((8, width), f32),
        chip_state=((STATE, width // 2), bf16),
        chip_decay=((8, width // 2), f32),
        chain_state=((nz, STATE, width // 2), bf16),
        chain_decay=((nz, 8, width // 2), f32),
        before=((STATE, width // 2), f32),
        incoming=((2, STATE, width // 2), bf16),
        entering=((STATE, width), bf16),
        near=((rows, width), f32),
        earlier=((rows, rows), bf16),
        pick=((nz, 2, 2 * cap, rows), bf16),
        amount=((nz, 2, 2 * cap, LANES), f32),
        arrived=((2, 2 * cap, model_width), bf16),
        result=((2, 2 * cap, quarter), bf16),
        yours=((nz, rows, quarter), bf16),
        theirs=((nz, rows, quarter), bf16),
        ours=((nz, rows, quarter), f32),
        going=((nz, rows, quarter), bf16),
        coming=((nz, rows, quarter), bf16),
        routed_bf=((rows, quarter), bf16),
        mixer_bf=((rows, quarter), bf16),
        routed_sum=((rows, quarter), f32),
        mixer_sum=((rows, quarter), f32),
    )
    for name, (shape, dtype) in vmem.items():
        scratch[name] = pltpu.VMEM(shape, dtype)
    sems = dict(
        local_sem=(len(FETCHED),),
        out_sem=(2,),
        tok_send=(nz, 4), tok_recv=(nz, 4), hid_send=(nz, 6), hid_recv=(nz, 6),
        mix_send=(6,), mix_recv=(6,), pair_send=(nz, tp), pair_recv=(nz, tp),
        z_send=(nz, 3, 2), z_recv=(nz, 3), share_send=(6,), share_recv=(6,), route_send=(n_ep,), route_recv=(n_ep,),
        halo_send=(3,), halo_recv=(3,), swap_send=(2,), swap_recv=(2,),
        chain_send=(2, nz), chain_recv=(2, nz), half_sem=(2,),
        pair_y_send=(nz,), pair_y_recv=(nz,), y_send=(nz,), y_recv=(nz,),
    )
    for name, shape in sems.items():
        scratch[name] = pltpu.SemaphoreType.DMA(shape)
    order = tuple(FETCHED)
    names = order + ("mixer_out", "routed_out") + tuple(scratch)
    out = jax.ShapeDtypeStruct((rows, quarter), bf16)
    return tuple(
        pl.pallas_call(
            functools.partial(body, dims, names),
            out_shape=(out, out),
            in_specs=[pl.BlockSpec(memory_space=pl.ANY)] * len(order),
            out_specs=(pl.BlockSpec(memory_space=pl.ANY),) * 2,
            scratch_shapes=list(scratch.values()),
            compiler_params=pltpu.CompilerParams(
                collective_id=0, has_side_effects=True, vmem_limit_bytes=VMEM_LIMIT
            ),
            name="mixer_and_experts",
        )(*[argument[n] for n in order])
    )


VMEM_LIMIT = 62 * 1024 * 1024 + 512 * 1024
ARGUMENTS = (
    "x", "b", "c", "gate", "step", "extra", "hld", "skip", "vk", "bk", "ck", "mscale", "wm",
    "rows", "scale", "ids", "wts", "wg", "wu", "wd", "sg", "su", "sd",
)
FETCHED = (
    "rows", "scale", "ids", "wts", "x", "b", "c", "sg", "su", "vk", "bk", "ck", "step", "extra", "hld",
    "wg", "wu", "gate", "skip", "mscale", "wd", "sd", "wm",
)


def choose(*given):
    argument = dict(zip(ARGUMENTS, given))
    n_ep, tp = lax.axis_size("ep"), lax.axis_size("tp")
    rows = argument["rows"].shape[0]
    experts = argument["wg"].shape[0]
    cap = max(2, 3 * rows * TOP_K // (2 * experts * n_ep))
    wide = all(argument[n].shape[-1] % LANES == 0 for n in ("x", "b", "wg", "wd", "sg"))
    fits = tp == 4 and n_ep % 2 == 0 and n_ep >= 6 and experts == 2
    fits = fits and wide and cap % 16 == 0 and rows % 32 == 0
    return fused_on_device(*given) if fits else on_device(*given)


def solution(mesh):
    return jax.shard_map(
        choose,
        mesh=mesh,
        in_specs=(
            P("ep", "tp"),
            P("ep", "tp"),
            P("ep", "tp"),
            P("ep", "tp"),
            P("ep", "tp"),
            P("ep", "tp"),
            P("tp"),
            P("tp"),
            P(None, "tp"),
            P(None, "tp"),
            P(None, "tp"),
            P("tp"),
            P(None, "tp"),
            P("ep", None),
            P(),
            P("ep", None),
            P("ep", None),
            P("ep", None, "tp"),
            P("ep", None, "tp"),
            P("ep", None, "tp"),
            P(None, "tp"),
            P(None, "tp"),
            P(None, "tp"),
        ),
        out_specs=(P("ep", "tp"), P("ep", "tp")),
        check_vma=False,
    )
```

```python
import functools
import types

import jax
import jax.numpy as jnp
from jax import lax
from jax.experimental import pallas as pl
from jax.experimental.pallas import tpu as pltpu
from jax.sharding import PartitionSpec as P

HEAD_DIM = 64
STATE = 128
CONV_TAPS = 4
BLOCK = 128
TOP_K = 4


epsilon = 1e-05
precise = lax.Precision.HIGHEST


def passed_along(x, axis, by):
    size = lax.axis_size(axis)
    pairs = [(i, i + by) for i in range(size) if 0 <= i + by < size]
    return lax.ppermute(x, axis, pairs)


def carried_in(total_log, state, axis):
    size = lax.axis_size(axis)
    place = lax.axis_index(axis)
    log = passed_along(total_log, axis, 1)
    hold = passed_along(state.astype(jnp.bfloat16), axis, 1).astype(jnp.float32)
    by = 1
    while by < size - 1:
        before = passed_along(hold.astype(jnp.bfloat16), axis, by).astype(jnp.float32)
        hold = hold + jnp.exp(log)[:, None, None] * before
        log = log + passed_along(log, axis, by)
        by *= 2
    return hold


def conv_silu(tail_rows, source, weights):
    length = source.shape[0]
    padded = jnp.concatenate([tail_rows, source], axis=0)
    total_sum = jnp.zeros(source.shape, jnp.float32)
    for tap_index in range(CONV_TAPS):
        total_sum = (
            total_sum
            + padded[tap_index : tap_index + length].astype(jnp.float32) * weights[tap_index]
        )
    return jax.nn.silu(total_sum).astype(jnp.bfloat16)


def carry_blocks(carried, inputs):
    block_decay, block_state = inputs
    return (carried * block_decay[:, None, None] + block_state, carried)


def earlier_counts(mask, rows):
    at = jnp.arange(rows)
    tri = (at[:, None] < at[None, :]).astype(jnp.bfloat16)
    return lax.dot_general(
        mask.astype(jnp.bfloat16),
        tri,
        (((mask.ndim - 1,), (0,)), ((), ())),
        preferred_element_type=jnp.float32,
    )


def on_device(
    mixer_value_input,
    input_state_matrix,
    output_state_matrix,
    output_gate_input,
    step_input,
    extra_log_decay,
    head_log_decay,
    head_skip_scale,
    value_kernel,
    input_matrix_kernel,
    output_matrix_kernel,
    mixer_norm_scale,
    mixer_output_weight,
    second_token_rows,
    expert_norm_scale,
    routed_expert_index,
    routed_expert_weight,
    routed_gate_weight,
    routed_up_weight,
    routed_down_weight,
    shared_gate_weight,
    shared_up_weight,
    shared_down_weight,
):
    length = mixer_value_input.shape[0]
    heads_local = step_input.shape[1]
    width_x = mixer_value_input.shape[1]
    width_b = input_state_matrix.shape[1]
    groups_local = width_b // STATE
    head_ratio = heads_local // groups_local
    nblocks = length // BLOCK
    lead_row = length - CONV_TAPS + 1
    edge_rows = jnp.concatenate(
        [
            mixer_value_input[lead_row:],
            input_state_matrix[lead_row:],
            output_state_matrix[lead_row:],
        ],
        axis=1,
    )
    tail_rows = passed_along(edge_rows, "ep", 1)
    rows_local = second_token_rows.shape[0]
    model_width = second_token_rows.shape[1]
    local_experts = routed_gate_weight.shape[0]
    ep_count = lax.axis_size("ep")
    experts = local_experts * ep_count
    capacity = max(2, 3 * rows_local * TOP_K // (2 * experts))
    col_width = model_width // lax.axis_size("tp")
    rows_wide = second_token_rows.astype(jnp.float32)
    normed = (
        rows_wide
        * lax.rsqrt(jnp.mean(rows_wide * rows_wide, axis=-1, keepdims=True) + epsilon)
        * expert_norm_scale
    ).astype(jnp.bfloat16)
    ids = routed_expert_index.T.astype(jnp.float32)
    id_rows = -(-ids.size // col_width)
    id_block = jnp.pad(
        ids.astype(jnp.bfloat16).reshape(-1), (0, id_rows * col_width - ids.size)
    ).reshape(id_rows, col_width)
    id_block = jnp.pad(id_block, ((0, -id_rows % 8), (0, 0)))
    my_columns = lax.dynamic_slice_in_dim(normed, lax.axis_index("tp") * col_width, col_width, 1)
    outgoing, value_rows, in_rows, out_rows = lax.optimization_barrier(
        (
            jnp.concatenate([my_columns, id_block], axis=0),
            mixer_value_input,
            input_state_matrix,
            output_state_matrix,
        )
    )
    everyone = lax.all_gather(outgoing, "ep", axis=0)
    values = conv_silu(tail_rows[:, :width_x], value_rows, value_kernel)
    in_mat = conv_silu(
        tail_rows[:, width_x : width_x + width_b], in_rows, input_matrix_kernel
    )
    out_mat = conv_silu(
        tail_rows[:, width_x + width_b :], out_rows, output_matrix_kernel
    )
    step_length = jax.nn.softplus(step_input)
    decay_logarithm = -jnp.exp(head_log_decay)[None, :] * step_length + extra_log_decay
    running = jnp.cumsum(decay_logarithm.reshape(nblocks, BLOCK, heads_local), axis=1)
    value_wide = values.astype(jnp.float32).reshape(nblocks, BLOCK, heads_local, HEAD_DIM)
    scaled = value_wide * step_length.reshape(nblocks, BLOCK, heads_local)[..., None]
    in_blocks = in_mat.reshape(nblocks, BLOCK, groups_local, STATE)
    out_blocks = out_mat.reshape(nblocks, BLOCK, groups_local, STATE)
    scores = jnp.einsum(
        "bign,bjgn->bgij", out_blocks, in_blocks, preferred_element_type=jnp.float32
    )
    scores = jnp.repeat(scores, head_ratio, axis=1)
    spread = jnp.transpose(running[:, :, None, :] - running[:, None, :, :], (0, 3, 1, 2))
    lower_mask = jnp.tril(jnp.ones((BLOCK, BLOCK), bool))[None, None]
    decay_mat = jnp.where(lower_mask, jnp.exp(jnp.where(lower_mask, spread, 0.0)), 0.0)
    inside = jnp.einsum("bhij,bjhp->bihp", scores * decay_mat, scaled, precision=precise)
    out_head = jnp.repeat(out_blocks.astype(jnp.float32), head_ratio, axis=2)
    in_head = jnp.repeat(in_blocks.astype(jnp.float32), head_ratio, axis=2)
    block_logs = running[:, -1]
    to_end = jnp.exp(block_logs[:, None, :] - running)
    block_state = jnp.einsum("bjhn,bjh,bjhp->bhpn", in_head, to_end, scaled, precision=precise)
    start_state = jnp.zeros((heads_local, HEAD_DIM, STATE), jnp.float32)
    local_total, local_prev = lax.scan(
        carry_blocks, start_state, (jnp.exp(block_logs), block_state)
    )
    before_logs = jnp.cumsum(block_logs, axis=0) - block_logs
    everyone, local_total = lax.optimization_barrier((everyone, local_total))
    incoming = carried_in(jnp.sum(block_logs, axis=0), local_total, "ep")
    their_rows = everyone[:, :rows_local]
    their_ids = everyone[:, rows_local : rows_local + id_rows].reshape(ep_count, -1)
    their_ids = their_ids[:, : ids.size].reshape(ep_count, TOP_K, rows_local).astype(jnp.float32)
    mine = (lax.axis_index("ep") * local_experts + jnp.arange(local_experts)).astype(jnp.float32)
    named = jnp.any(their_ids[:, None] == mine[None, :, None, None], axis=2)
    seat = jnp.where(named, earlier_counts(named, rows_local), -1.0)
    seats = jnp.arange(capacity, dtype=jnp.float32)
    pick = (seat[:, :, None, :] == seats[None, None, :, None]).astype(jnp.bfloat16)
    arrived = jnp.stack(
        [
            jnp.einsum(
                "bsr,brd->bsd", pick[:, j], their_rows, preferred_element_type=jnp.float32
            )
            .astype(jnp.bfloat16)
            .reshape(ep_count * capacity, col_width)
            for j in range(local_experts)
        ]
    )
    column_piece = lax.all_gather(arrived, "tp", axis=2, tiled=True)
    column_piece, incoming = lax.optimization_barrier((column_piece, incoming))
    entering = local_prev + jnp.exp(before_logs)[:, :, None, None] * incoming[None]
    carried_term = (
        jnp.einsum("bihn,bhpn->bihp", out_head, entering, precision=precise)
        * jnp.exp(running)[..., None]
    )
    mixed_heads = (inside + carried_term).reshape(length, heads_local, HEAD_DIM)
    mixed_heads = mixed_heads + head_skip_scale[None, :, None] * value_wide.reshape(
        length, heads_local, HEAD_DIM
    )
    gated_heads = mixed_heads * jax.nn.silu(output_gate_input.astype(jnp.float32)).reshape(
        length, heads_local, HEAD_DIM
    )
    grouped = gated_heads.reshape(length, groups_local, head_ratio * HEAD_DIM)
    grouped = grouped * lax.rsqrt(jnp.mean(grouped * grouped, axis=-1, keepdims=True) + epsilon)
    mixer_normed = (grouped.reshape(length, width_x) * mixer_norm_scale).astype(jnp.bfloat16)
    gate_pre = jnp.einsum(
        "esd,edf->esf", column_piece, routed_gate_weight, preferred_element_type=jnp.float32
    )
    up_pre = jnp.einsum(
        "esd,edf->esf", column_piece, routed_up_weight, preferred_element_type=jnp.float32
    )
    hidden = (jax.nn.silu(gate_pre) * up_pre).astype(jnp.bfloat16)
    shared_hidden = (
        jax.nn.silu(jnp.dot(normed, shared_gate_weight, preferred_element_type=jnp.float32))
        * jnp.dot(normed, shared_up_weight, preferred_element_type=jnp.float32)
    ).astype(jnp.bfloat16)
    whole_hidden = lax.all_gather(hidden, "tp", axis=2, tiled=True)
    both = lax.all_gather(
        jnp.concatenate([mixer_normed, shared_hidden], axis=1), "tp", axis=1, tiled=True
    ).reshape(length, lax.axis_size("tp"), -1)
    whole_mix = both[:, :, :width_x].reshape(length, -1)
    whole_shared = both[:, :, width_x:].reshape(length, -1)
    mixer_output = jnp.dot(
        whole_mix, mixer_output_weight, preferred_element_type=jnp.float32
    ).astype(jnp.bfloat16)
    expert_result = jnp.einsum(
        "esf,efd->esd", whole_hidden, routed_down_weight, preferred_element_type=jnp.float32
    ).astype(jnp.bfloat16)
    going = jnp.concatenate(
        [expert_result[j].reshape(ep_count, capacity, col_width) for j in range(local_experts)],
        axis=1,
    )
    returned = lax.all_to_all(going, "ep", split_axis=0, concat_axis=0, tiled=True)
    returned = returned.reshape(experts * capacity, col_width)
    kinds = jnp.arange(experts, dtype=jnp.float32)
    chosen = ids[:, None, :] == kinds[None, :, None]
    count = earlier_counts(jnp.any(chosen, axis=0), rows_local)
    position = jnp.sum(jnp.where(chosen, count[None], 0.0), axis=1)
    slot = (ids * capacity + position).T.astype(jnp.int32)
    columns = jnp.arange(experts * capacity, dtype=jnp.int32)[None, :]
    spread = jnp.zeros((rows_local, experts * capacity), jnp.float32)
    for k in range(TOP_K):
        spread = spread + jnp.where(
            slot[:, k : k + 1] == columns, routed_expert_weight[:, k : k + 1], 0.0
        )
    high = lax.reduce_precision(spread, 8, 7)
    low = (spread - high).astype(jnp.bfloat16)
    routed_sum = jnp.dot(
        high.astype(jnp.bfloat16), returned, preferred_element_type=jnp.float32
    ) + jnp.dot(low, returned, preferred_element_type=jnp.float32)
    shared_result = jnp.dot(whole_shared, shared_down_weight, preferred_element_type=jnp.float32)
    routed_out = (routed_sum + shared_result).astype(jnp.bfloat16)
    return (mixer_output, routed_out)


MESH = pl.DeviceIdType.MESH
HALO = 16
LANES = 128


def silu(v):
    return v / (1.0 + jnp.exp(-v))


def dot(a, b, contract=((1,), (0,)), exact=False):
    return lax.dot_general(
        a,
        b,
        (contract, ((), ())),
        precision=precise if exact else None,
        preferred_element_type=jnp.float32,
    )


def iota(shape, axis):
    return lax.broadcasted_iota(jnp.int32, shape, axis)


def at(start, size):
    return pl.ds(pl.multiple_of(start, size), size)


def body(dims, names, *refs):
    r = types.SimpleNamespace(**dict(zip(names, refs)))
    n_ep, rows, cap, ratio = dims.n_ep, dims.rows, dims.cap, dims.ratio
    nz = n_ep // 2
    half = rows // 2
    tp = dims.tp
    quarter = dims.quarter
    heads, groups, width = dims.heads, dims.groups, dims.width
    band = ratio * HEAD_DIM
    ff, sff = dims.ff, dims.sff
    f32, bf16 = jnp.float32, jnp.bfloat16

    e, t = lax.axis_index("ep"), lax.axis_index("tp")
    z, c = lax.div(e, 2), lax.rem(e, 2)
    other = 1 - c
    partner = e + 1 - 2 * c
    tx = t + 1 - 2 * lax.rem(t, 2)
    ty = lax.rem(t + 2, tp)
    td = tp - 1 - t

    def remote(src, dst, send, recv, to):
        return pltpu.make_async_remote_copy(
            src_ref=src, dst_ref=dst, send_sem=send, recv_sem=recv, device_id=to, device_id_type=MESH
        )

    fetched = dims.fetched

    def fetch(name):
        return pltpu.make_async_copy(
            getattr(r, name), getattr(r, "v_" + name), r.local_sem.at[fetched.index(name)]
        )

    for name in fetched:
        fetch(name).start()

    def got(*wanted):
        for name in wanted:
            fetch(name).wait()

    barrier = pltpu.get_barrier_semaphore()
    for by in range(1, n_ep):
        pl.semaphore_signal(barrier, inc=1, device_id=(lax.rem(e + by, n_ep), t), device_id_type=MESH)
    for to in (tx, ty):
        pl.semaphore_signal(barrier, inc=1, device_id=(e, to), device_id_type=MESH)

    longer = jnp.maximum(z, nz - 1 - z)
    inward = jnp.where(2 * z > nz - 1, -1, 1)

    def zsource(k):
        return jnp.where(k <= longer, z + inward * k, z - inward * (k - longer))

    def sent(ref, sem):
        remote(ref, ref, sem, sem, (partner, t)).wait_send()

    def landed(ref, sem):
        remote(ref, ref, sem, sem, (partner, t)).wait_recv()

    def plane(buf, send, recv):
        def leg(q, piece, slot, to):
            return remote(buf(q, piece), buf(q, piece), send, recv(slot), (e, to))

        def start():
            leg(t, 0, 0, tx).start()
            leg(t, 1, 1, ty).start()
            leg(t, 1, 2, tx).start()
            leg(t, 0, 3, ty).start()

        def relay():
            leg(tx, 0, 0, tx).wait_recv()
            leg(tx, 0, 4, ty).start()
            leg(ty, 1, 1, ty).wait_recv()
            leg(ty, 1, 5, tx).start()

        return types.SimpleNamespace(start=start, relay=relay)

    def token_leg(source, q, piece, slot, to):
        ref = r.tok.at[2 * source + c, q, pl.ds(piece * half, half)]
        return remote(ref, ref, r.tok_send, r.tok_recv.at[source, slot], (e, to))

    def token_legs(source, piece):
        return token_leg(source, t, piece, 0, tx), token_leg(source, t, piece, 1, ty)

    def hiddens(k):
        return plane(
            lambda q, piece: r.hid.at[k, q, pl.ds(piece * 2 * cap, 2 * cap)],
            r.hid_send,
            lambda slot: r.hid_recv.at[k, min(slot, 2)],
        )

    shares = plane(
        lambda q, piece: r.share.at[q, pl.ds(piece * half, half)],
        r.share_send,
        lambda slot: r.share_recv.at[min(slot, 2)],
    )
    mixes = plane(
        lambda q, piece: r.mix.at[q, pl.ds(piece * half, half)],
        r.mix_send,
        lambda slot: r.mix_recv.at[min(slot, 4)],
    )

    def across(source, q, whose):
        ref = r.tok.at[2 * source + whose, q]
        return remote(ref, ref, r.pair_send, r.pair_recv.at[source], (partner, t))

    def along(source, slot, up):
        block = 2 * source + c
        ref = r.tok.at[block, td] if slot == 2 else r.tok.at[block, t, pl.ds(slot * half, half)]
        to = 2 * (z - 1 + 2 * up) + c
        return remote(ref, ref, r.z_send.at[source, up], r.z_recv.at[source, slot], (to, t))

    def onward(up):
        return z + 1 < nz if up else z - 1 >= 0

    def sides(s, act):
        @pl.when(z - s >= 0)
        def _():
            act(z - s, 1)

        @pl.when(z + s < nz)
        def _():
            act(z + s, 0)

    def pass_on(source, slot, up):
        along(source, slot, 1 - up).wait_recv()

        @pl.when(onward(up))
        def _():
            along(source, slot, up).start()

    def near_piece(piece, source, up):
        pass_on(source, piece, up)
        for one in token_legs(source, piece):
            one.start()

    def near_part(source, up):
        near_piece(0, source, up)
        near_piece(1, source, up)
        across(source, t, c).start()

    def near_rest(source, up):
        near_piece(1, source, up)
        across(source, t, c).start()

    def far_part(source, up):
        pass_on(source, 2, up)
        across(source, td, c).start()

    def route_to(by):
        ref = r.route.at[e]
        return remote(ref, ref, r.route_send, r.route_recv.at[e], (lax.rem(e + by, n_ep), t))

    def route_from(source):
        ref = r.route.at[source]
        return remote(ref, ref, r.route_send, r.route_recv.at[source], (e, t))

    edges = ((r.v_x, r.halo_x), (r.v_b, r.halo_b), (r.v_c, r.halo_c))

    def halo(i):
        src, dst = edges[i]
        return remote(
            src.at[pl.ds(rows - HALO, HALO)], dst, r.halo_send.at[i], r.halo_recv.at[i], (lax.rem(e + 1, n_ep), t)
        )

    got("rows", "scale")
    step_rows = 16

    def norm_rows(i, _):
        part = r.v_rows[at(i * step_rows, step_rows), :].astype(f32)
        by = lax.rsqrt(jnp.mean(part * part, axis=-1, keepdims=True) + epsilon)
        part = (part * by * r.v_scale[...]).astype(bf16)
        for q in range(tp):
            r.tok[e, q, at(i * step_rows, step_rows), :] = part[:, q * quarter : (q + 1) * quarter]
        return 0

    lax.fori_loop(0, rows // step_rows, norm_rows, 0, unroll=4)
    got("ids", "wts")
    below = iota((rows, rows), 0)
    right = iota((rows, rows), 1)
    r.earlier[...] = (below < right).astype(bf16)
    r.route[e, 0:TOP_K, :] = r.v_ids[...].astype(f32)
    r.route[e, TOP_K : 2 * TOP_K, :] = r.v_wts[...]
    got("x", "b", "c")
    pl.semaphore_wait(barrier, n_ep - 1 + 2)

    @pl.when(e + 1 < n_ep)
    def _():
        for i in range(3):
            halo(i).start()

    for by in range(1, n_ep):
        route_to(by).start()
    for slot in range(3):
        for up in (1, 0):

            @pl.when(onward(up))
            def _():
                along(z, slot, up).start()

    for q in range(tp):
        across(z, q, c).start()
    got("sg", "su")
    gate, up = 0.0, 0.0
    for q in range(tp):
        part = r.tok[e, q]
        gate = gate + dot(part, r.v_sg[q * quarter : (q + 1) * quarter, :])
        up = up + dot(part, r.v_su[q * quarter : (q + 1) * quarter, :])
    r.share[t] = (silu(gate) * up).astype(bf16)
    shares.start()

    def enter(k):
        source = zsource(k)
        seats = iota((cap, rows), 0).astype(f32)
        for c2 in range(2):
            block = 2 * source + c2
            ids = r.route[block, 0:TOP_K, :]
            weights = r.route[block, TOP_K : 2 * TOP_K, :]
            for j in range(2):
                hit = ids == (2 * e + j).astype(f32)
                named = jnp.sum(jnp.where(hit, 1.0, 0.0), axis=0, keepdims=True)
                given = jnp.sum(jnp.where(hit, weights, 0.0), axis=0, keepdims=True)
                count = dot(jnp.broadcast_to(named, (16, rows)).astype(bf16), r.earlier[...])
                seat = jnp.where(named > 0.0, count[0:1, :], -1.0)
                taken = seats == seat
                r.pick[k, c2, j * cap : (j + 1) * cap, :] = jnp.where(taken, 1.0, 0.0).astype(bf16)
                amount = jnp.sum(jnp.where(taken, given, 0.0), axis=1, keepdims=True)
                r.amount[k, j, c2 * cap : (c2 + 1) * cap, :] = jnp.broadcast_to(amount, (cap, LANES))
            for q in range(tp):
                chosen = dot(r.pick[k, c2], r.tok[block, q]).astype(bf16)
                for j in range(2):
                    r.arrived[j, c2 * cap : (c2 + 1) * cap, q * quarter : (q + 1) * quarter] = chosen[
                        j * cap : (j + 1) * cap, :
                    ]
        for j in range(2):
            gate = dot(r.arrived[j], r.v_wg[j])
            up = dot(r.arrived[j], r.v_wu[j])
            r.hid[k, t, j * 2 * cap : (j + 1) * 2 * cap, :] = (silu(gate) * up).astype(bf16)

    @pl.when(e > 0)
    def _():
        for i in range(3):
            halo(i).wait_recv()

    @pl.when(e == 0)
    def _():
        for _, dst in edges:
            dst[...] = jnp.zeros_like(dst)

    got("vk", "bk", "ck", "step", "extra", "hld")

    def conv(src, edge, taps, out):
        def chunk(i, _):
            lanes = at(i * LANES, LANES)
            r.padded[0:8, :] = edge[:, lanes].astype(f32)[HALO - 8 :]
            r.padded[8 : 8 + rows, :] = src[:, lanes].astype(f32)
            total = jnp.zeros((rows, LANES), f32)
            for k in range(CONV_TAPS):
                lead = 8 - CONV_TAPS + 1 + k
                total = total + r.padded[lead : lead + rows, :] * taps[k : k + 1, lanes]
            out[:, lanes] = silu(total).astype(bf16)
            return 0

        lax.fori_loop(0, src.shape[1] // LANES, chunk, 0)

    conv(r.v_x, r.halo_x, r.v_vk, r.vals)
    conv(r.v_b, r.halo_b, r.v_bk, r.inm)
    conv(r.v_c, r.halo_c, r.v_ck, r.outm)
    route_from(partner).wait_recv()
    got("wg", "wu")
    landed(r.tok.at[2 * z + other], r.pair_recv.at[z])
    enter(0)
    hiddens(0).start()
    shares.relay()
    sides(1, functools.partial(near_piece, 0))
    pre = r.v_step[...]
    steps = jnp.maximum(pre, 0.0) + jnp.log(1.0 + jnp.exp(-jnp.abs(pre)))
    diagonal = iota((heads, heads), 0) == iota((heads, heads), 1)
    rate = jnp.sum(jnp.where(diagonal, jnp.exp(r.v_hld[...]), 0.0), axis=1, keepdims=True)
    decay = -rate * steps + r.v_extra[...]
    upto = (below <= right).astype(f32)
    cum_t = dot(decay, upto, exact=True)
    cum = dot((right <= below).astype(f32), decay, ((1,), (1,)), exact=True)
    r.cum[...] = cum
    r.cum_t[...] = cum_t
    r.step_t[...] = steps
    spread_heads = (lax.div(iota((heads, width), 1), HEAD_DIM) == iota((heads, width), 0)).astype(f32)
    r.growth[...] = dot(jnp.exp(cum), spread_heads, exact=True)
    to_end = jnp.exp(cum_t[:, rows - 1 : rows] - cum_t) * steps
    r.to_end[...] = dot(to_end, spread_heads, ((0,), (0,)), exact=True)
    for g in range(groups):
        lanes = pl.ds(g * band, band)
        weighted = (r.vals[:, lanes].astype(f32) * r.to_end[:, lanes]).astype(bf16)
        r.state[:, lanes] = dot(r.inm[:, g * STATE : (g + 1) * STATE], weighted, ((0,), (0,)))
    r.state_out[...] = r.state[...].astype(bf16)
    r.decay_out[...] = jnp.broadcast_to(r.growth[rows - 1 : rows, :], (8, width))

    def swap(i):
        src, dst = ((r.state_out, r.state_in), (r.decay_out, r.decay_in))[i]
        return remote(src, dst, r.swap_send.at[i], r.swap_recv.at[i], (partner, t))

    for i in range(2):
        swap(i).start()
    side = width // 2
    mine_lanes = at(c * side, side)

    def chain(up):
        to = 2 * (z + up) + c
        return remote(r.after, r.before, r.chain_sem.at[0], r.chain_sem.at[1], (to, t))

    def halves(whose):
        ref = r.incoming.at[whose]
        return remote(ref, ref, r.half_sem.at[0], r.half_sem.at[1], (partner, t))

    def chain_step():
        for i in range(2):
            swap(i).wait_recv()
        ours, theirs = r.state[:, mine_lanes], r.state_in[:, mine_lanes].astype(f32)
        our_decay, their_decay = r.decay_out[:, mine_lanes], r.decay_in[:, mine_lanes]
        first = jnp.where(c == 0, ours, theirs)
        second = jnp.where(c == 0, theirs, ours)
        late = jnp.where(c == 0, their_decay, our_decay)
        chip = late[0:1, :] * first + second

        @pl.when(z == 0)
        def _():
            r.before[...] = jnp.zeros_like(r.before)

        @pl.when(z > 0)
        def _():
            chain(0).wait_recv()

        r.incoming[c] = r.before[...]
        halves(c).start()

        @pl.when(onward(1))
        def _():
            both = our_decay[0:1, :] * their_decay[0:1, :]
            r.after[...] = (both * r.before[...].astype(f32) + chip).astype(bf16)
            chain(1).start()

    def inside():
        mid = rows // 2
        lane = iota((mid, 2 * HEAD_DIM), 1) < HEAD_DIM
        for g in range(groups):
            cols = slice(g * STATE, (g + 1) * STATE)
            for part in range(2):
                span = slice(part * mid, (part + 1) * mid)
                reach = (part + 1) * mid
                scores = dot(r.outm[span, cols], r.inm[0:reach, cols], ((1,), (1,)))
                mask = iota((mid, reach), 0) + part * mid >= iota((mid, reach), 1)
                for p in range(ratio // 2):
                    pair = []
                    head = g * ratio + 2 * p
                    lanes = slice(head * HEAD_DIM, (head + 2) * HEAD_DIM)
                    for h in (head, head + 1):
                        diff = r.cum[span, h : h + 1] - r.cum_t[h : h + 1, 0:reach]
                        grid = scores * jnp.exp(jnp.where(mask, diff, -1e30)) * r.step_t[h : h + 1, 0:reach]
                        pair.append(dot(grid.astype(bf16), r.vals[0:reach, lanes]))
                    r.near[span, lanes] = jnp.where(lane, pair[0], pair[1])

    def back_pair(k):
        return remote(r.yours.at[k], r.theirs.at[k], r.pair_y_send, r.pair_y_recv.at[k], (partner, t))

    def back(k):
        source = zsource(k)
        return remote(r.going.at[k], r.coming.at[z], r.y_send, r.y_recv.at[z], (2 * source + c, t))

    def back_in(source):
        return remote(r.going.at[0], r.coming.at[source], r.y_send, r.y_recv.at[source], (e, t))

    def leave(k, carry=0):
        landed(r.hid.at[k, 0:2], r.hid_recv.at[k, 2])
        for j in range(2):
            total = 0.0
            for q in range(tp):
                total = total + dot(
                    r.hid[k, q, j * 2 * cap : (j + 1) * 2 * cap, :], r.v_wd[j, q * ff : (q + 1) * ff, :]
                )
            total = (total * r.amount[k, j, :, 0:1]).astype(bf16)
            for c2 in range(2):
                r.result[c2, j * cap : (j + 1) * cap, :] = total[c2 * cap : (c2 + 1) * cap, :]
        r.yours[k] = dot(r.pick[k, other], r.result[other], ((0,), (0,))).astype(bf16)
        back_pair(k).start()
        r.ours[k] = dot(r.pick[k, c], r.result[c], ((0,), (0,)))
        return carry

    edge = jnp.logical_or(z == 0, z == nz - 1)
    second = jnp.logical_or(z == 1, z == nz - 2)

    def passing():
        to = 2 * (z + inward) + c
        return remote(r.going.at[2], r.passed, r.y_send, r.passed_sem, (to, t))

    def send_back(k, carry=0):
        @pl.when(jnp.logical_not(jnp.logical_and(k == 1, second)))
        def _():
            back_pair(k).wait_recv()
            r.going[k] = (r.ours[k] + r.theirs[k].astype(f32)).astype(bf16)
            aside = jnp.logical_and(k == 2, edge)

            @pl.when(aside)
            def _():
                passing().start()

            @pl.when(jnp.logical_not(aside))
            def _():
                back(k).start()

        return carry

    def join_back():
        @pl.when(second)
        def _():
            back_pair(1).wait_recv()
            landed(r.passed, r.passed_sem)
            total = r.ours[1] + r.theirs[1].astype(f32) + r.passed[...].astype(f32)
            r.going[1] = total.astype(bf16)
            back(1).start()


    sides(1, near_rest)

    @pl.when(z == 0)
    def _():
        chain_step()

    hiddens(0).relay()

    def stage(k, _):
        source = zsource(k)

        sides(k, far_part)

        @pl.when(k == 1)
        def _():
            inside()

        @pl.when(k == 2)
        def _():
            got("wd")

        @pl.when(k == nz - 1)
        def _():
            hiddens(k - 1).relay()

        for slot, q in ((0, tx), (1, ty)):
            landed(r.tok.at[2 * source + c, q], r.tok_recv.at[source, slot])
            across(source, q, c).start()
        for c2 in range(2):
            route_from(2 * source + c2).wait_recv()

        @pl.when(k != nz - 2)
        def _():
            sides(k + 1, near_part)

        @pl.when(k == z)
        def _():
            chain_step()

        landed(r.tok.at[2 * source + other], r.pair_recv.at[source])
        enter(k)
        hiddens(k).start()

        @pl.when(k == nz - 2)
        def _():
            sides(k + 1, near_part)

        @pl.when(jnp.logical_and(k > 1, k < nz - 1))
        def _():
            hiddens(k - 1).relay()

        return 0

    lax.fori_loop(1, nz, stage, 0)

    got("gate", "skip", "mscale")

    def mixer_end():
        halves(other).wait_recv()
        spread_heads = (lax.div(iota((heads, width), 1), HEAD_DIM) == iota((heads, width), 0)).astype(f32)
        skip = dot(jnp.broadcast_to(r.v_skip[...], (8, heads)), spread_heads, exact=True)[0:1, :]
        for s in range(2):
            lanes = slice(s * side, (s + 1) * side)
            hold = r.incoming[s].astype(f32)
            later = r.decay_in[0:1, lanes] * hold + r.state_in[:, lanes].astype(f32)
            r.entering[:, lanes] = jnp.where(c == 0, hold, later).astype(bf16)
        for g in range(groups):
            lanes = slice(g * band, (g + 1) * band)
            far = dot(r.outm[:, g * STATE : (g + 1) * STATE], r.entering[:, lanes]) * r.growth[:, lanes]
            mixed = r.near[:, lanes] + far + skip[:, lanes] * r.vals[:, lanes].astype(f32)
            gated = mixed * silu(r.v_gate[:, lanes].astype(f32))
            by = lax.rsqrt(jnp.mean(gated * gated, axis=-1, keepdims=True) + epsilon)
            r.mix[t, :, lanes] = (gated * by * r.v_mscale[:, lanes]).astype(bf16)

    lax.fori_loop(1, nz - 1, lambda i, carry: leave(nz - 1 - i, carry), 0)
    send_back(nz - 2)
    mixer_end()
    lax.fori_loop(2, nz - 1, lambda i, carry: send_back(nz - 1 - i, carry), 0)
    hiddens(nz - 1).relay()
    mixes.start()
    leave(nz - 1)
    leave(0)
    join_back()
    send_back(nz - 1)
    got("sd", "wm")

    landed(r.share.at[0:2], r.share_recv.at[2])
    routed = 0.0
    for q in range(tp):
        routed = routed + dot(r.share[q], r.v_sd[q * sff : (q + 1) * sff, :])
    r.mixer_sum[...] = dot(r.mix[t], r.v_wm[at(t * width, width), :])
    mixes.relay()
    back_pair(0).wait_recv()
    r.routed_sum[...] = routed + r.ours[0] + r.theirs[0].astype(f32)

    def add_back(k, _):
        source = zsource(k)
        low = jnp.logical_and(source == 0, z == 2)
        high = jnp.logical_and(source == nz - 1, z == nz - 3)

        @pl.when(jnp.logical_not(jnp.logical_or(low, high)))
        def _():
            back_in(source).wait_recv()
            r.routed_sum[...] += r.coming[source].astype(f32)

        return 0

    def add_mix(q):
        r.mixer_sum[...] += dot(r.mix[q], r.v_wm[at(q * width, width), :])

    def outcopy(i):
        src, dst = ((r.mixer_bf, r.mixer_out), (r.routed_bf, r.routed_out))[i]
        return pltpu.make_async_copy(src, dst, r.out_sem.at[i])

    landed(r.mix.at[0, 0:half], r.mix_recv.at[2])
    add_mix(tx)
    landed(r.mix.at[0, 0:half], r.mix_recv.at[3])
    add_mix(ty)
    lax.fori_loop(1, nz, add_back, 0)
    r.routed_bf[...] = r.routed_sum[...].astype(bf16)
    outcopy(1).start()
    landed(r.mix.at[0], r.mix_recv.at[4])
    add_mix(td)
    r.mixer_bf[...] = r.mixer_sum[...].astype(bf16)
    outcopy(0).start()

    @pl.when(e + 1 < n_ep)
    def _():
        for i in range(3):
            halo(i).wait_send()

    sent(r.route.at[0 : n_ep - 1], r.route_send)
    for i in range(2):
        swap(i).wait_send()

    @pl.when(onward(1))
    def _():
        chain(1).wait_send()

    halves(c).wait_send()
    sent(r.mix.at[0:3], r.mix_send)
    sent(r.share.at[0:3], r.share_send)
    sent(r.hid.at[:, 0:3], r.hid_send)
    sent(r.tok.at[0 : nz - 1, 0:2], r.tok_send)
    sent(r.tok.at[0:nz], r.pair_send)
    sent(r.yours, r.pair_y_send)
    sent(r.going.at[0 : nz - 1], r.y_send)

    def drain(source, _):
        for up in range(2):
            passed = source <= z if up else source >= z

            @pl.when(jnp.logical_and(passed, onward(up)))
            def _():
                sent(r.tok.at[0, 0:2], r.z_send.at[source, up])

        return 0

    lax.fori_loop(0, nz, drain, 0)
    for i in range(2):
        outcopy(i).wait()


def hand_out_body(first, second, first_out, second_out, held, sems):
    steps = []
    for i, (src, dst) in enumerate(((first, first_out), (second, second_out))):
        steps.append(
            (
                pltpu.make_async_copy(src, held.at[i], sems.at[i, 0]),
                pltpu.make_async_copy(held.at[i], dst, sems.at[i, 1]),
            )
        )
    for arrive, _ in steps:
        arrive.start()
    for arrive, depart in steps:
        arrive.wait()
        depart.start()
    for _, depart in steps:
        depart.wait()


def hand_out(first, second):
    out = jax.ShapeDtypeStruct(first.shape, first.dtype)
    return tuple(
        pl.pallas_call(
            hand_out_body,
            out_shape=(out, out),
            in_specs=[pl.BlockSpec(memory_space=pl.ANY)] * 2,
            out_specs=(pl.BlockSpec(memory_space=pl.ANY),) * 2,
            scratch_shapes=[pltpu.VMEM((2,) + first.shape, first.dtype), pltpu.SemaphoreType.DMA((2, 2))],
            name="hand_out",
        )(first, second)
    )


def fused_on_device(*given):
    argument = dict(zip(ARGUMENTS, given))
    rows, model_width = argument["rows"].shape
    n_ep, tp = lax.axis_size("ep"), lax.axis_size("tp")
    nz = n_ep // 2
    heads = argument["step"].shape[1]
    width = argument["x"].shape[1]
    state_width = argument["b"].shape[1]
    groups = state_width // STATE
    local_experts, _, ff = argument["wg"].shape
    sff = argument["sg"].shape[1]
    quarter = argument["wd"].shape[2]
    cap = max(2, 3 * rows * TOP_K // (2 * local_experts * n_ep))
    for name in ("hld", "skip", "mscale", "scale"):
        argument[name] = argument[name].reshape(1, -1)
    for name in ("ids", "wts", "step", "extra"):
        argument[name] = argument[name].T
    dims = types.SimpleNamespace(
        n_ep=n_ep, tp=tp, rows=rows, cap=cap, ratio=heads // groups, quarter=quarter, heads=heads,
        groups=groups, width=width, ff=ff, sff=sff,
        fetched=FETCHED,
    )
    f32, bf16 = jnp.float32, jnp.bfloat16
    scratch = dict(("v_" + n, pltpu.VMEM(argument[n].shape, argument[n].dtype)) for n in FETCHED)
    vmem = dict(
        tok=((n_ep, tp, rows, quarter), bf16),
        hid=((nz, tp, 4 * cap, ff), bf16),
        mix=((tp, rows, width), bf16),
        share=((tp, rows, sff), bf16),
        route=((n_ep, 2 * TOP_K, rows), f32),
        halo_x=((HALO, width), bf16),
        halo_b=((HALO, state_width), bf16),
        halo_c=((HALO, state_width), bf16),
        padded=((8 + rows, LANES), f32),
        vals=((rows, width), bf16),
        inm=((rows, state_width), bf16),
        outm=((rows, state_width), bf16),
        cum=((rows, heads), f32),
        cum_t=((heads, rows), f32),
        step_t=((heads, rows), f32),
        growth=((rows, width), f32),
        to_end=((rows, width), f32),
        state=((STATE, width), f32),
        state_out=((STATE, width), bf16),
        state_in=((STATE, width), bf16),
        decay_out=((8, width), f32),
        decay_in=((8, width), f32),
        before=((STATE, width // 2), bf16),
        after=((STATE, width // 2), bf16),
        incoming=((2, STATE, width // 2), bf16),
        entering=((STATE, width), bf16),
        near=((rows, width), f32),
        earlier=((rows, rows), bf16),
        pick=((nz, 2, 2 * cap, rows), bf16),
        amount=((nz, 2, 2 * cap, LANES), f32),
        arrived=((2, 2 * cap, model_width), bf16),
        result=((2, 2 * cap, quarter), bf16),
        yours=((nz, rows, quarter), bf16),
        theirs=((nz, rows, quarter), bf16),
        ours=((nz, rows, quarter), f32),
        going=((nz, rows, quarter), bf16),
        coming=((nz, rows, quarter), bf16),
        passed=((rows, quarter), bf16),
        routed_bf=((rows, quarter), bf16),
        mixer_bf=((rows, quarter), bf16),
        routed_sum=((rows, quarter), f32),
        mixer_sum=((rows, quarter), f32),
    )
    for name, (shape, dtype) in vmem.items():
        scratch[name] = pltpu.VMEM(shape, dtype)
    sems = dict(
        local_sem=(len(FETCHED),),
        out_sem=(2,),
        tok_send=(), tok_recv=(nz, 2), hid_send=(), hid_recv=(nz, 3),
        mix_send=(), mix_recv=(5,), pair_send=(), pair_recv=(nz,),
        z_send=(nz, 2), z_recv=(nz, 3), share_send=(), share_recv=(3,), route_send=(), route_recv=(n_ep,),
        halo_send=(3,), halo_recv=(3,), swap_send=(2,), swap_recv=(2,),
        chain_sem=(2,), half_sem=(2,), passed_sem=(),
        pair_y_send=(), pair_y_recv=(nz,), y_send=(), y_recv=(nz,),
    )
    for name, shape in sems.items():
        scratch[name] = pltpu.SemaphoreType.DMA(shape)
    order = tuple(FETCHED)
    names = order + ("mixer_out", "routed_out") + tuple(scratch)
    out = jax.ShapeDtypeStruct((rows, quarter), bf16)
    return hand_out(
        *pl.pallas_call(
            functools.partial(body, dims, names),
            out_shape=(out, out),
            in_specs=[pl.BlockSpec(memory_space=pl.ANY)] * len(order),
            out_specs=(pl.BlockSpec(memory_space=pl.ANY),) * 2,
            scratch_shapes=list(scratch.values()),
            compiler_params=pltpu.CompilerParams(
                collective_id=0, has_side_effects=True, vmem_limit_bytes=VMEM_LIMIT
            ),
            name="mixer_and_experts",
        )(*[argument[n] for n in order])
    )


VMEM_LIMIT = 62 * 1024 * 1024 + 512 * 1024
ARGUMENTS = (
    "x", "b", "c", "gate", "step", "extra", "hld", "skip", "vk", "bk", "ck", "mscale", "wm",
    "rows", "scale", "ids", "wts", "wg", "wu", "wd", "sg", "su", "sd",
)
FETCHED = (
    "rows", "scale", "ids", "wts", "x", "b", "c", "sg", "su", "vk", "bk", "ck", "step", "extra", "hld",
    "wg", "wu", "gate", "skip", "mscale", "wd", "sd", "wm",
)


def choose(*given):
    argument = dict(zip(ARGUMENTS, given))
    n_ep, tp = lax.axis_size("ep"), lax.axis_size("tp")
    rows = argument["rows"].shape[0]
    experts = argument["wg"].shape[0]
    cap = max(2, 3 * rows * TOP_K // (2 * experts * n_ep))
    wide = all(argument[n].shape[-1] % LANES == 0 for n in ("x", "b", "wg", "wd", "sg"))
    fits = tp == 4 and n_ep % 2 == 0 and n_ep >= 8 and experts == 2
    fits = fits and wide and cap % 16 == 0 and rows % 32 == 0
    return fused_on_device(*given) if fits else on_device(*given)


def solution(mesh):
    return jax.shard_map(
        choose,
        mesh=mesh,
        in_specs=(
            P("ep", "tp"),
            P("ep", "tp"),
            P("ep", "tp"),
            P("ep", "tp"),
            P("ep", "tp"),
            P("ep", "tp"),
            P("tp"),
            P("tp"),
            P(None, "tp"),
            P(None, "tp"),
            P(None, "tp"),
            P("tp"),
            P(None, "tp"),
            P("ep", None),
            P(),
            P("ep", None),
            P("ep", None),
            P("ep", None, "tp"),
            P("ep", None, "tp"),
            P("ep", None, "tp"),
            P(None, "tp"),
            P(None, "tp"),
            P(None, "tp"),
        ),
        out_specs=(P("ep", "tp"), P("ep", "tp")),
        check_vma=False,
    )
```

```python
import functools
import types

import jax
import jax.numpy as jnp
from jax import lax
from jax.experimental import pallas as pl
from jax.experimental.pallas import tpu as pltpu
from jax.sharding import PartitionSpec as P

HEAD_DIM = 64
STATE = 128
CONV_TAPS = 4
BLOCK = 128
TOP_K = 4


epsilon = 1e-05
precise = lax.Precision.HIGHEST


def passed_along(x, axis, by):
    size = lax.axis_size(axis)
    pairs = [(i, i + by) for i in range(size) if 0 <= i + by < size]
    return lax.ppermute(x, axis, pairs)


def carried_in(total_log, state, axis):
    size = lax.axis_size(axis)
    place = lax.axis_index(axis)
    log = passed_along(total_log, axis, 1)
    hold = passed_along(state.astype(jnp.bfloat16), axis, 1).astype(jnp.float32)
    by = 1
    while by < size - 1:
        before = passed_along(hold.astype(jnp.bfloat16), axis, by).astype(jnp.float32)
        hold = hold + jnp.exp(log)[:, None, None] * before
        log = log + passed_along(log, axis, by)
        by *= 2
    return hold


def conv_silu(tail_rows, source, weights):
    length = source.shape[0]
    padded = jnp.concatenate([tail_rows, source], axis=0)
    total_sum = jnp.zeros(source.shape, jnp.float32)
    for tap_index in range(CONV_TAPS):
        total_sum = (
            total_sum
            + padded[tap_index : tap_index + length].astype(jnp.float32) * weights[tap_index]
        )
    return jax.nn.silu(total_sum).astype(jnp.bfloat16)


def carry_blocks(carried, inputs):
    block_decay, block_state = inputs
    return (carried * block_decay[:, None, None] + block_state, carried)


def earlier_counts(mask, rows):
    at = jnp.arange(rows)
    tri = (at[:, None] < at[None, :]).astype(jnp.bfloat16)
    return lax.dot_general(
        mask.astype(jnp.bfloat16),
        tri,
        (((mask.ndim - 1,), (0,)), ((), ())),
        preferred_element_type=jnp.float32,
    )


def on_device(
    mixer_value_input,
    input_state_matrix,
    output_state_matrix,
    output_gate_input,
    step_input,
    extra_log_decay,
    head_log_decay,
    head_skip_scale,
    value_kernel,
    input_matrix_kernel,
    output_matrix_kernel,
    mixer_norm_scale,
    mixer_output_weight,
    second_token_rows,
    expert_norm_scale,
    routed_expert_index,
    routed_expert_weight,
    routed_gate_weight,
    routed_up_weight,
    routed_down_weight,
    shared_gate_weight,
    shared_up_weight,
    shared_down_weight,
):
    length = mixer_value_input.shape[0]
    heads_local = step_input.shape[1]
    width_x = mixer_value_input.shape[1]
    width_b = input_state_matrix.shape[1]
    groups_local = width_b // STATE
    head_ratio = heads_local // groups_local
    nblocks = length // BLOCK
    lead_row = length - CONV_TAPS + 1
    edge_rows = jnp.concatenate(
        [
            mixer_value_input[lead_row:],
            input_state_matrix[lead_row:],
            output_state_matrix[lead_row:],
        ],
        axis=1,
    )
    tail_rows = passed_along(edge_rows, "ep", 1)
    rows_local = second_token_rows.shape[0]
    model_width = second_token_rows.shape[1]
    local_experts = routed_gate_weight.shape[0]
    ep_count = lax.axis_size("ep")
    experts = local_experts * ep_count
    capacity = max(2, 3 * rows_local * TOP_K // (2 * experts))
    col_width = model_width // lax.axis_size("tp")
    rows_wide = second_token_rows.astype(jnp.float32)
    normed = (
        rows_wide
        * lax.rsqrt(jnp.mean(rows_wide * rows_wide, axis=-1, keepdims=True) + epsilon)
        * expert_norm_scale
    ).astype(jnp.bfloat16)
    ids = routed_expert_index.T.astype(jnp.float32)
    id_rows = -(-ids.size // col_width)
    id_block = jnp.pad(
        ids.astype(jnp.bfloat16).reshape(-1), (0, id_rows * col_width - ids.size)
    ).reshape(id_rows, col_width)
    id_block = jnp.pad(id_block, ((0, -id_rows % 8), (0, 0)))
    my_columns = lax.dynamic_slice_in_dim(normed, lax.axis_index("tp") * col_width, col_width, 1)
    outgoing, value_rows, in_rows, out_rows = lax.optimization_barrier(
        (
            jnp.concatenate([my_columns, id_block], axis=0),
            mixer_value_input,
            input_state_matrix,
            output_state_matrix,
        )
    )
    everyone = lax.all_gather(outgoing, "ep", axis=0)
    values = conv_silu(tail_rows[:, :width_x], value_rows, value_kernel)
    in_mat = conv_silu(
        tail_rows[:, width_x : width_x + width_b], in_rows, input_matrix_kernel
    )
    out_mat = conv_silu(
        tail_rows[:, width_x + width_b :], out_rows, output_matrix_kernel
    )
    step_length = jax.nn.softplus(step_input)
    decay_logarithm = -jnp.exp(head_log_decay)[None, :] * step_length + extra_log_decay
    running = jnp.cumsum(decay_logarithm.reshape(nblocks, BLOCK, heads_local), axis=1)
    value_wide = values.astype(jnp.float32).reshape(nblocks, BLOCK, heads_local, HEAD_DIM)
    scaled = value_wide * step_length.reshape(nblocks, BLOCK, heads_local)[..., None]
    in_blocks = in_mat.reshape(nblocks, BLOCK, groups_local, STATE)
    out_blocks = out_mat.reshape(nblocks, BLOCK, groups_local, STATE)
    scores = jnp.einsum(
        "bign,bjgn->bgij", out_blocks, in_blocks, preferred_element_type=jnp.float32
    )
    scores = jnp.repeat(scores, head_ratio, axis=1)
    spread = jnp.transpose(running[:, :, None, :] - running[:, None, :, :], (0, 3, 1, 2))
    lower_mask = jnp.tril(jnp.ones((BLOCK, BLOCK), bool))[None, None]
    decay_mat = jnp.where(lower_mask, jnp.exp(jnp.where(lower_mask, spread, 0.0)), 0.0)
    inside = jnp.einsum("bhij,bjhp->bihp", scores * decay_mat, scaled, precision=precise)
    out_head = jnp.repeat(out_blocks.astype(jnp.float32), head_ratio, axis=2)
    in_head = jnp.repeat(in_blocks.astype(jnp.float32), head_ratio, axis=2)
    block_logs = running[:, -1]
    to_end = jnp.exp(block_logs[:, None, :] - running)
    block_state = jnp.einsum("bjhn,bjh,bjhp->bhpn", in_head, to_end, scaled, precision=precise)
    start_state = jnp.zeros((heads_local, HEAD_DIM, STATE), jnp.float32)
    local_total, local_prev = lax.scan(
        carry_blocks, start_state, (jnp.exp(block_logs), block_state)
    )
    before_logs = jnp.cumsum(block_logs, axis=0) - block_logs
    everyone, local_total = lax.optimization_barrier((everyone, local_total))
    incoming = carried_in(jnp.sum(block_logs, axis=0), local_total, "ep")
    their_rows = everyone[:, :rows_local]
    their_ids = everyone[:, rows_local : rows_local + id_rows].reshape(ep_count, -1)
    their_ids = their_ids[:, : ids.size].reshape(ep_count, TOP_K, rows_local).astype(jnp.float32)
    mine = (lax.axis_index("ep") * local_experts + jnp.arange(local_experts)).astype(jnp.float32)
    named = jnp.any(their_ids[:, None] == mine[None, :, None, None], axis=2)
    seat = jnp.where(named, earlier_counts(named, rows_local), -1.0)
    seats = jnp.arange(capacity, dtype=jnp.float32)
    pick = (seat[:, :, None, :] == seats[None, None, :, None]).astype(jnp.bfloat16)
    arrived = jnp.stack(
        [
            jnp.einsum(
                "bsr,brd->bsd", pick[:, j], their_rows, preferred_element_type=jnp.float32
            )
            .astype(jnp.bfloat16)
            .reshape(ep_count * capacity, col_width)
            for j in range(local_experts)
        ]
    )
    column_piece = lax.all_gather(arrived, "tp", axis=2, tiled=True)
    column_piece, incoming = lax.optimization_barrier((column_piece, incoming))
    entering = local_prev + jnp.exp(before_logs)[:, :, None, None] * incoming[None]
    carried_term = (
        jnp.einsum("bihn,bhpn->bihp", out_head, entering, precision=precise)
        * jnp.exp(running)[..., None]
    )
    mixed_heads = (inside + carried_term).reshape(length, heads_local, HEAD_DIM)
    mixed_heads = mixed_heads + head_skip_scale[None, :, None] * value_wide.reshape(
        length, heads_local, HEAD_DIM
    )
    gated_heads = mixed_heads * jax.nn.silu(output_gate_input.astype(jnp.float32)).reshape(
        length, heads_local, HEAD_DIM
    )
    grouped = gated_heads.reshape(length, groups_local, head_ratio * HEAD_DIM)
    grouped = grouped * lax.rsqrt(jnp.mean(grouped * grouped, axis=-1, keepdims=True) + epsilon)
    mixer_normed = (grouped.reshape(length, width_x) * mixer_norm_scale).astype(jnp.bfloat16)
    gate_pre = jnp.einsum(
        "esd,edf->esf", column_piece, routed_gate_weight, preferred_element_type=jnp.float32
    )
    up_pre = jnp.einsum(
        "esd,edf->esf", column_piece, routed_up_weight, preferred_element_type=jnp.float32
    )
    hidden = (jax.nn.silu(gate_pre) * up_pre).astype(jnp.bfloat16)
    shared_hidden = (
        jax.nn.silu(jnp.dot(normed, shared_gate_weight, preferred_element_type=jnp.float32))
        * jnp.dot(normed, shared_up_weight, preferred_element_type=jnp.float32)
    ).astype(jnp.bfloat16)
    whole_hidden = lax.all_gather(hidden, "tp", axis=2, tiled=True)
    both = lax.all_gather(
        jnp.concatenate([mixer_normed, shared_hidden], axis=1), "tp", axis=1, tiled=True
    ).reshape(length, lax.axis_size("tp"), -1)
    whole_mix = both[:, :, :width_x].reshape(length, -1)
    whole_shared = both[:, :, width_x:].reshape(length, -1)
    mixer_output = jnp.dot(
        whole_mix, mixer_output_weight, preferred_element_type=jnp.float32
    ).astype(jnp.bfloat16)
    expert_result = jnp.einsum(
        "esf,efd->esd", whole_hidden, routed_down_weight, preferred_element_type=jnp.float32
    ).astype(jnp.bfloat16)
    going = jnp.concatenate(
        [expert_result[j].reshape(ep_count, capacity, col_width) for j in range(local_experts)],
        axis=1,
    )
    returned = lax.all_to_all(going, "ep", split_axis=0, concat_axis=0, tiled=True)
    returned = returned.reshape(experts * capacity, col_width)
    kinds = jnp.arange(experts, dtype=jnp.float32)
    chosen = ids[:, None, :] == kinds[None, :, None]
    count = earlier_counts(jnp.any(chosen, axis=0), rows_local)
    position = jnp.sum(jnp.where(chosen, count[None], 0.0), axis=1)
    slot = (ids * capacity + position).T.astype(jnp.int32)
    columns = jnp.arange(experts * capacity, dtype=jnp.int32)[None, :]
    spread = jnp.zeros((rows_local, experts * capacity), jnp.float32)
    for k in range(TOP_K):
        spread = spread + jnp.where(
            slot[:, k : k + 1] == columns, routed_expert_weight[:, k : k + 1], 0.0
        )
    high = lax.reduce_precision(spread, 8, 7)
    low = (spread - high).astype(jnp.bfloat16)
    routed_sum = jnp.dot(
        high.astype(jnp.bfloat16), returned, preferred_element_type=jnp.float32
    ) + jnp.dot(low, returned, preferred_element_type=jnp.float32)
    shared_result = jnp.dot(whole_shared, shared_down_weight, preferred_element_type=jnp.float32)
    routed_out = (routed_sum + shared_result).astype(jnp.bfloat16)
    return (mixer_output, routed_out)


MESH = pl.DeviceIdType.MESH
HALO = 16
LANES = 128


def silu(v):
    return v / (1.0 + jnp.exp(-v))


def dot(a, b, contract=((1,), (0,)), exact=False):
    return lax.dot_general(
        a,
        b,
        (contract, ((), ())),
        precision=precise if exact else None,
        preferred_element_type=jnp.float32,
    )


def iota(shape, axis):
    return lax.broadcasted_iota(jnp.int32, shape, axis)


def at(start, size):
    return pl.ds(pl.multiple_of(start, size), size)


def body(dims, names, *refs):
    r = types.SimpleNamespace(**dict(zip(names, refs)))
    n_ep, rows, cap, ratio = dims.n_ep, dims.rows, dims.cap, dims.ratio
    nz = n_ep // 2
    half = rows // 2
    tp = dims.tp
    quarter = dims.quarter
    heads, groups, width = dims.heads, dims.groups, dims.width
    band = ratio * HEAD_DIM
    ff, sff = dims.ff, dims.sff
    f32, bf16 = jnp.float32, jnp.bfloat16

    e, t = lax.axis_index("ep"), lax.axis_index("tp")
    z, c = lax.div(e, 2), lax.rem(e, 2)
    other = 1 - c
    partner = e + 1 - 2 * c
    tx = t + 1 - 2 * lax.rem(t, 2)
    ty = lax.rem(t + 2, tp)
    td = tp - 1 - t

    def remote(src, dst, send, recv, to):
        return pltpu.make_async_remote_copy(
            src_ref=src, dst_ref=dst, send_sem=send, recv_sem=recv, device_id=to, device_id_type=MESH
        )

    fetched = dims.fetched

    def fetch(name):
        return pltpu.make_async_copy(
            getattr(r, name), getattr(r, "v_" + name), r.local_sem.at[fetched.index(name)]
        )

    for name in fetched:
        fetch(name).start()

    def got(*wanted):
        for name in wanted:
            fetch(name).wait()

    barrier = pltpu.get_barrier_semaphore()
    for by in range(1, n_ep):
        pl.semaphore_signal(barrier, inc=1, device_id=(lax.rem(e + by, n_ep), t), device_id_type=MESH)
    for to in (tx, ty):
        pl.semaphore_signal(barrier, inc=1, device_id=(e, to), device_id_type=MESH)

    longer = jnp.maximum(z, nz - 1 - z)
    inward = jnp.where(2 * z > nz - 1, -1, 1)

    def zsource(k):
        return jnp.where(k <= longer, z + inward * k, z - inward * (k - longer))

    def sent(ref, sem):
        remote(ref, ref, sem, sem, (partner, t)).wait_send()

    def landed(ref, sem):
        remote(ref, ref, sem, sem, (partner, t)).wait_recv()

    def plane(buf, send, recv):
        def leg(q, piece, slot, to):
            return remote(buf(q, piece), buf(q, piece), send, recv(slot), (e, to))

        def lead():
            leg(t, 0, 0, tx).start()
            leg(t, 1, 1, ty).start()

        def follow():
            leg(t, 1, 2, tx).start()
            leg(t, 0, 3, ty).start()

        def start():
            lead()
            follow()

        def relay():
            leg(tx, 0, 0, tx).wait_recv()
            leg(tx, 0, 4, ty).start()
            leg(ty, 1, 1, ty).wait_recv()
            leg(ty, 1, 5, tx).start()

        return types.SimpleNamespace(start=start, lead=lead, follow=follow, relay=relay)

    def token_leg(source, q, piece, slot, to):
        ref = r.tok.at[2 * source + c, q, pl.ds(piece * half, half)]
        return remote(ref, ref, r.tok_send, r.tok_recv.at[source, slot], (e, to))

    def token_legs(source, piece):
        return token_leg(source, t, piece, 0, tx), token_leg(source, t, piece, 1, ty)

    def hiddens(k):
        return plane(
            lambda q, piece: r.hid.at[k, q, pl.ds(piece * 2 * cap, 2 * cap)],
            r.hid_send,
            lambda slot: r.hid_recv.at[k, min(slot, 2)],
        )

    shares = plane(
        lambda q, piece: r.share.at[q, pl.ds(piece * half, half)],
        r.share_send,
        lambda slot: r.share_recv.at[min(slot, 2)],
    )
    mixes = plane(
        lambda q, piece: r.mix.at[q, pl.ds(piece * half, half)],
        r.mix_send,
        lambda slot: r.mix_recv.at[min(slot, 4)],
    )

    def across(source, q, whose):
        ref = r.tok.at[2 * source + whose, q]
        return remote(ref, ref, r.pair_send, r.pair_recv.at[source], (partner, t))

    def along(source, slot, up):
        block = 2 * source + c
        ref = r.tok.at[block, td] if slot == 2 else r.tok.at[block, t, pl.ds(slot * half, half)]
        to = 2 * (z - 1 + 2 * up) + c
        return remote(ref, ref, r.z_send.at[source, up], r.z_recv.at[source, slot], (to, t))

    def onward(up):
        to = z - 1 + 2 * up
        return jnp.logical_and(to >= 0, to < nz)

    def sides(s, act):
        for way in (1, -1):
            source = z + way * inward * s

            @pl.when(jnp.logical_and(source >= 0, source < nz))
            def _(source=source, way=way):
                act(source, lax.div(1 - way * inward, 2), way)

    def pass_on(source, slot, up):
        along(source, slot, 1 - up).wait_recv()

        @pl.when(onward(up))
        def _():
            along(source, slot, up).start()

    def near_piece(piece, source, up, way):
        pass_on(source, piece, up)
        if way > 0:
            for one in token_legs(source, piece):
                one.start()

    def near_rest(source, up, way):
        near_piece(1, source, up, way)
        if way > 0:
            across(source, t, c).start()

    def near_part(source, up, way):
        near_piece(0, source, up, way)
        near_rest(source, up, way)

    def late_legs(k):
        source = zsource(k)

        @pl.when(jnp.logical_and(k > longer, k < nz))
        def _():
            for piece in range(2):
                for one in token_legs(source, piece):
                    one.start()
            across(source, t, c).start()

    def far_part(source, up, way):
        pass_on(source, 2, up)
        across(source, td, c).start()

    def route_to(to):
        ref = r.route.at[e]
        return remote(ref, ref, r.route_send, r.route_recv.at[e], (to, t))

    def route_from(source):
        ref = r.route.at[source]
        return remote(ref, ref, r.route_send, r.route_recv.at[source], (e, t))

    edges = ((r.v_x, r.halo_x), (r.v_b, r.halo_b), (r.v_c, r.halo_c))

    def halo(i):
        src, dst = edges[i]
        return remote(
            src.at[pl.ds(rows - HALO, HALO)], dst, r.halo_send.at[i], r.halo_recv.at[i], (lax.rem(e + 1, n_ep), t)
        )

    got("rows", "scale")
    step_rows = 16

    def norm_rows(i, _):
        part = r.v_rows[at(i * step_rows, step_rows), :].astype(f32)
        by = lax.rsqrt(jnp.mean(part * part, axis=-1, keepdims=True) + epsilon)
        part = (part * by * r.v_scale[...]).astype(bf16)
        for q in range(tp):
            r.tok[e, q, at(i * step_rows, step_rows), :] = part[:, q * quarter : (q + 1) * quarter]
        return 0

    lax.fori_loop(0, rows // step_rows, norm_rows, 0, unroll=4)
    got("ids", "wts")
    below = iota((rows, rows), 0)
    right = iota((rows, rows), 1)
    r.earlier[...] = (below < right).astype(bf16)
    r.route[e, 0:TOP_K, :] = r.v_ids[...].astype(f32)
    r.route[e, TOP_K : 2 * TOP_K, :] = r.v_wts[...]
    got("x", "b", "c")
    pl.semaphore_wait(barrier, n_ep - 1 + 2)

    @pl.when(e + 1 < n_ep)
    def _():
        for i in range(3):
            halo(i).start()

    route_to(partner).start()
    for slot in range(3):
        for up in (1, 0):

            @pl.when(onward(up))
            def _():
                along(z, slot, up).start()

    for q in range(tp):
        across(z, q, c).start()
    for by in range(1, n_ep):
        to = lax.rem(e + by, n_ep)

        @pl.when(to != partner)
        def _(to=to):
            route_to(to).start()

    got("sg", "su")
    gate, up = 0.0, 0.0
    for q in range(tp):
        part = r.tok[e, q]
        gate = gate + dot(part, r.v_sg[q * quarter : (q + 1) * quarter, :])
        up = up + dot(part, r.v_su[q * quarter : (q + 1) * quarter, :])
    r.share[t] = (silu(gate) * up).astype(bf16)
    shares.start()

    def enter(k):
        source = zsource(k)
        seats = iota((cap, rows), 0).astype(f32)
        for c2 in range(2):
            block = 2 * source + c2
            ids = r.route[block, 0:TOP_K, :]
            weights = r.route[block, TOP_K : 2 * TOP_K, :]
            for j in range(2):
                hit = ids == (2 * e + j).astype(f32)
                named = jnp.sum(jnp.where(hit, 1.0, 0.0), axis=0, keepdims=True)
                given = jnp.sum(jnp.where(hit, weights, 0.0), axis=0, keepdims=True)
                count = dot(jnp.broadcast_to(named, (16, rows)).astype(bf16), r.earlier[...])
                seat = jnp.where(named > 0.0, count[0:1, :], -1.0)
                taken = seats == seat
                r.pick[k, c2, j * cap : (j + 1) * cap, :] = jnp.where(taken, 1.0, 0.0).astype(bf16)
                amount = jnp.sum(jnp.where(taken, given, 0.0), axis=1, keepdims=True)
                r.amount[k, j, c2 * cap : (c2 + 1) * cap, :] = jnp.broadcast_to(amount, (cap, LANES))
            for q in range(tp):
                chosen = dot(r.pick[k, c2], r.tok[block, q]).astype(bf16)
                for j in range(2):
                    r.arrived[j, c2 * cap : (c2 + 1) * cap, q * quarter : (q + 1) * quarter] = chosen[
                        j * cap : (j + 1) * cap, :
                    ]
        for j in range(2):
            gate = dot(r.arrived[j], r.v_wg[j])
            up = dot(r.arrived[j], r.v_wu[j])
            r.hid[k, t, j * 2 * cap : (j + 1) * 2 * cap, :] = (silu(gate) * up).astype(bf16)

    @pl.when(e > 0)
    def _():
        for i in range(3):
            halo(i).wait_recv()

    @pl.when(e == 0)
    def _():
        for _, dst in edges:
            dst[...] = jnp.zeros_like(dst)

    got("vk", "bk", "ck", "step", "extra", "hld")

    def conv(src, edge, taps, out):
        def chunk(i, _):
            lanes = at(i * LANES, LANES)
            r.padded[0:8, :] = edge[:, lanes].astype(f32)[HALO - 8 :]
            r.padded[8 : 8 + rows, :] = src[:, lanes].astype(f32)
            total = jnp.zeros((rows, LANES), f32)
            for k in range(CONV_TAPS):
                lead = 8 - CONV_TAPS + 1 + k
                total = total + r.padded[lead : lead + rows, :] * taps[k : k + 1, lanes]
            out[:, lanes] = silu(total).astype(bf16)
            return 0

        lax.fori_loop(0, src.shape[1] // LANES, chunk, 0)

    conv(r.v_x, r.halo_x, r.v_vk, r.vals)
    conv(r.v_b, r.halo_b, r.v_bk, r.inm)
    conv(r.v_c, r.halo_c, r.v_ck, r.outm)
    route_from(partner).wait_recv()
    got("wg", "wu")
    landed(r.tok.at[2 * z + other], r.pair_recv.at[z])
    enter(0)
    hiddens(0).start()
    shares.relay()
    sides(1, functools.partial(near_piece, 0))
    pre = r.v_step[...]
    steps = jnp.maximum(pre, 0.0) + jnp.log(1.0 + jnp.exp(-jnp.abs(pre)))
    diagonal = iota((heads, heads), 0) == iota((heads, heads), 1)
    rate = jnp.sum(jnp.where(diagonal, jnp.exp(r.v_hld[...]), 0.0), axis=1, keepdims=True)
    decay = -rate * steps + r.v_extra[...]
    upto = (below <= right).astype(f32)
    cum_t = dot(decay, upto, exact=True)
    cum = dot((right <= below).astype(f32), decay, ((1,), (1,)), exact=True)
    r.cum[...] = cum
    r.cum_t[...] = cum_t
    r.step_t[...] = steps
    spread_heads = (lax.div(iota((heads, width), 1), HEAD_DIM) == iota((heads, width), 0)).astype(f32)
    r.growth[...] = dot(jnp.exp(cum), spread_heads, exact=True)
    to_end = jnp.exp(cum_t[:, rows - 1 : rows] - cum_t) * steps
    r.to_end[...] = dot(to_end, spread_heads, ((0,), (0,)), exact=True)
    for g in range(groups):
        lanes = pl.ds(g * band, band)
        weighted = (r.vals[:, lanes].astype(f32) * r.to_end[:, lanes]).astype(bf16)
        r.state[:, lanes] = dot(r.inm[:, g * STATE : (g + 1) * STATE], weighted, ((0,), (0,)))
    r.state_out[...] = r.state[...].astype(bf16)
    r.decay_out[...] = jnp.broadcast_to(r.growth[rows - 1 : rows, :], (8, width))

    def swap(i):
        src, dst = ((r.state_out, r.state_in), (r.decay_out, r.decay_in))[i]
        return remote(src, dst, r.swap_send.at[i], r.swap_recv.at[i], (partner, t))

    for i in range(2):
        swap(i).start()
    side = width // 2
    mine_lanes = at(c * side, side)

    def chain(up):
        to = 2 * (z + up) + c
        return remote(r.after, r.before, r.chain_sem.at[0], r.chain_sem.at[1], (to, t))

    def halves(whose):
        ref = r.incoming.at[whose]
        return remote(ref, ref, r.half_sem.at[0], r.half_sem.at[1], (partner, t))

    def chain_step():
        for i in range(2):
            swap(i).wait_recv()
        ours, theirs = r.state[:, mine_lanes], r.state_in[:, mine_lanes].astype(f32)
        our_decay, their_decay = r.decay_out[:, mine_lanes], r.decay_in[:, mine_lanes]
        first = jnp.where(c == 0, ours, theirs)
        second = jnp.where(c == 0, theirs, ours)
        late = jnp.where(c == 0, their_decay, our_decay)
        chip = late[0:1, :] * first + second

        @pl.when(z == 0)
        def _():
            r.before[...] = jnp.zeros_like(r.before)

        @pl.when(z > 0)
        def _():
            chain(0).wait_recv()

        r.incoming[c] = r.before[...]
        halves(c).start()

        @pl.when(onward(1))
        def _():
            both = our_decay[0:1, :] * their_decay[0:1, :]
            r.after[...] = (both * r.before[...].astype(f32) + chip).astype(bf16)
            chain(1).start()

    def inside():
        mid = rows // 2
        lane = iota((mid, 2 * HEAD_DIM), 1) < HEAD_DIM
        for g in range(groups):
            cols = slice(g * STATE, (g + 1) * STATE)
            for part in range(2):
                span = slice(part * mid, (part + 1) * mid)
                reach = (part + 1) * mid
                scores = dot(r.outm[span, cols], r.inm[0:reach, cols], ((1,), (1,)))
                mask = iota((mid, reach), 0) + part * mid >= iota((mid, reach), 1)
                for p in range(ratio // 2):
                    pair = []
                    head = g * ratio + 2 * p
                    lanes = slice(head * HEAD_DIM, (head + 2) * HEAD_DIM)
                    for h in (head, head + 1):
                        diff = r.cum[span, h : h + 1] - r.cum_t[h : h + 1, 0:reach]
                        grid = scores * jnp.exp(jnp.where(mask, diff, -1e30)) * r.step_t[h : h + 1, 0:reach]
                        pair.append(dot(grid.astype(bf16), r.vals[0:reach, lanes]))
                    r.near[span, lanes] = jnp.where(lane, pair[0], pair[1])

    def back_pair(k):
        return remote(r.yours.at[k], r.theirs.at[k], r.pair_y_send, r.pair_y_recv.at[k], (partner, t))

    def back(k):
        source = zsource(k)
        return remote(r.going.at[k], r.coming.at[z], r.y_send, r.y_recv.at[z], (2 * source + c, t))

    def back_in(source):
        return remote(r.going.at[0], r.coming.at[source], r.y_send, r.y_recv.at[source], (e, t))

    def leave(k, carry=0):
        landed(r.hid.at[k, 0:2], r.hid_recv.at[k, 2])
        for j in range(2):
            total = 0.0
            for q in range(tp):
                total = total + dot(
                    r.hid[k, q, j * 2 * cap : (j + 1) * 2 * cap, :], r.v_wd[j, q * ff : (q + 1) * ff, :]
                )
            total = (total * r.amount[k, j, :, 0:1]).astype(bf16)
            for c2 in range(2):
                r.result[c2, j * cap : (j + 1) * cap, :] = total[c2 * cap : (c2 + 1) * cap, :]
        r.yours[k] = dot(r.pick[k, other], r.result[other], ((0,), (0,))).astype(bf16)
        back_pair(k).start()
        r.ours[k] = dot(r.pick[k, c], r.result[c], ((0,), (0,)))
        return carry

    edge = jnp.logical_or(z == 0, z == nz - 1)
    second = jnp.logical_or(z == 1, z == nz - 2)

    def passing():
        to = 2 * (z + inward) + c
        return remote(r.going.at[2], r.passed, r.y_send, r.passed_sem, (to, t))

    def send_back(k, carry=0):
        @pl.when(jnp.logical_not(jnp.logical_and(k == 1, second)))
        def _():
            back_pair(k).wait_recv()
            r.going[k] = (r.ours[k] + r.theirs[k].astype(f32)).astype(bf16)
            aside = jnp.logical_and(k == 2, edge)

            @pl.when(aside)
            def _():
                passing().start()

            @pl.when(jnp.logical_not(aside))
            def _():
                back(k).start()

        return carry

    def join_back():
        @pl.when(second)
        def _():
            back_pair(1).wait_recv()
            landed(r.passed, r.passed_sem)
            total = r.ours[1] + r.theirs[1].astype(f32) + r.passed[...].astype(f32)
            r.going[1] = total.astype(bf16)
            back(1).start()


    sides(1, near_rest)

    @pl.when(z == 0)
    def _():
        chain_step()

    hiddens(0).relay()

    def stage(k, _):
        source = zsource(k)

        sides(k, far_part)

        @pl.when(k == 1)
        def _():
            inside()

        @pl.when(k == 2)
        def _():
            got("wd")

        @pl.when(k == nz - 1)
        def _():
            hiddens(k - 1).relay()

        for slot, q in ((0, tx), (1, ty)):
            landed(r.tok.at[2 * source + c, q], r.tok_recv.at[source, slot])
            across(source, q, c).start()
        for c2 in range(2):
            route_from(2 * source + c2).wait_recv()

        @pl.when(k != nz - 2)
        def _():
            sides(k + 1, near_part)

        @pl.when(k == z)
        def _():
            chain_step()

        landed(r.tok.at[2 * source + other], r.pair_recv.at[source])
        enter(k)
        hiddens(k).lead()

        @pl.when(k == nz - 2)
        def _():
            sides(k + 1, near_part)

        hiddens(k).follow()
        late_legs(k + 2)

        @pl.when(jnp.logical_and(k > 1, k < nz - 1))
        def _():
            hiddens(k - 1).relay()

        return 0

    lax.fori_loop(1, nz, stage, 0)

    got("gate", "skip", "mscale")

    def mixer_end():
        halves(other).wait_recv()
        spread_heads = (lax.div(iota((heads, width), 1), HEAD_DIM) == iota((heads, width), 0)).astype(f32)
        skip = dot(jnp.broadcast_to(r.v_skip[...], (8, heads)), spread_heads, exact=True)[0:1, :]
        for s in range(2):
            lanes = slice(s * side, (s + 1) * side)
            hold = r.incoming[s].astype(f32)
            later = r.decay_in[0:1, lanes] * hold + r.state_in[:, lanes].astype(f32)
            r.entering[:, lanes] = jnp.where(c == 0, hold, later).astype(bf16)
        for g in range(groups):
            lanes = slice(g * band, (g + 1) * band)
            far = dot(r.outm[:, g * STATE : (g + 1) * STATE], r.entering[:, lanes]) * r.growth[:, lanes]
            mixed = r.near[:, lanes] + far + skip[:, lanes] * r.vals[:, lanes].astype(f32)
            gated = mixed * silu(r.v_gate[:, lanes].astype(f32))
            by = lax.rsqrt(jnp.mean(gated * gated, axis=-1, keepdims=True) + epsilon)
            r.mix[t, :, lanes] = (gated * by * r.v_mscale[:, lanes]).astype(bf16)

    lax.fori_loop(1, nz - 1, lambda i, carry: leave(nz - 1 - i, carry), 0)
    send_back(nz - 2)
    mixer_end()
    lax.fori_loop(2, nz - 1, lambda i, carry: send_back(nz - 1 - i, carry), 0)
    hiddens(nz - 1).relay()
    mixes.start()
    leave(nz - 1)
    leave(0)
    join_back()
    send_back(nz - 1)
    got("sd", "wm")

    landed(r.share.at[0:2], r.share_recv.at[2])
    routed = 0.0
    for q in range(tp):
        routed = routed + dot(r.share[q], r.v_sd[q * sff : (q + 1) * sff, :])
    r.mixer_sum[...] = dot(r.mix[t], r.v_wm[at(t * width, width), :])
    mixes.relay()
    back_pair(0).wait_recv()
    r.routed_sum[...] = routed + r.ours[0] + r.theirs[0].astype(f32)

    def add_back(k, _):
        source = zsource(k)
        low = jnp.logical_and(source == 0, z == 2)
        high = jnp.logical_and(source == nz - 1, z == nz - 3)

        @pl.when(jnp.logical_not(jnp.logical_or(low, high)))
        def _():
            back_in(source).wait_recv()
            r.routed_sum[...] += r.coming[source].astype(f32)

        return 0

    def add_mix(q):
        r.mixer_sum[...] += dot(r.mix[q], r.v_wm[at(q * width, width), :])

    def outcopy(i):
        src, dst = ((r.mixer_bf, r.mixer_out), (r.routed_bf, r.routed_out))[i]
        return pltpu.make_async_copy(src, dst, r.out_sem.at[i])

    landed(r.mix.at[0, 0:half], r.mix_recv.at[2])
    add_mix(tx)
    landed(r.mix.at[0, 0:half], r.mix_recv.at[3])
    add_mix(ty)
    lax.fori_loop(1, nz, add_back, 0)
    r.routed_bf[...] = r.routed_sum[...].astype(bf16)
    outcopy(1).start()
    landed(r.mix.at[0], r.mix_recv.at[4])
    add_mix(td)
    r.mixer_bf[...] = r.mixer_sum[...].astype(bf16)
    outcopy(0).start()

    @pl.when(e + 1 < n_ep)
    def _():
        for i in range(3):
            halo(i).wait_send()

    sent(r.route.at[0 : n_ep - 1], r.route_send)
    for i in range(2):
        swap(i).wait_send()

    @pl.when(onward(1))
    def _():
        chain(1).wait_send()

    halves(c).wait_send()
    sent(r.mix.at[0:3], r.mix_send)
    sent(r.share.at[0:3], r.share_send)
    sent(r.hid.at[:, 0:3], r.hid_send)
    sent(r.tok.at[0 : nz - 1, 0:2], r.tok_send)
    sent(r.tok.at[0:nz], r.pair_send)
    sent(r.yours, r.pair_y_send)
    sent(r.going.at[0 : nz - 1], r.y_send)

    def drain(source, _):
        for up in range(2):
            passed = source <= z if up else source >= z

            @pl.when(jnp.logical_and(passed, onward(up)))
            def _():
                sent(r.tok.at[0, 0:2], r.z_send.at[source, up])

        return 0

    lax.fori_loop(0, nz, drain, 0)
    for i in range(2):
        outcopy(i).wait()


def hand_out_body(first, second, first_out, second_out, held, sems):
    steps = []
    for i, (src, dst) in enumerate(((first, first_out), (second, second_out))):
        steps.append(
            (
                pltpu.make_async_copy(src, held.at[i], sems.at[i, 0]),
                pltpu.make_async_copy(held.at[i], dst, sems.at[i, 1]),
            )
        )
    for arrive, _ in steps:
        arrive.start()
    for arrive, depart in steps:
        arrive.wait()
        depart.start()
    for _, depart in steps:
        depart.wait()


def hand_out(first, second):
    out = jax.ShapeDtypeStruct(first.shape, first.dtype)
    return tuple(
        pl.pallas_call(
            hand_out_body,
            out_shape=(out, out),
            in_specs=[pl.BlockSpec(memory_space=pl.ANY)] * 2,
            out_specs=(pl.BlockSpec(memory_space=pl.ANY),) * 2,
            scratch_shapes=[pltpu.VMEM((2,) + first.shape, first.dtype), pltpu.SemaphoreType.DMA((2, 2))],
            name="hand_out",
        )(first, second)
    )


def fused_on_device(*given):
    argument = dict(zip(ARGUMENTS, given))
    rows, model_width = argument["rows"].shape
    n_ep, tp = lax.axis_size("ep"), lax.axis_size("tp")
    nz = n_ep // 2
    heads = argument["step"].shape[1]
    width = argument["x"].shape[1]
    state_width = argument["b"].shape[1]
    groups = state_width // STATE
    local_experts, _, ff = argument["wg"].shape
    sff = argument["sg"].shape[1]
    quarter = argument["wd"].shape[2]
    cap = max(2, 3 * rows * TOP_K // (2 * local_experts * n_ep))
    for name in ("hld", "skip", "mscale", "scale"):
        argument[name] = argument[name].reshape(1, -1)
    for name in ("ids", "wts", "step", "extra"):
        argument[name] = argument[name].T
    dims = types.SimpleNamespace(
        n_ep=n_ep, tp=tp, rows=rows, cap=cap, ratio=heads // groups, quarter=quarter, heads=heads,
        groups=groups, width=width, ff=ff, sff=sff,
        fetched=FETCHED,
    )
    f32, bf16 = jnp.float32, jnp.bfloat16
    scratch = dict(("v_" + n, pltpu.VMEM(argument[n].shape, argument[n].dtype)) for n in FETCHED)
    vmem = dict(
        tok=((n_ep, tp, rows, quarter), bf16),
        hid=((nz, tp, 4 * cap, ff), bf16),
        mix=((tp, rows, width), bf16),
        share=((tp, rows, sff), bf16),
        route=((n_ep, 2 * TOP_K, rows), f32),
        halo_x=((HALO, width), bf16),
        halo_b=((HALO, state_width), bf16),
        halo_c=((HALO, state_width), bf16),
        padded=((8 + rows, LANES), f32),
        vals=((rows, width), bf16),
        inm=((rows, state_width), bf16),
        outm=((rows, state_width), bf16),
        cum=((rows, heads), f32),
        cum_t=((heads, rows), f32),
        step_t=((heads, rows), f32),
        growth=((rows, width), f32),
        to_end=((rows, width), f32),
        state=((STATE, width), f32),
        state_out=((STATE, width), bf16),
        state_in=((STATE, width), bf16),
        decay_out=((8, width), f32),
        decay_in=((8, width), f32),
        before=((STATE, width // 2), bf16),
        after=((STATE, width // 2), bf16),
        incoming=((2, STATE, width // 2), bf16),
        entering=((STATE, width), bf16),
        near=((rows, width), f32),
        earlier=((rows, rows), bf16),
        pick=((nz, 2, 2 * cap, rows), bf16),
        amount=((nz, 2, 2 * cap, LANES), f32),
        arrived=((2, 2 * cap, model_width), bf16),
        result=((2, 2 * cap, quarter), bf16),
        yours=((nz, rows, quarter), bf16),
        theirs=((nz, rows, quarter), bf16),
        ours=((nz, rows, quarter), f32),
        going=((nz, rows, quarter), bf16),
        coming=((nz, rows, quarter), bf16),
        passed=((rows, quarter), bf16),
        routed_bf=((rows, quarter), bf16),
        mixer_bf=((rows, quarter), bf16),
        routed_sum=((rows, quarter), f32),
        mixer_sum=((rows, quarter), f32),
    )
    for name, (shape, dtype) in vmem.items():
        scratch[name] = pltpu.VMEM(shape, dtype)
    sems = dict(
        local_sem=(len(FETCHED),),
        out_sem=(2,),
        tok_send=(), tok_recv=(nz, 2), hid_send=(), hid_recv=(nz, 3),
        mix_send=(), mix_recv=(5,), pair_send=(), pair_recv=(nz,),
        z_send=(nz, 2), z_recv=(nz, 3), share_send=(), share_recv=(3,), route_send=(), route_recv=(n_ep,),
        halo_send=(3,), halo_recv=(3,), swap_send=(2,), swap_recv=(2,),
        chain_sem=(2,), half_sem=(2,), passed_sem=(),
        pair_y_send=(), pair_y_recv=(nz,), y_send=(), y_recv=(nz,),
    )
    for name, shape in sems.items():
        scratch[name] = pltpu.SemaphoreType.DMA(shape)
    order = tuple(FETCHED)
    names = order + ("mixer_out", "routed_out") + tuple(scratch)
    out = jax.ShapeDtypeStruct((rows, quarter), bf16)
    return hand_out(
        *pl.pallas_call(
            functools.partial(body, dims, names),
            out_shape=(out, out),
            in_specs=[pl.BlockSpec(memory_space=pl.ANY)] * len(order),
            out_specs=(pl.BlockSpec(memory_space=pl.ANY),) * 2,
            scratch_shapes=list(scratch.values()),
            compiler_params=pltpu.CompilerParams(
                collective_id=0, has_side_effects=True, vmem_limit_bytes=VMEM_LIMIT
            ),
            name="mixer_and_experts",
        )(*[argument[n] for n in order])
    )


VMEM_LIMIT = 62 * 1024 * 1024 + 512 * 1024
ARGUMENTS = (
    "x", "b", "c", "gate", "step", "extra", "hld", "skip", "vk", "bk", "ck", "mscale", "wm",
    "rows", "scale", "ids", "wts", "wg", "wu", "wd", "sg", "su", "sd",
)
FETCHED = (
    "rows", "scale", "ids", "wts", "x", "b", "c", "sg", "su", "vk", "bk", "ck", "step", "extra", "hld",
    "wg", "wu", "gate", "skip", "mscale", "wd", "sd", "wm",
)


def choose(*given):
    argument = dict(zip(ARGUMENTS, given))
    n_ep, tp = lax.axis_size("ep"), lax.axis_size("tp")
    rows = argument["rows"].shape[0]
    experts = argument["wg"].shape[0]
    cap = max(2, 3 * rows * TOP_K // (2 * experts * n_ep))
    wide = all(argument[n].shape[-1] % LANES == 0 for n in ("x", "b", "wg", "wd", "sg"))
    fits = tp == 4 and n_ep % 2 == 0 and n_ep >= 8 and experts == 2
    fits = fits and wide and cap % 16 == 0 and rows % 32 == 0
    return fused_on_device(*given) if fits else on_device(*given)


def solution(mesh):
    return jax.shard_map(
        choose,
        mesh=mesh,
        in_specs=(
            P("ep", "tp"),
            P("ep", "tp"),
            P("ep", "tp"),
            P("ep", "tp"),
            P("ep", "tp"),
            P("ep", "tp"),
            P("tp"),
            P("tp"),
            P(None, "tp"),
            P(None, "tp"),
            P(None, "tp"),
            P("tp"),
            P(None, "tp"),
            P("ep", None),
            P(),
            P("ep", None),
            P("ep", None),
            P("ep", None, "tp"),
            P("ep", None, "tp"),
            P("ep", None, "tp"),
            P(None, "tp"),
            P(None, "tp"),
            P(None, "tp"),
        ),
        out_specs=(P("ep", "tp"), P("ep", "tp")),
        check_vma=False,
    )
```

```python
import functools
import types

import jax
import jax.numpy as jnp
from jax import lax
from jax.experimental import pallas as pl
from jax.experimental.pallas import tpu as pltpu
from jax.sharding import PartitionSpec as P

HEAD_DIM = 64
STATE = 128
CONV_TAPS = 4
BLOCK = 128
TOP_K = 4


epsilon = 1e-05
precise = lax.Precision.HIGHEST


def passed_along(x, axis, by):
    size = lax.axis_size(axis)
    pairs = [(i, i + by) for i in range(size) if 0 <= i + by < size]
    return lax.ppermute(x, axis, pairs)


def carried_in(total_log, state, axis):
    size = lax.axis_size(axis)
    place = lax.axis_index(axis)
    log = passed_along(total_log, axis, 1)
    hold = passed_along(state.astype(jnp.bfloat16), axis, 1).astype(jnp.float32)
    by = 1
    while by < size - 1:
        before = passed_along(hold.astype(jnp.bfloat16), axis, by).astype(jnp.float32)
        hold = hold + jnp.exp(log)[:, None, None] * before
        log = log + passed_along(log, axis, by)
        by *= 2
    return hold


def conv_silu(tail_rows, source, weights):
    length = source.shape[0]
    padded = jnp.concatenate([tail_rows, source], axis=0)
    total_sum = jnp.zeros(source.shape, jnp.float32)
    for tap_index in range(CONV_TAPS):
        total_sum = (
            total_sum
            + padded[tap_index : tap_index + length].astype(jnp.float32) * weights[tap_index]
        )
    return jax.nn.silu(total_sum).astype(jnp.bfloat16)


def carry_blocks(carried, inputs):
    block_decay, block_state = inputs
    return (carried * block_decay[:, None, None] + block_state, carried)


def earlier_counts(mask, rows):
    at = jnp.arange(rows)
    tri = (at[:, None] < at[None, :]).astype(jnp.bfloat16)
    return lax.dot_general(
        mask.astype(jnp.bfloat16),
        tri,
        (((mask.ndim - 1,), (0,)), ((), ())),
        preferred_element_type=jnp.float32,
    )


def on_device(
    mixer_value_input,
    input_state_matrix,
    output_state_matrix,
    output_gate_input,
    step_input,
    extra_log_decay,
    head_log_decay,
    head_skip_scale,
    value_kernel,
    input_matrix_kernel,
    output_matrix_kernel,
    mixer_norm_scale,
    mixer_output_weight,
    second_token_rows,
    expert_norm_scale,
    routed_expert_index,
    routed_expert_weight,
    routed_gate_weight,
    routed_up_weight,
    routed_down_weight,
    shared_gate_weight,
    shared_up_weight,
    shared_down_weight,
):
    length = mixer_value_input.shape[0]
    heads_local = step_input.shape[1]
    width_x = mixer_value_input.shape[1]
    width_b = input_state_matrix.shape[1]
    groups_local = width_b // STATE
    head_ratio = heads_local // groups_local
    nblocks = length // BLOCK
    lead_row = length - CONV_TAPS + 1
    edge_rows = jnp.concatenate(
        [
            mixer_value_input[lead_row:],
            input_state_matrix[lead_row:],
            output_state_matrix[lead_row:],
        ],
        axis=1,
    )
    tail_rows = passed_along(edge_rows, "ep", 1)
    rows_local = second_token_rows.shape[0]
    model_width = second_token_rows.shape[1]
    local_experts = routed_gate_weight.shape[0]
    ep_count = lax.axis_size("ep")
    experts = local_experts * ep_count
    capacity = max(2, 3 * rows_local * TOP_K // (2 * experts))
    col_width = model_width // lax.axis_size("tp")
    rows_wide = second_token_rows.astype(jnp.float32)
    normed = (
        rows_wide
        * lax.rsqrt(jnp.mean(rows_wide * rows_wide, axis=-1, keepdims=True) + epsilon)
        * expert_norm_scale
    ).astype(jnp.bfloat16)
    ids = routed_expert_index.T.astype(jnp.float32)
    id_rows = -(-ids.size // col_width)
    id_block = jnp.pad(
        ids.astype(jnp.bfloat16).reshape(-1), (0, id_rows * col_width - ids.size)
    ).reshape(id_rows, col_width)
    id_block = jnp.pad(id_block, ((0, -id_rows % 8), (0, 0)))
    my_columns = lax.dynamic_slice_in_dim(normed, lax.axis_index("tp") * col_width, col_width, 1)
    outgoing, value_rows, in_rows, out_rows = lax.optimization_barrier(
        (
            jnp.concatenate([my_columns, id_block], axis=0),
            mixer_value_input,
            input_state_matrix,
            output_state_matrix,
        )
    )
    everyone = lax.all_gather(outgoing, "ep", axis=0)
    values = conv_silu(tail_rows[:, :width_x], value_rows, value_kernel)
    in_mat = conv_silu(
        tail_rows[:, width_x : width_x + width_b], in_rows, input_matrix_kernel
    )
    out_mat = conv_silu(
        tail_rows[:, width_x + width_b :], out_rows, output_matrix_kernel
    )
    step_length = jax.nn.softplus(step_input)
    decay_logarithm = -jnp.exp(head_log_decay)[None, :] * step_length + extra_log_decay
    running = jnp.cumsum(decay_logarithm.reshape(nblocks, BLOCK, heads_local), axis=1)
    value_wide = values.astype(jnp.float32).reshape(nblocks, BLOCK, heads_local, HEAD_DIM)
    scaled = value_wide * step_length.reshape(nblocks, BLOCK, heads_local)[..., None]
    in_blocks = in_mat.reshape(nblocks, BLOCK, groups_local, STATE)
    out_blocks = out_mat.reshape(nblocks, BLOCK, groups_local, STATE)
    scores = jnp.einsum(
        "bign,bjgn->bgij", out_blocks, in_blocks, preferred_element_type=jnp.float32
    )
    scores = jnp.repeat(scores, head_ratio, axis=1)
    spread = jnp.transpose(running[:, :, None, :] - running[:, None, :, :], (0, 3, 1, 2))
    lower_mask = jnp.tril(jnp.ones((BLOCK, BLOCK), bool))[None, None]
    decay_mat = jnp.where(lower_mask, jnp.exp(jnp.where(lower_mask, spread, 0.0)), 0.0)
    inside = jnp.einsum("bhij,bjhp->bihp", scores * decay_mat, scaled, precision=precise)
    out_head = jnp.repeat(out_blocks.astype(jnp.float32), head_ratio, axis=2)
    in_head = jnp.repeat(in_blocks.astype(jnp.float32), head_ratio, axis=2)
    block_logs = running[:, -1]
    to_end = jnp.exp(block_logs[:, None, :] - running)
    block_state = jnp.einsum("bjhn,bjh,bjhp->bhpn", in_head, to_end, scaled, precision=precise)
    start_state = jnp.zeros((heads_local, HEAD_DIM, STATE), jnp.float32)
    local_total, local_prev = lax.scan(
        carry_blocks, start_state, (jnp.exp(block_logs), block_state)
    )
    before_logs = jnp.cumsum(block_logs, axis=0) - block_logs
    everyone, local_total = lax.optimization_barrier((everyone, local_total))
    incoming = carried_in(jnp.sum(block_logs, axis=0), local_total, "ep")
    their_rows = everyone[:, :rows_local]
    their_ids = everyone[:, rows_local : rows_local + id_rows].reshape(ep_count, -1)
    their_ids = their_ids[:, : ids.size].reshape(ep_count, TOP_K, rows_local).astype(jnp.float32)
    mine = (lax.axis_index("ep") * local_experts + jnp.arange(local_experts)).astype(jnp.float32)
    named = jnp.any(their_ids[:, None] == mine[None, :, None, None], axis=2)
    seat = jnp.where(named, earlier_counts(named, rows_local), -1.0)
    seats = jnp.arange(capacity, dtype=jnp.float32)
    pick = (seat[:, :, None, :] == seats[None, None, :, None]).astype(jnp.bfloat16)
    arrived = jnp.stack(
        [
            jnp.einsum(
                "bsr,brd->bsd", pick[:, j], their_rows, preferred_element_type=jnp.float32
            )
            .astype(jnp.bfloat16)
            .reshape(ep_count * capacity, col_width)
            for j in range(local_experts)
        ]
    )
    column_piece = lax.all_gather(arrived, "tp", axis=2, tiled=True)
    column_piece, incoming = lax.optimization_barrier((column_piece, incoming))
    entering = local_prev + jnp.exp(before_logs)[:, :, None, None] * incoming[None]
    carried_term = (
        jnp.einsum("bihn,bhpn->bihp", out_head, entering, precision=precise)
        * jnp.exp(running)[..., None]
    )
    mixed_heads = (inside + carried_term).reshape(length, heads_local, HEAD_DIM)
    mixed_heads = mixed_heads + head_skip_scale[None, :, None] * value_wide.reshape(
        length, heads_local, HEAD_DIM
    )
    gated_heads = mixed_heads * jax.nn.silu(output_gate_input.astype(jnp.float32)).reshape(
        length, heads_local, HEAD_DIM
    )
    grouped = gated_heads.reshape(length, groups_local, head_ratio * HEAD_DIM)
    grouped = grouped * lax.rsqrt(jnp.mean(grouped * grouped, axis=-1, keepdims=True) + epsilon)
    mixer_normed = (grouped.reshape(length, width_x) * mixer_norm_scale).astype(jnp.bfloat16)
    gate_pre = jnp.einsum(
        "esd,edf->esf", column_piece, routed_gate_weight, preferred_element_type=jnp.float32
    )
    up_pre = jnp.einsum(
        "esd,edf->esf", column_piece, routed_up_weight, preferred_element_type=jnp.float32
    )
    hidden = (jax.nn.silu(gate_pre) * up_pre).astype(jnp.bfloat16)
    shared_hidden = (
        jax.nn.silu(jnp.dot(normed, shared_gate_weight, preferred_element_type=jnp.float32))
        * jnp.dot(normed, shared_up_weight, preferred_element_type=jnp.float32)
    ).astype(jnp.bfloat16)
    whole_hidden = lax.all_gather(hidden, "tp", axis=2, tiled=True)
    both = lax.all_gather(
        jnp.concatenate([mixer_normed, shared_hidden], axis=1), "tp", axis=1, tiled=True
    ).reshape(length, lax.axis_size("tp"), -1)
    whole_mix = both[:, :, :width_x].reshape(length, -1)
    whole_shared = both[:, :, width_x:].reshape(length, -1)
    mixer_output = jnp.dot(
        whole_mix, mixer_output_weight, preferred_element_type=jnp.float32
    ).astype(jnp.bfloat16)
    expert_result = jnp.einsum(
        "esf,efd->esd", whole_hidden, routed_down_weight, preferred_element_type=jnp.float32
    ).astype(jnp.bfloat16)
    going = jnp.concatenate(
        [expert_result[j].reshape(ep_count, capacity, col_width) for j in range(local_experts)],
        axis=1,
    )
    returned = lax.all_to_all(going, "ep", split_axis=0, concat_axis=0, tiled=True)
    returned = returned.reshape(experts * capacity, col_width)
    kinds = jnp.arange(experts, dtype=jnp.float32)
    chosen = ids[:, None, :] == kinds[None, :, None]
    count = earlier_counts(jnp.any(chosen, axis=0), rows_local)
    position = jnp.sum(jnp.where(chosen, count[None], 0.0), axis=1)
    slot = (ids * capacity + position).T.astype(jnp.int32)
    columns = jnp.arange(experts * capacity, dtype=jnp.int32)[None, :]
    spread = jnp.zeros((rows_local, experts * capacity), jnp.float32)
    for k in range(TOP_K):
        spread = spread + jnp.where(
            slot[:, k : k + 1] == columns, routed_expert_weight[:, k : k + 1], 0.0
        )
    high = lax.reduce_precision(spread, 8, 7)
    low = (spread - high).astype(jnp.bfloat16)
    routed_sum = jnp.dot(
        high.astype(jnp.bfloat16), returned, preferred_element_type=jnp.float32
    ) + jnp.dot(low, returned, preferred_element_type=jnp.float32)
    shared_result = jnp.dot(whole_shared, shared_down_weight, preferred_element_type=jnp.float32)
    routed_out = (routed_sum + shared_result).astype(jnp.bfloat16)
    return (mixer_output, routed_out)


MESH = pl.DeviceIdType.MESH
HALO = 16
LANES = 128


def silu(v):
    return v / (1.0 + jnp.exp(-v))


def dot(a, b, contract=((1,), (0,)), exact=False):
    return lax.dot_general(
        a,
        b,
        (contract, ((), ())),
        precision=precise if exact else None,
        preferred_element_type=jnp.float32,
    )


def iota(shape, axis):
    return lax.broadcasted_iota(jnp.int32, shape, axis)


def at(start, size):
    return pl.ds(pl.multiple_of(start, size), size)


def body(dims, names, *refs):
    r = types.SimpleNamespace(**dict(zip(names, refs)))
    n_ep, rows, cap, ratio = dims.n_ep, dims.rows, dims.cap, dims.ratio
    nz = n_ep // 2
    half = rows // 2
    tp = dims.tp
    quarter = dims.quarter
    heads, groups, width = dims.heads, dims.groups, dims.width
    band = ratio * HEAD_DIM
    ff, sff = dims.ff, dims.sff
    f32, bf16 = jnp.float32, jnp.bfloat16

    e, t = lax.axis_index("ep"), lax.axis_index("tp")
    z, c = lax.div(e, 2), lax.rem(e, 2)
    other = 1 - c
    partner = e + 1 - 2 * c
    tx = t + 1 - 2 * lax.rem(t, 2)
    ty = lax.rem(t + 2, tp)
    td = tp - 1 - t

    def remote(src, dst, send, recv, to):
        return pltpu.make_async_remote_copy(
            src_ref=src, dst_ref=dst, send_sem=send, recv_sem=recv, device_id=to, device_id_type=MESH
        )

    fetched = dims.fetched

    def fetch(name):
        return pltpu.make_async_copy(
            getattr(r, name), getattr(r, "v_" + name), r.local_sem.at[fetched.index(name)]
        )

    for name in fetched:
        fetch(name).start()

    def got(*wanted):
        for name in wanted:
            fetch(name).wait()

    barrier = pltpu.get_barrier_semaphore()
    for by in range(1, n_ep):
        pl.semaphore_signal(barrier, inc=1, device_id=(lax.rem(e + by, n_ep), t), device_id_type=MESH)
    for to in (tx, ty):
        pl.semaphore_signal(barrier, inc=1, device_id=(e, to), device_id_type=MESH)

    longer = jnp.maximum(z, nz - 1 - z)
    inward = jnp.where(2 * z > nz - 1, -1, 1)

    def zsource(k):
        return jnp.where(k <= longer, z + inward * k, z - inward * (k - longer))

    def sent(ref, sem):
        remote(ref, ref, sem, sem, (partner, t)).wait_send()

    def landed(ref, sem):
        remote(ref, ref, sem, sem, (partner, t)).wait_recv()

    def plane(buf, send, recv):
        def leg(q, piece, slot, to):
            return remote(buf(q, piece), buf(q, piece), send, recv(slot), (e, to))

        def lead():
            leg(t, 0, 0, tx).start()
            leg(t, 1, 1, ty).start()

        def follow():
            leg(t, 1, 2, tx).start()
            leg(t, 0, 3, ty).start()

        def start():
            lead()
            follow()

        def relay():
            leg(tx, 0, 0, tx).wait_recv()
            leg(tx, 0, 4, ty).start()
            leg(ty, 1, 1, ty).wait_recv()
            leg(ty, 1, 5, tx).start()

        return types.SimpleNamespace(start=start, lead=lead, follow=follow, relay=relay)

    def token_leg(source, q, piece, slot, to):
        ref = r.tok.at[2 * source + c, q, pl.ds(piece * half, half)]
        return remote(ref, ref, r.tok_send, r.tok_recv.at[source, slot], (e, to))

    def token_legs(source, piece):
        return token_leg(source, t, piece, 0, tx), token_leg(source, t, piece, 1, ty)

    def hiddens(k):
        return plane(
            lambda q, piece: r.hid.at[k, q, pl.ds(piece * 2 * cap, 2 * cap)],
            r.hid_send,
            lambda slot: r.hid_recv.at[k, min(slot, 2)],
        )

    shares = plane(
        lambda q, piece: r.share.at[q, pl.ds(piece * half, half)],
        r.share_send,
        lambda slot: r.share_recv.at[min(slot, 2)],
    )
    mixes = plane(
        lambda q, piece: r.mix.at[q, pl.ds(piece * half, half)],
        r.mix_send,
        lambda slot: r.mix_recv.at[min(slot, 4)],
    )

    def across(source, q, whose):
        ref = r.tok.at[2 * source + whose, q]
        return remote(ref, ref, r.pair_send, r.pair_recv.at[source], (partner, t))

    def along(source, slot, up):
        block = 2 * source + c
        ref = r.tok.at[block, td] if slot == 2 else r.tok.at[block, t, pl.ds(slot * half, half)]
        to = 2 * (z - 1 + 2 * up) + c
        return remote(ref, ref, r.z_send.at[source, up], r.z_recv.at[source, slot], (to, t))

    def onward(up):
        to = z - 1 + 2 * up
        return jnp.logical_and(to >= 0, to < nz)

    def sides(s, act):
        for way in (1, -1):
            source = z + way * inward * s

            @pl.when(jnp.logical_and(source >= 0, source < nz))
            def _(source=source, way=way):
                act(source, lax.div(1 - way * inward, 2), way)

    def pass_on(source, slot, up):
        along(source, slot, 1 - up).wait_recv()

        @pl.when(onward(up))
        def _():
            along(source, slot, up).start()

    def near_piece(piece, source, up, way):
        pass_on(source, piece, up)
        if way > 0:
            for one in token_legs(source, piece):
                one.start()

    def near_rest(source, up, way):
        near_piece(1, source, up, way)
        if way > 0:
            across(source, t, c).start()

    def near_part(source, up, way):
        near_piece(0, source, up, way)
        near_rest(source, up, way)

    def late_legs(k):
        source = zsource(k)

        @pl.when(jnp.logical_and(k > longer, k < nz))
        def _():
            for piece in range(2):
                for one in token_legs(source, piece):
                    one.start()
            across(source, t, c).start()

    def far_part(source, up, way):
        pass_on(source, 2, up)
        across(source, td, c).start()

    def route_to(to):
        ref = r.route.at[e]
        return remote(ref, ref, r.route_send, r.route_recv.at[e], (to, t))

    def route_from(source):
        ref = r.route.at[source]
        return remote(ref, ref, r.route_send, r.route_recv.at[source], (e, t))

    edges = ((r.v_x, r.halo_x), (r.v_b, r.halo_b), (r.v_c, r.halo_c))

    def halo(i):
        src, dst = edges[i]
        return remote(
            src.at[pl.ds(rows - HALO, HALO)], dst, r.halo_send.at[i], r.halo_recv.at[i], (lax.rem(e + 1, n_ep), t)
        )

    got("rows", "scale")
    step_rows = 16

    def norm_rows(i, _):
        part = r.v_rows[at(i * step_rows, step_rows), :].astype(f32)
        by = lax.rsqrt(jnp.mean(part * part, axis=-1, keepdims=True) + epsilon)
        part = (part * by * r.v_scale[...]).astype(bf16)
        for q in range(tp):
            r.tok[e, q, at(i * step_rows, step_rows), :] = part[:, q * quarter : (q + 1) * quarter]
        return 0

    lax.fori_loop(0, rows // step_rows, norm_rows, 0, unroll=4)
    got("ids", "wts")
    below = iota((rows, rows), 0)
    right = iota((rows, rows), 1)
    r.earlier[...] = (below < right).astype(bf16)
    r.route[e, 0:TOP_K, :] = r.v_ids[...].astype(f32)
    r.route[e, TOP_K : 2 * TOP_K, :] = r.v_wts[...]
    got("x", "b", "c")
    pl.semaphore_wait(barrier, n_ep - 1 + 2)

    @pl.when(e + 1 < n_ep)
    def _():
        for i in range(3):
            halo(i).start()

    route_to(partner).start()
    for slot in range(3):
        for up in (1, 0):

            @pl.when(onward(up))
            def _():
                along(z, slot, up).start()

    for q in range(tp):
        across(z, q, c).start()
    for by in range(1, n_ep):
        to = lax.rem(e + by, n_ep)

        @pl.when(to != partner)
        def _(to=to):
            route_to(to).start()

    got("sg", "su")
    gate, up = 0.0, 0.0
    for q in range(tp):
        part = r.tok[e, q]
        gate = gate + dot(part, r.v_sg[q * quarter : (q + 1) * quarter, :])
        up = up + dot(part, r.v_su[q * quarter : (q + 1) * quarter, :])
    r.share[t] = (silu(gate) * up).astype(bf16)
    shares.start()

    def enter(k):
        source = zsource(k)
        seats = iota((cap, rows), 0).astype(f32)
        for c2 in range(2):
            block = 2 * source + c2
            ids = r.route[block, 0:TOP_K, :]
            weights = r.route[block, TOP_K : 2 * TOP_K, :]
            for j in range(2):
                hit = ids == (2 * e + j).astype(f32)
                named = jnp.sum(jnp.where(hit, 1.0, 0.0), axis=0, keepdims=True)
                given = jnp.sum(jnp.where(hit, weights, 0.0), axis=0, keepdims=True)
                count = dot(jnp.broadcast_to(named, (16, rows)).astype(bf16), r.earlier[...])
                seat = jnp.where(named > 0.0, count[0:1, :], -1.0)
                taken = seats == seat
                r.pick[k, c2, j * cap : (j + 1) * cap, :] = jnp.where(taken, 1.0, 0.0).astype(bf16)
                amount = jnp.sum(jnp.where(taken, given, 0.0), axis=1, keepdims=True)
                r.amount[k, j, c2 * cap : (c2 + 1) * cap, :] = jnp.broadcast_to(amount, (cap, LANES))
            for q in range(tp):
                chosen = dot(r.pick[k, c2], r.tok[block, q]).astype(bf16)
                for j in range(2):
                    r.arrived[j, c2 * cap : (c2 + 1) * cap, q * quarter : (q + 1) * quarter] = chosen[
                        j * cap : (j + 1) * cap, :
                    ]
        for j in range(2):
            gate = dot(r.arrived[j], r.v_wg[j])
            up = dot(r.arrived[j], r.v_wu[j])
            r.hid[k, t, j * 2 * cap : (j + 1) * 2 * cap, :] = (silu(gate) * up).astype(bf16)

    @pl.when(e > 0)
    def _():
        for i in range(3):
            halo(i).wait_recv()

    @pl.when(e == 0)
    def _():
        for _, dst in edges:
            dst[...] = jnp.zeros_like(dst)

    got("vk", "bk", "ck", "step", "extra", "hld")

    def conv(src, edge, taps, out):
        def chunk(i, _):
            lanes = at(i * LANES, LANES)
            r.padded[0:8, :] = edge[:, lanes].astype(f32)[HALO - 8 :]
            r.padded[8 : 8 + rows, :] = src[:, lanes].astype(f32)
            total = jnp.zeros((rows, LANES), f32)
            for k in range(CONV_TAPS):
                lead = 8 - CONV_TAPS + 1 + k
                total = total + r.padded[lead : lead + rows, :] * taps[k : k + 1, lanes]
            out[:, lanes] = silu(total).astype(bf16)
            return 0

        lax.fori_loop(0, src.shape[1] // LANES, chunk, 0)

    conv(r.v_x, r.halo_x, r.v_vk, r.vals)
    conv(r.v_b, r.halo_b, r.v_bk, r.inm)
    conv(r.v_c, r.halo_c, r.v_ck, r.outm)
    route_from(partner).wait_recv()
    got("wg", "wu")
    landed(r.tok.at[2 * z + other], r.pair_recv.at[z])
    enter(0)
    hiddens(0).start()
    shares.relay()
    sides(1, functools.partial(near_piece, 0))
    pre = r.v_step[...]
    steps = jnp.maximum(pre, 0.0) + jnp.log(1.0 + jnp.exp(-jnp.abs(pre)))
    diagonal = iota((heads, heads), 0) == iota((heads, heads), 1)
    rate = jnp.sum(jnp.where(diagonal, jnp.exp(r.v_hld[...]), 0.0), axis=1, keepdims=True)
    decay = -rate * steps + r.v_extra[...]
    upto = (below <= right).astype(f32)
    cum_t = dot(decay, upto, exact=True)
    cum = dot((right <= below).astype(f32), decay, ((1,), (1,)), exact=True)
    r.cum[...] = cum
    r.cum_t[...] = cum_t
    r.step_t[...] = steps
    spread_heads = (lax.div(iota((heads, width), 1), HEAD_DIM) == iota((heads, width), 0)).astype(f32)
    r.growth[...] = dot(jnp.exp(cum), spread_heads, exact=True)
    to_end = jnp.exp(cum_t[:, rows - 1 : rows] - cum_t) * steps
    r.to_end[...] = dot(to_end, spread_heads, ((0,), (0,)), exact=True)
    for g in range(groups):
        lanes = pl.ds(g * band, band)
        weighted = (r.vals[:, lanes].astype(f32) * r.to_end[:, lanes]).astype(bf16)
        r.state[:, lanes] = dot(r.inm[:, g * STATE : (g + 1) * STATE], weighted, ((0,), (0,)))
    r.state_out[...] = r.state[...].astype(bf16)
    r.decay_out[...] = jnp.broadcast_to(r.growth[rows - 1 : rows, :], (8, width))

    def swap(i):
        src, dst = ((r.state_out, r.state_in), (r.decay_out, r.decay_in))[i]
        return remote(src, dst, r.swap_send.at[i], r.swap_recv.at[i], (partner, t))

    for i in range(2):
        swap(i).start()
    side = width // 2
    mine_lanes = at(c * side, side)

    def chain(up):
        to = 2 * (z + up) + c
        return remote(r.after, r.before, r.chain_sem.at[0], r.chain_sem.at[1], (to, t))

    def halves(whose):
        ref = r.incoming.at[whose]
        return remote(ref, ref, r.half_sem.at[0], r.half_sem.at[1], (partner, t))

    def chain_step():
        for i in range(2):
            swap(i).wait_recv()
        ours, theirs = r.state[:, mine_lanes], r.state_in[:, mine_lanes].astype(f32)
        our_decay, their_decay = r.decay_out[:, mine_lanes], r.decay_in[:, mine_lanes]
        first = jnp.where(c == 0, ours, theirs)
        second = jnp.where(c == 0, theirs, ours)
        late = jnp.where(c == 0, their_decay, our_decay)
        chip = late[0:1, :] * first + second

        @pl.when(z == 0)
        def _():
            r.before[...] = jnp.zeros_like(r.before)

        @pl.when(z > 0)
        def _():
            chain(0).wait_recv()

        r.incoming[c] = r.before[...]
        halves(c).start()

        @pl.when(onward(1))
        def _():
            both = our_decay[0:1, :] * their_decay[0:1, :]
            r.after[...] = (both * r.before[...].astype(f32) + chip).astype(bf16)
            chain(1).start()

    def inside():
        mid = rows // 2
        lane = iota((mid, 2 * HEAD_DIM), 1) < HEAD_DIM
        for g in range(groups):
            cols = slice(g * STATE, (g + 1) * STATE)
            for part in range(2):
                span = slice(part * mid, (part + 1) * mid)
                reach = (part + 1) * mid
                scores = dot(r.outm[span, cols], r.inm[0:reach, cols], ((1,), (1,)))
                mask = iota((mid, reach), 0) + part * mid >= iota((mid, reach), 1)
                for p in range(ratio // 2):
                    pair = []
                    head = g * ratio + 2 * p
                    lanes = slice(head * HEAD_DIM, (head + 2) * HEAD_DIM)
                    for h in (head, head + 1):
                        diff = r.cum[span, h : h + 1] - r.cum_t[h : h + 1, 0:reach]
                        grid = scores * jnp.exp(jnp.where(mask, diff, -1e30)) * r.step_t[h : h + 1, 0:reach]
                        pair.append(dot(grid.astype(bf16), r.vals[0:reach, lanes]))
                    r.near[span, lanes] = jnp.where(lane, pair[0], pair[1])

    def back_pair(k):
        return remote(r.yours.at[k], r.theirs.at[k], r.pair_y_send, r.pair_y_recv.at[k], (partner, t))

    def back(k):
        source = zsource(k)
        return remote(r.going.at[k], r.coming.at[z], r.y_send, r.y_recv.at[z], (2 * source + c, t))

    def back_in(source):
        return remote(r.going.at[0], r.coming.at[source], r.y_send, r.y_recv.at[source], (e, t))

    def leave(k, carry=0):
        landed(r.hid.at[k, 0:2], r.hid_recv.at[k, 2])
        for j in range(2):
            total = 0.0
            for q in range(tp):
                total = total + dot(
                    r.hid[k, q, j * 2 * cap : (j + 1) * 2 * cap, :], r.v_wd[j, q * ff : (q + 1) * ff, :]
                )
            total = (total * r.amount[k, j, :, 0:1]).astype(bf16)
            for c2 in range(2):
                r.result[c2, j * cap : (j + 1) * cap, :] = total[c2 * cap : (c2 + 1) * cap, :]
        r.yours[k] = dot(r.pick[k, other], r.result[other], ((0,), (0,))).astype(bf16)
        back_pair(k).start()
        r.ours[k] = dot(r.pick[k, c], r.result[c], ((0,), (0,)))
        return carry

    edge = jnp.logical_or(z == 0, z == nz - 1)
    second = jnp.logical_or(z == 1, z == nz - 2)

    def passing():
        to = 2 * (z + inward) + c
        return remote(r.going.at[2], r.passed, r.y_send, r.passed_sem, (to, t))

    def send_back(k, carry=0):
        @pl.when(jnp.logical_not(jnp.logical_and(k == 1, second)))
        def _():
            back_pair(k).wait_recv()
            r.going[k] = (r.ours[k] + r.theirs[k].astype(f32)).astype(bf16)
            aside = jnp.logical_and(k == 2, edge)

            @pl.when(aside)
            def _():
                passing().start()

            @pl.when(jnp.logical_not(aside))
            def _():
                back(k).start()

        return carry

    def join_back():
        @pl.when(second)
        def _():
            back_pair(1).wait_recv()
            landed(r.passed, r.passed_sem)
            total = r.ours[1] + r.theirs[1].astype(f32) + r.passed[...].astype(f32)
            r.going[1] = total.astype(bf16)
            back(1).start()


    sides(1, near_rest)

    @pl.when(z == 0)
    def _():
        chain_step()

    hiddens(0).relay()

    def stage(k, _):
        source = zsource(k)

        sides(k, far_part)

        @pl.when(k == 1)
        def _():
            inside()

        @pl.when(k == 2)
        def _():
            got("wd")

        @pl.when(k == nz - 1)
        def _():
            hiddens(k - 1).relay()

        for slot, q in ((0, tx), (1, ty)):
            landed(r.tok.at[2 * source + c, q], r.tok_recv.at[source, slot])
            across(source, q, c).start()
        for c2 in range(2):
            route_from(2 * source + c2).wait_recv()

        @pl.when(k != nz - 2)
        def _():
            sides(k + 1, near_part)

        @pl.when(k == z)
        def _():
            chain_step()

        landed(r.tok.at[2 * source + other], r.pair_recv.at[source])
        enter(k)
        hiddens(k).lead()

        @pl.when(k == nz - 2)
        def _():
            sides(k + 1, near_part)

        hiddens(k).follow()
        late_legs(k + 2)

        @pl.when(jnp.logical_and(k > 1, k < nz - 1))
        def _():
            hiddens(k - 1).relay()

        return 0

    lax.fori_loop(1, nz, stage, 0)

    got("gate", "skip", "mscale")

    def mixer_end():
        halves(other).wait_recv()
        spread_heads = (lax.div(iota((heads, width), 1), HEAD_DIM) == iota((heads, width), 0)).astype(f32)
        skip = dot(jnp.broadcast_to(r.v_skip[...], (8, heads)), spread_heads, exact=True)[0:1, :]
        for s in range(2):
            lanes = slice(s * side, (s + 1) * side)
            hold = r.incoming[s].astype(f32)
            later = r.decay_in[0:1, lanes] * hold + r.state_in[:, lanes].astype(f32)
            r.entering[:, lanes] = jnp.where(c == 0, hold, later).astype(bf16)
        for g in range(groups):
            lanes = slice(g * band, (g + 1) * band)
            far = dot(r.outm[:, g * STATE : (g + 1) * STATE], r.entering[:, lanes]) * r.growth[:, lanes]
            mixed = r.near[:, lanes] + far + skip[:, lanes] * r.vals[:, lanes].astype(f32)
            gated = mixed * silu(r.v_gate[:, lanes].astype(f32))
            by = lax.rsqrt(jnp.mean(gated * gated, axis=-1, keepdims=True) + epsilon)
            r.mix[t, :, lanes] = (gated * by * r.v_mscale[:, lanes]).astype(bf16)

    mixer_end()
    leave(nz - 2)
    hiddens(nz - 1).relay()
    mixes.start()
    send_back(nz - 2)
    lax.fori_loop(2, nz - 1, lambda i, carry: leave(nz - 1 - i, carry), 0)
    lax.fori_loop(2, nz - 1, lambda i, carry: send_back(nz - 1 - i, carry), 0)
    leave(nz - 1)
    leave(0)
    join_back()
    send_back(nz - 1)
    got("sd", "wm")

    landed(r.share.at[0:2], r.share_recv.at[2])
    routed = 0.0
    for q in range(tp):
        routed = routed + dot(r.share[q], r.v_sd[q * sff : (q + 1) * sff, :])
    r.mixer_sum[...] = dot(r.mix[t], r.v_wm[at(t * width, width), :])
    mixes.relay()
    back_pair(0).wait_recv()
    r.routed_sum[...] = routed + r.ours[0] + r.theirs[0].astype(f32)

    def add_back(k, _):
        source = zsource(k)
        low = jnp.logical_and(source == 0, z == 2)
        high = jnp.logical_and(source == nz - 1, z == nz - 3)

        @pl.when(jnp.logical_not(jnp.logical_or(low, high)))
        def _():
            back_in(source).wait_recv()
            r.routed_sum[...] += r.coming[source].astype(f32)

        return 0

    def add_mix(q):
        r.mixer_sum[...] += dot(r.mix[q], r.v_wm[at(q * width, width), :])

    def outcopy(i):
        src, dst = ((r.mixer_bf, r.mixer_out), (r.routed_bf, r.routed_out))[i]
        return pltpu.make_async_copy(src, dst, r.out_sem.at[i])

    landed(r.mix.at[0, 0:half], r.mix_recv.at[2])
    add_mix(tx)
    landed(r.mix.at[0, 0:half], r.mix_recv.at[3])
    add_mix(ty)
    lax.fori_loop(1, nz, add_back, 0)
    r.routed_bf[...] = r.routed_sum[...].astype(bf16)
    outcopy(1).start()
    landed(r.mix.at[0], r.mix_recv.at[4])
    add_mix(td)
    r.mixer_bf[...] = r.mixer_sum[...].astype(bf16)
    outcopy(0).start()

    @pl.when(e + 1 < n_ep)
    def _():
        for i in range(3):
            halo(i).wait_send()

    sent(r.route.at[0 : n_ep - 1], r.route_send)
    for i in range(2):
        swap(i).wait_send()

    @pl.when(onward(1))
    def _():
        chain(1).wait_send()

    halves(c).wait_send()
    sent(r.mix.at[0:3], r.mix_send)
    sent(r.share.at[0:3], r.share_send)
    sent(r.hid.at[:, 0:3], r.hid_send)
    sent(r.tok.at[0 : nz - 1, 0:2], r.tok_send)
    sent(r.tok.at[0:nz], r.pair_send)
    sent(r.yours, r.pair_y_send)
    sent(r.going.at[0 : nz - 1], r.y_send)

    def drain(source, _):
        for up in range(2):
            passed = source <= z if up else source >= z

            @pl.when(jnp.logical_and(passed, onward(up)))
            def _():
                sent(r.tok.at[0, 0:2], r.z_send.at[source, up])

        return 0

    lax.fori_loop(0, nz, drain, 0)
    for i in range(2):
        outcopy(i).wait()


def hand_out_body(first, second, first_out, second_out, held, sems):
    steps = []
    for i, (src, dst) in enumerate(((first, first_out), (second, second_out))):
        steps.append(
            (
                pltpu.make_async_copy(src, held.at[i], sems.at[i, 0]),
                pltpu.make_async_copy(held.at[i], dst, sems.at[i, 1]),
            )
        )
    for arrive, _ in steps:
        arrive.start()
    for arrive, depart in steps:
        arrive.wait()
        depart.start()
    for _, depart in steps:
        depart.wait()


def hand_out(first, second):
    out = jax.ShapeDtypeStruct(first.shape, first.dtype)
    return tuple(
        pl.pallas_call(
            hand_out_body,
            out_shape=(out, out),
            in_specs=[pl.BlockSpec(memory_space=pl.ANY)] * 2,
            out_specs=(pl.BlockSpec(memory_space=pl.ANY),) * 2,
            scratch_shapes=[pltpu.VMEM((2,) + first.shape, first.dtype), pltpu.SemaphoreType.DMA((2, 2))],
            name="hand_out",
        )(first, second)
    )


def fused_on_device(*given):
    argument = dict(zip(ARGUMENTS, given))
    rows, model_width = argument["rows"].shape
    n_ep, tp = lax.axis_size("ep"), lax.axis_size("tp")
    nz = n_ep // 2
    heads = argument["step"].shape[1]
    width = argument["x"].shape[1]
    state_width = argument["b"].shape[1]
    groups = state_width // STATE
    local_experts, _, ff = argument["wg"].shape
    sff = argument["sg"].shape[1]
    quarter = argument["wd"].shape[2]
    cap = max(2, 3 * rows * TOP_K // (2 * local_experts * n_ep))
    for name in ("hld", "skip", "mscale", "scale"):
        argument[name] = argument[name].reshape(1, -1)
    for name in ("ids", "wts", "step", "extra"):
        argument[name] = argument[name].T
    dims = types.SimpleNamespace(
        n_ep=n_ep, tp=tp, rows=rows, cap=cap, ratio=heads // groups, quarter=quarter, heads=heads,
        groups=groups, width=width, ff=ff, sff=sff,
        fetched=FETCHED,
    )
    f32, bf16 = jnp.float32, jnp.bfloat16
    scratch = dict(("v_" + n, pltpu.VMEM(argument[n].shape, argument[n].dtype)) for n in FETCHED)
    vmem = dict(
        tok=((n_ep, tp, rows, quarter), bf16),
        hid=((nz, tp, 4 * cap, ff), bf16),
        mix=((tp, rows, width), bf16),
        share=((tp, rows, sff), bf16),
        route=((n_ep, 2 * TOP_K, rows), f32),
        halo_x=((HALO, width), bf16),
        halo_b=((HALO, state_width), bf16),
        halo_c=((HALO, state_width), bf16),
        padded=((8 + rows, LANES), f32),
        vals=((rows, width), bf16),
        inm=((rows, state_width), bf16),
        outm=((rows, state_width), bf16),
        cum=((rows, heads), f32),
        cum_t=((heads, rows), f32),
        step_t=((heads, rows), f32),
        growth=((rows, width), f32),
        to_end=((rows, width), f32),
        state=((STATE, width), f32),
        state_out=((STATE, width), bf16),
        state_in=((STATE, width), bf16),
        decay_out=((8, width), f32),
        decay_in=((8, width), f32),
        before=((STATE, width // 2), bf16),
        after=((STATE, width // 2), bf16),
        incoming=((2, STATE, width // 2), bf16),
        entering=((STATE, width), bf16),
        near=((rows, width), f32),
        earlier=((rows, rows), bf16),
        pick=((nz, 2, 2 * cap, rows), bf16),
        amount=((nz, 2, 2 * cap, LANES), f32),
        arrived=((2, 2 * cap, model_width), bf16),
        result=((2, 2 * cap, quarter), bf16),
        yours=((nz, rows, quarter), bf16),
        theirs=((nz, rows, quarter), bf16),
        ours=((nz, rows, quarter), f32),
        going=((nz, rows, quarter), bf16),
        coming=((nz, rows, quarter), bf16),
        passed=((rows, quarter), bf16),
        routed_bf=((rows, quarter), bf16),
        mixer_bf=((rows, quarter), bf16),
        routed_sum=((rows, quarter), f32),
        mixer_sum=((rows, quarter), f32),
    )
    for name, (shape, dtype) in vmem.items():
        scratch[name] = pltpu.VMEM(shape, dtype)
    sems = dict(
        local_sem=(len(FETCHED),),
        out_sem=(2,),
        tok_send=(), tok_recv=(nz, 2), hid_send=(), hid_recv=(nz, 3),
        mix_send=(), mix_recv=(5,), pair_send=(), pair_recv=(nz,),
        z_send=(nz, 2), z_recv=(nz, 3), share_send=(), share_recv=(3,), route_send=(), route_recv=(n_ep,),
        halo_send=(3,), halo_recv=(3,), swap_send=(2,), swap_recv=(2,),
        chain_sem=(2,), half_sem=(2,), passed_sem=(),
        pair_y_send=(), pair_y_recv=(nz,), y_send=(), y_recv=(nz,),
    )
    for name, shape in sems.items():
        scratch[name] = pltpu.SemaphoreType.DMA(shape)
    order = tuple(FETCHED)
    names = order + ("mixer_out", "routed_out") + tuple(scratch)
    out = jax.ShapeDtypeStruct((rows, quarter), bf16)
    return hand_out(
        *pl.pallas_call(
            functools.partial(body, dims, names),
            out_shape=(out, out),
            in_specs=[pl.BlockSpec(memory_space=pl.ANY)] * len(order),
            out_specs=(pl.BlockSpec(memory_space=pl.ANY),) * 2,
            scratch_shapes=list(scratch.values()),
            compiler_params=pltpu.CompilerParams(
                collective_id=0, has_side_effects=True, vmem_limit_bytes=VMEM_LIMIT
            ),
            name="mixer_and_experts",
        )(*[argument[n] for n in order])
    )


VMEM_LIMIT = 62 * 1024 * 1024 + 512 * 1024
ARGUMENTS = (
    "x", "b", "c", "gate", "step", "extra", "hld", "skip", "vk", "bk", "ck", "mscale", "wm",
    "rows", "scale", "ids", "wts", "wg", "wu", "wd", "sg", "su", "sd",
)
FETCHED = (
    "rows", "scale", "ids", "wts", "x", "b", "c", "sg", "su", "vk", "bk", "ck", "step", "extra", "hld",
    "wg", "wu", "gate", "skip", "mscale", "wd", "sd", "wm",
)


def choose(*given):
    argument = dict(zip(ARGUMENTS, given))
    n_ep, tp = lax.axis_size("ep"), lax.axis_size("tp")
    rows = argument["rows"].shape[0]
    experts = argument["wg"].shape[0]
    cap = max(2, 3 * rows * TOP_K // (2 * experts * n_ep))
    wide = all(argument[n].shape[-1] % LANES == 0 for n in ("x", "b", "wg", "wd", "sg"))
    fits = tp == 4 and n_ep % 2 == 0 and n_ep >= 8 and experts == 2
    fits = fits and wide and cap % 16 == 0 and rows % 32 == 0
    return fused_on_device(*given) if fits else on_device(*given)


def solution(mesh):
    return jax.shard_map(
        choose,
        mesh=mesh,
        in_specs=(
            P("ep", "tp"),
            P("ep", "tp"),
            P("ep", "tp"),
            P("ep", "tp"),
            P("ep", "tp"),
            P("ep", "tp"),
            P("tp"),
            P("tp"),
            P(None, "tp"),
            P(None, "tp"),
            P(None, "tp"),
            P("tp"),
            P(None, "tp"),
            P("ep", None),
            P(),
            P("ep", None),
            P("ep", None),
            P("ep", None, "tp"),
            P("ep", None, "tp"),
            P("ep", None, "tp"),
            P(None, "tp"),
            P(None, "tp"),
            P(None, "tp"),
        ),
        out_specs=(P("ep", "tp"), P("ep", "tp")),
        check_vma=False,
    )
```
